32 devices in a mesh: grp: 2 (over y), kv: 4 (over z), tp: 4 (over x, core).
Axes of the slice: x: 2, y: 2, z: 4, core: 2. Of those that a mesh axis runs over, the one named last changes fastest.
Arguments:
- tokens: bfloat16 [8, 3, 4096], P(('grp', 'kv')), parts along dimension 0, may hold values from -6 to 6
- input_norm_scale: float32 [4096], replicated, may hold values from 0.1 to 1.9
- head_input_matrix: bfloat16 [4096, 8192], P('kv', 'tp'), may hold values from -0.09375 to 0.09375
- output_gate_matrix: bfloat16 [4096, 8192], P('kv', 'tp'), may hold values from -0.09375 to 0.09375
- group_input_matrix: bfloat16 [4096, 512], P('kv', 'tp'), may hold values from -0.09375 to 0.09375
- group_readout_matrix: bfloat16 [4096, 512], P('kv', 'tp'), may hold values from -0.09375 to 0.09375
- step_size_matrix: bfloat16 [4096, 128], P(None, 'tp'), may hold values from -0.09375 to 0.09375
- step_size_bias: float32 [128], P('tp'), may hold values from -4 to -1
- log_decay_rate: float32 [128], P('tp'), may hold values from -4.6 to 2
- direct_path_weight: float32 [128], P('tp'), may hold values from 0.1 to 1.9
- convolution_tap_weight: bfloat16 [4, 8, 1152], P(None, 'tp'), may hold values from -3 to 3
- convolution_history_rows: bfloat16 [8, 6, 8, 1152], P(('grp', 'kv'), None, 'tp'), parts along dimension 0, may hold values from -6 to 6
- per_proposal_states: float32 [8, 3, 128, 64, 64], P(('grp', 'kv'), None, 'tp'), parts along dimension 0, may hold values from -4 to 4
- accepted: int32 [8], P(('grp', 'kv')), parts along dimension 0, may hold values from 1 to 3
- proposal_extra_decay: float32 [8, 3, 128], P(('grp', 'kv'), None, 'tp'), parts along dimension 0, may hold values from -0.69 to 0
- group_norm_scale: float32 [8192], P('tp'), may hold values from 0.1 to 1.9
- output_projection_matrix: bfloat16 [8192, 4096], P('tp', 'kv'), may hold values from -0.0625 to 0.0625
Outputs:
- mixed: bfloat16 [8, 3, 4096], P(('grp', 'tp'), None, 'kv'), parts along dimension 0
- new_states: float32 [8, 3, 128, 64, 64], P(('grp', 'kv'), None, 'tp'), parts along dimension 0
- new_tail: bfloat16 [8, 6, 8, 1152], P(('grp', 'kv'), None, 'tp'), parts along dimension 0
The draws below stay inside these ranges and needn't reach their ends.
There are 2 independent parts, one for each index of `grp`. The reference program is written for one: setup_inputs(seed, part) draws one part's arguments, and reference() takes and returns one part's arrays. A program takes and returns all parts, laid end to end along the dimension named above; an argument that names none is the same for every part. Nothing has to cross between parts.
All inputs are finite; a program needn't handle non-finite values.
Results may differ from the reference program's by a relative error of at most 0.015.
Values may be sent and summed in bfloat16 or wider, within the bound.
No kernel may reach another device: no remote copies, remote signals or barrier semaphores. Data moves between devices by JAX's collectives and lax.ppermute only.
A program may use at most 64 MiB of HBM per device.

```python
import jax
import jax.numpy as jnp
from jax import lax

D = 4096
HEADS = 128
HEAD_DIM = 64
GROUPS = 8
STATE = 64
CONV_W = 4
PROP = 3
SEQS = 4
GROUP_CH = 1152
TAIL = 6
N_TP = 4


def draw_proposal_extra_decay(key, part):
    first_key, second_key = jax.random.split(jax.random.fold_in(key, 11))
    struck = jax.random.uniform(first_key, (SEQS, PROP, HEADS), jnp.float32) < 0.15
    depth = jax.random.uniform(second_key, (SEQS, PROP, HEADS), jnp.float32, 0.22, 0.69)
    return jnp.where(struck, -depth, 0.0).astype(jnp.float32)


def touch_ends(result, stream_key, least, largest):
    longest = result.shape.index(max(result.shape))
    spots = []
    for shift in (0, 1):
        where = [jax.random.randint(jax.random.fold_in(stream_key, axis), (), 0, length) for axis, length in enumerate(result.shape)]
        where[longest] = (where[longest] + shift) % result.shape[longest]
        spots.append(tuple(where))
    return result.at[spots[0]].set(least).at[spots[1]].set(largest)


def block_scale(stream_key, extent, pieces, smallest, top_value):
    level, own = 1.0, jax.random.fold_in(stream_key, 6)
    for axis_at, parts in pieces:
        heights = jnp.exp(jax.random.uniform(jax.random.fold_in(own, axis_at), (parts,), jnp.float32, smallest / len(pieces), top_value / len(pieces)))
        level = level * jnp.repeat(heights, extent[axis_at] // parts).reshape([-1 if axis == axis_at else 1 for axis in range(len(extent))])
    return level


def noise(rng, extent, deviation, reach, cuts=(), kind=jnp.bfloat16):
    gain = block_scale(rng, extent, cuts, -0.22, 0.18) if cuts else 1.0
    entries = jax.random.normal(rng, extent, jnp.float32) * deviation * gain
    return jnp.minimum(jnp.maximum(entries, -reach), reach).astype(kind)


def setup_inputs(seed: int = 0, part: int = 0) -> dict:
    key_of = jax.random.split(jax.random.key(seed), 18)
    part_splits = jax.random.split(jax.random.fold_in(key_of[17], part), 18)
    tokens = noise(part_splits[0], (SEQS, PROP, D), 1.0, 6.0, ((0, 4),))
    input_norm_scale = jnp.clip(1.0 + 0.18 * jax.random.normal(key_of[1], (D,), jnp.float32), 0.1, 1.9)
    head_input_matrix = noise(key_of[2], (D, HEADS * HEAD_DIM), D ** -0.5, 0.09375, ((0, 4), (1, 4)))
    output_gate_matrix = noise(key_of[3], (D, HEADS * HEAD_DIM), D ** -0.5, 0.09375, ((0, 4), (1, 4)))
    group_input_matrix = noise(key_of[4], (D, GROUPS * STATE), D ** -0.5, 0.09375, ((0, 4), (1, 4)))
    group_readout_matrix = noise(key_of[5], (D, GROUPS * STATE), D ** -0.5, 0.09375, ((0, 4), (1, 4)))
    step_size_matrix = noise(key_of[6], (D, HEADS), D ** -0.5, 0.09375, ((1, 4),))
    step_size_bias = jnp.clip(-4.0 + 3.0 * jax.random.uniform(key_of[7], (HEADS,), jnp.float32) ** block_scale(key_of[7], (HEADS,), ((0, 4),), -0.2, 0.2), -4.0, -1.0)
    log_decay_rate = jnp.clip(-4.6 + 6.6 * jax.random.uniform(key_of[8], (HEADS,), jnp.float32) ** block_scale(key_of[8], (HEADS,), ((0, 4),), -0.2, 0.2), -4.6, 2.0)
    direct_path_weight = jnp.clip(1.0 + 0.18 * jax.random.normal(key_of[9], (HEADS,), jnp.float32), 0.1, 1.9)
    convolution_tap_weight = noise(key_of[10], (CONV_W, GROUPS, GROUP_CH), 0.5, 3.0, ((1, 4),))
    convolution_history_rows = noise(part_splits[11], (SEQS, TAIL, GROUPS, GROUP_CH), 1.0, 6.0, ((0, 4), (2, 4)))
    per_proposal_states = noise(part_splits[12], (SEQS, PROP, HEADS, HEAD_DIM, STATE), 0.5, 4.0, ((0, 4), (2, 4)), jnp.float32)
    accepted = touch_ends(jax.random.randint(part_splits[13], (SEQS,), 1, PROP + 1), jax.random.fold_in(part_splits[13], 1), 1, PROP).astype(jnp.int32)
    proposal_extra_decay = draw_proposal_extra_decay(jax.random.fold_in(jax.random.fold_in(key_of[17], part), 71), part)
    group_norm_scale = jnp.clip(1.0 + 0.18 * jax.random.normal(key_of[15], (HEADS * HEAD_DIM,), jnp.float32), 0.1, 1.9)
    output_projection_matrix = noise(key_of[16], (HEADS * HEAD_DIM, D), (HEADS * HEAD_DIM) ** -0.5, 0.0625, ((0, 4), (1, 4)))
    return {"tokens": tokens, "input_norm_scale": input_norm_scale, "head_input_matrix": head_input_matrix, "output_gate_matrix": output_gate_matrix, "group_input_matrix": group_input_matrix, "group_readout_matrix": group_readout_matrix, "step_size_matrix": step_size_matrix, "step_size_bias": step_size_bias, "log_decay_rate": log_decay_rate, "direct_path_weight": direct_path_weight, "convolution_tap_weight": convolution_tap_weight, "convolution_history_rows": convolution_history_rows, "per_proposal_states": per_proposal_states, "accepted": accepted, "proposal_extra_decay": proposal_extra_decay, "group_norm_scale": group_norm_scale, "output_projection_matrix": output_projection_matrix}


epsilon = 1e-06

def rms_scale(values):
    return lax.rsqrt(lax.optimization_barrier(jnp.mean(values * values, axis=-1, keepdims=True)) + epsilon)

def causal_states(log_decay_factor, head_step_size, ssm_inputs, inject, start_state):
    cumulative = jnp.cumsum(log_decay_factor, axis=1)
    length = log_decay_factor.shape[1]
    lower = (jnp.arange(length)[:, None] >= jnp.arange(length)[None, :])[None, :, :, None]
    spread = cumulative[:, :, None, :] - cumulative[:, None, :, :]
    factors = jnp.where(lower, jnp.exp(jnp.where(lower, spread, 0.0)), 0.0)
    mixing = factors * head_step_size[:, None, :, :]
    carried = jnp.exp(cumulative)[..., None, None] * start_state[:, None]
    return carried + jnp.einsum('sjih,sihp,sihn->sjhpn', mixing, ssm_inputs, inject)

def combine_head_outputs(incoming_token_rows, gate_portion, unactivated_step, step_size_bias, log_decay_rate, direct_path_weight, convolution_tap_weight, convolution_history_rows, per_proposal_states, accepted, proposal_extra_decay, group_norm_scale):
    sequences, proposals, group_count, group_width = incoming_token_rows.shape
    head_count = step_size_bias.shape[0]
    head_dim = per_proposal_states.shape[3]
    state_size = per_proposal_states.shape[4]
    per_group = head_count // group_count
    group_inner = per_group * head_dim
    tap_count = convolution_tap_weight.shape[0]
    offsets = accepted[:, None] + jnp.arange(tap_count - 1, dtype=jnp.int32)[None, :]
    context = jnp.take_along_axis(convolution_history_rows, offsets[:, :, None, None], axis=1)
    convolution_span = jnp.concatenate([context, incoming_token_rows], axis=1)
    widened = convolution_span.astype(jnp.float32)
    convolved = jnp.zeros((sequences, proposals, group_count, group_width), jnp.float32)
    for conv_tap in range(tap_count):
        convolved = convolved + widened[:, conv_tap:conv_tap + proposals] * convolution_tap_weight[conv_tap].astype(jnp.float32)
    activated = jax.nn.silu(convolved)
    ssm_inputs = activated[..., :group_inner].reshape(sequences, proposals, head_count, head_dim)
    inject = jnp.repeat(activated[..., group_inner:group_inner + state_size], per_group, axis=2)
    readout = jnp.repeat(activated[..., group_inner + state_size:], per_group, axis=2)
    head_step_size = jax.nn.softplus(unactivated_step + step_size_bias)
    log_decay_factor = proposal_extra_decay - jnp.exp(log_decay_rate) * head_step_size
    chosen = (accepted - 1)[:, None, None, None, None]
    start_state = jnp.take_along_axis(per_proposal_states, chosen, axis=1)[:, 0]
    running_state_rows = causal_states(log_decay_factor, head_step_size, ssm_inputs, inject, start_state)
    response = jnp.einsum('sjhn,sjhpn->sjhp', readout, running_state_rows) + direct_path_weight[:, None] * ssm_inputs
    gate_raw = gate_portion.astype(jnp.float32).reshape(sequences, proposals, head_count, head_dim)
    gate_applied_output = (response * jax.nn.silu(gate_raw)).reshape(sequences, proposals, group_count, group_inner)
    scaled = gate_applied_output * rms_scale(gate_applied_output) * group_norm_scale.reshape(group_count, group_inner)
    flat_gated = scaled.astype(jnp.bfloat16).reshape(sequences, proposals, head_count * head_dim)
    return (flat_gated, running_state_rows, convolution_span)

def reference(tokens, input_norm_scale, head_input_matrix, output_gate_matrix, group_input_matrix, group_readout_matrix, step_size_matrix, step_size_bias, log_decay_rate, direct_path_weight, convolution_tap_weight, convolution_history_rows, per_proposal_states, accepted, proposal_extra_decay, group_norm_scale, output_projection_matrix):
    widened = tokens.astype(jnp.float32)
    normed = (widened * rms_scale(widened) * input_norm_scale).astype(jnp.bfloat16)
    flattened = normed.reshape(SEQS * PROP, D)

    def project(weight):
        return jnp.dot(flattened, weight, preferred_element_type=jnp.float32).astype(jnp.bfloat16)
    per_group = HEADS // GROUPS
    part_input = project(head_input_matrix).reshape(SEQS, PROP, GROUPS, per_group * HEAD_DIM)
    part_inject = project(group_input_matrix).reshape(SEQS, PROP, GROUPS, STATE)
    part_readout = project(group_readout_matrix).reshape(SEQS, PROP, GROUPS, STATE)
    gate_portion = project(output_gate_matrix).reshape(SEQS, PROP, HEADS * HEAD_DIM)
    unactivated_step = jnp.dot(flattened, step_size_matrix, preferred_element_type=jnp.float32).reshape(SEQS, PROP, HEADS)
    incoming_token_rows = jnp.concatenate([part_input, part_inject, part_readout], axis=-1)
    gate_applied_output, running_state_rows, convolution_span = combine_head_outputs(incoming_token_rows, gate_portion, unactivated_step, step_size_bias, log_decay_rate, direct_path_weight, convolution_tap_weight, convolution_history_rows, per_proposal_states, accepted, proposal_extra_decay, group_norm_scale)
    block_width = HEADS * HEAD_DIM // N_TP
    gathered = gate_applied_output.reshape(SEQS * PROP, HEADS * HEAD_DIM)
    total = jnp.zeros((SEQS * PROP, D), jnp.float32)
    for shard in range(N_TP):
        partial_sum = jnp.dot(gathered[:, shard * block_width:(shard + 1) * block_width], output_projection_matrix[shard * block_width:(shard + 1) * block_width], preferred_element_type=jnp.float32)
        total = total + lax.optimization_barrier(partial_sum.astype(jnp.bfloat16)).astype(jnp.float32)
    mixed = total.astype(jnp.bfloat16).reshape(SEQS, PROP, D)
    return (mixed, running_state_rows, convolution_span)
```

```python
import functools

import jax
import jax.numpy as jnp
from jax import lax
from jax.experimental import pallas as pl
from jax.experimental.pallas import tpu as pltpu
from jax.sharding import PartitionSpec as P

epsilon = 1e-06
F32 = jnp.float32
BF16 = jnp.bfloat16
ROWS = 8


def vmem(x):
    return pltpu.with_memory_space_constraint(x, pltpu.VMEM)


VMEM_SPEC = pl.BlockSpec(memory_space=pltpu.VMEM)
SMEM_SPEC = pl.BlockSpec(memory_space=pltpu.SMEM)
HBM_SPEC = pl.BlockSpec(memory_space=pl.ANY)


def call(body, outs, ins, specs, name, flops=0, scratch=(), out_specs=None, limit=20 << 20):
    return pl.pallas_call(
        body,
        out_shape=outs,
        in_specs=specs,
        out_specs=out_specs or [VMEM_SPEC] * len(outs),
        scratch_shapes=list(scratch),
        cost_estimate=pl.CostEstimate(flops=flops, transcendentals=0, bytes_accessed=0),
        compiler_params=pltpu.CompilerParams(vmem_limit_bytes=limit),
        name=name,
    )(*ins)


def exchange(blocks, axis, count):
    got = []
    for step in range(1, count):
        pairs = [(i, i ^ step) for i in range(count)]
        got.append(lax.ppermute(blocks[step], axis, pairs))
    return got


def silu(v):
    return v * jax.nn.sigmoid(v)


def split(v):
    high = v.astype(BF16)
    return high, (v - high.astype(F32)).astype(BF16)


def norm_body(count, tokens, scale, normed, *slices):
    me = lax.axis_index("kv")
    width = slices[0].shape[1]
    values = tokens[0].astype(F32)
    mean = jnp.mean(values * values, axis=-1, keepdims=True)
    normed[...] = (values * lax.rsqrt(mean + epsilon) * scale[...]).astype(BF16)
    for step in range(count):
        start = pl.multiple_of(lax.bitwise_xor(me, step) * width, 128)
        slices[step][...] = normed[:, pl.ds(start, width)]


def step_body(head_dim, normed, step_t, bias, rate, direct, extra, coef, small, table):
    props, heads = extra.shape
    raw = lax.dot_general(
        normed[...], step_t[...], (((1,), (1,)), ((), ())), preferred_element_type=F32
    )
    size = jax.nn.softplus(raw + bias[...])
    decay = extra[...] - jnp.exp(rate[...]) * size
    table[...] = jnp.zeros_like(table)
    small[...] = jnp.zeros_like(small)
    small[0:props, :] = jnp.exp(decay)
    total = []
    for j in range(props):
        row = decay[j : j + 1]
        total.append(row if j == 0 else total[-1] + row)
        table[j : j + 1, :] = jnp.exp(total[j])
    for i in range(props):
        own = size[i : i + 1]
        for j in range(i, props):
            at = (1 + i) * ROWS + j
            table[at : at + 1, :] = jnp.exp(total[j] - total[i]) * own
    at = (1 + props) * ROWS
    table[at : at + 1, :] = direct[...]
    width = coef.shape[-1]
    lane = lax.broadcasted_iota(jnp.int32, (heads, width), 1)
    head = lax.broadcasted_iota(jnp.int32, (heads, width), 0)
    spread = jnp.where(lane // head_dim == head, 1.0, 0.0).astype(F32)
    wide = jnp.dot(
        table[...], spread, preferred_element_type=F32, precision=lax.Precision.HIGHEST
    )
    for part in range(coef.shape[0]):
        coef[part] = wide[part * ROWS : (part + 1) * ROWS]


def state_body(accepted, states, history, taps, start, high, low, early, taps_wide, sem):
    count = accepted[0]
    copy = pltpu.make_async_copy(states.at[0, count - 1], start, sem)
    copy.start()
    heads, head_dim, size = start.shape
    groups = taps.shape[1]
    tap_count = taps.shape[0]
    inner = heads // groups * head_dim
    per = heads // groups

    def widen(rows, target, at):
        rows = rows.astype(F32)
        for g in range(groups):
            row = rows[g : g + 1]
            target[at : at + 1, g * inner : (g + 1) * inner] = row[:, :inner]
            for part in range(2):
                base = groups * inner + part * groups * size + g * size
                target[at : at + 1, base : base + size] = row[
                    :, inner + part * size : inner + (part + 1) * size
                ]

    taps_wide[...] = jnp.zeros_like(taps_wide)
    early[...] = jnp.zeros_like(early)
    for k in range(tap_count):
        widen(taps[k], taps_wide, k)
    for k in range(tap_count - 1):
        widen(history[0, count + k], early, k)
    context = early[...]
    before = tap_count - 1
    total = context * taps_wide[0:1, :]
    keep = lax.broadcasted_iota(jnp.int32, (ROWS, 1), 0) < before
    for k in range(1, before):
        total = total + jnp.where(keep, pltpu.roll(context, ROWS - k, 0), 0.0) * taps_wide[k : k + 1, :]
    early[...] = jnp.where(keep, total, 0.0)

    high[...] = jnp.zeros_like(high)
    low[...] = jnp.zeros_like(low)
    copy.wait()
    pair = 128 // head_dim
    for g in range(groups):
        for block in range(per // pair):
            at = g * per + block * pair
            tile = start[at : at + pair].reshape(pair * head_dim, size).T
            big, rest = split(tile)
            cols = slice(at * head_dim, (at + pair) * head_dim)
            high[g * size : (g + 1) * size, cols] = big
            low[g * size : (g + 1) * size, cols] = rest


def stack_rows(parts, lhs):
    lhs[...] = jnp.zeros_like(lhs)
    for j, part in enumerate(parts):
        lhs[4 * j : 4 * j + part.shape[0], :] = part[...].astype(F32)
    return lhs[...].astype(BF16)


def project_body(count, *refs):
    slices = refs[:count]
    weights = refs[count : count + 4]
    own = refs[count + 4]
    outs = refs[count + 5 : count + 4 + count]
    lhs = stack_rows(slices, refs[-1])
    at = 0
    for weight in weights:
        width = weight.shape[1]
        result = jnp.dot(lhs, weight[...], preferred_element_type=F32)
        own[:, at : at + width] = result[0:4]
        for j, out in enumerate(outs, 1):
            out[:, at : at + width] = result[4 * j : 4 * j + 4].astype(BF16)
        at += width


def mixer_body(props, groups, *refs):
    own, *rest = refs
    count = len(rest) - 11
    others = rest[:count]
    coef, early, taps, high, low, gain, gated, fresh, act, summed, norms = rest[count:]
    inner = gain.shape[1]
    conv = early.shape[1]
    per = inner // groups
    both = (conv - inner) // 2
    size = both // groups
    summed[...] = jnp.zeros_like(summed)
    total = own[...]
    for other in others:
        total = total + other[...].astype(F32)
    summed[0:props, :] = total[0:props].astype(BF16).astype(F32)
    rows = summed[:, :conv]
    fresh[...] = rows
    tap_count = 4
    value = early[...] + rows * taps[tap_count - 1 : tap_count, :]
    for k in range(1, props):
        value = value + pltpu.roll(rows * taps[tap_count - 1 - k : tap_count - k, :], k, 0)
    value = silu(value)
    act[...] = value
    x = value[:, :inner]
    b = value[:, inner : inner + both]
    c = value[:, inner + both :]
    c_high, c_low = split(c)
    left = jnp.concatenate([c_high.astype(F32), c_low.astype(F32)], axis=0).astype(BF16)
    carried = jnp.dot(left, high[...], preferred_element_type=F32)
    carried = carried[:ROWS] + carried[ROWS:]
    carried = carried + jnp.dot(c_high, low[...], preferred_element_type=F32)
    lane = lax.broadcasted_iota(jnp.int32, (ROWS, both), 1)
    response = coef[0] * carried + coef[1 + props, 0:1, :] * x
    pieces = []
    weights = []
    for i in range(props):
        product = c * b[i : i + 1]
        weights.append(
            [
                jnp.sum(jnp.where(lane // size == g, product, 0.0), axis=1, keepdims=True)
                for g in range(groups)
            ]
        )
    gate = summed[:, conv:]
    gate = silu(gate)
    for g in range(groups):
        at = slice(g * per, (g + 1) * per)
        part = response[:, at]
        for i in range(props):
            part = part + coef[1 + i, :, at] * weights[i][g] * x[i : i + 1, at]
        part = part * gate[:, at]
        mean = jnp.sum(part * part, axis=1, keepdims=True) * (1.0 / per)
        pieces.append(part * lax.rsqrt(mean + epsilon) * gain[:, at])
    norms[...] = jnp.concatenate(pieces, axis=1)
    gated[...] = norms[0:4].astype(BF16)


def tail_body(props, accepted, start, small, act, coef, fresh, history, states, tail, held, sem):
    heads, head_dim, size = start.shape
    groups = history.shape[2]
    per = heads // groups
    inner = per * head_dim
    wide = heads * head_dim
    count = accepted[0]
    before = tail.shape[1] - props
    for k in range(before):
        tail[0, k] = history[0, count + k]
    for j in range(props):
        rows = []
        for g in range(groups):
            row = [fresh[j : j + 1, g * inner : (g + 1) * inner]]
            for part in range(2):
                base = wide + part * groups * size + g * size
                row.append(fresh[j : j + 1, base : base + size])
            rows.append(jnp.concatenate(row, axis=1))
        tail[0, before + j] = jnp.concatenate(rows, axis=0).astype(BF16)
    x = act[:, :wide]
    row_at = lax.broadcasted_iota(jnp.int32, (ROWS, 1), 0)
    steps = jnp.zeros((ROWS, wide), F32)
    for j in range(props):
        steps = jnp.where(row_at == j, coef[1 + j], steps)
    dx = x * steps
    dx_high, dx_low = split(dx)
    dx_high, dx_low = dx_high.astype(F32), dx_low.astype(F32)
    left = jnp.concatenate(
        [dx_high, dx_low, dx_high, jnp.zeros_like(dx)], axis=0
    ).astype(BF16)
    b = act[:, wide : wide + groups * size]
    b_high, b_low = split(b)
    b_high, b_low = b_high.astype(F32), b_low.astype(F32)
    copies = []
    for g in range(groups):
        blocks = []
        for j in range(props):
            hi = jnp.where(row_at == j, b_high, 0.0)
            lo = jnp.where(row_at == j, b_low, 0.0)
            full = jnp.concatenate([hi, hi, lo, jnp.zeros_like(hi)], axis=0)
            if g:
                full = pltpu.roll(full, groups * size - g * size, 1)
            blocks.append(full)
        right = jnp.concatenate(blocks, axis=1).astype(BF16)
        update = lax.dot_general(
            left[:, g * inner : (g + 1) * inner],
            right,
            (((0,), (0,)), ((), ())),
            preferred_element_type=F32,
        )
        lanes = groups * size
        for h in range(per):
            at = g * per + h
            state = start[at]
            for j in range(props):
                new = update[h * head_dim : (h + 1) * head_dim, j * lanes : j * lanes + size]
                state = state * small[j : j + 1, at : at + 1] + new
                held[j, at] = state
        copy = pltpu.make_async_copy(
            held.at[:, pl.ds(g * per, per)], states.at[0, :, pl.ds(g * per, per)], sem.at[g]
        )
        copy.start()
        copies.append(copy)
    for copy in copies:
        copy.wait()


def output_body(count, *refs):
    parts = refs[:count]
    weight = refs[count]
    outs = refs[count + 1 : count + 1 + count]
    result, lhs = refs[-2:]
    which = lax.bitwise_xor(lax.axis_index("kv"), lax.axis_index("tp"))
    product = jnp.dot(stack_rows(parts, lhs), weight[...], preferred_element_type=F32)
    for j in range(count):
        result[j, 0:4] = product[4 * j : 4 * j + 4]
    for step in range(count):
        outs[step][...] = result[lax.bitwise_xor(which, step), 0:4].astype(BF16)


def final_body(*refs):
    *parts, out = refs
    total = parts[0][...].astype(F32)
    for part in parts[1:]:
        total = total + part[...].astype(F32)
    out[0] = total[0 : out.shape[1]].astype(BF16)


def fast_local(
    count,
    tokens,
    input_norm_scale,
    head_input_matrix,
    output_gate_matrix,
    group_input_matrix,
    group_readout_matrix,
    step_size_matrix,
    step_size_bias,
    log_decay_rate,
    direct_path_weight,
    convolution_tap_weight,
    convolution_history_rows,
    per_proposal_states,
    accepted,
    proposal_extra_decay,
    group_norm_scale,
    output_projection_matrix,
):
    _, props, width = tokens.shape
    heads = step_size_bias.shape[0]
    _, tail_rows, groups, channels = convolution_history_rows.shape
    head_dim, size = per_proposal_states.shape[3:]
    inner = heads * head_dim
    conv = groups * channels
    rows = head_input_matrix.shape[0]
    total = conv + inner
    out_cols = output_projection_matrix.shape[1]

    normed, *slices = call(
        functools.partial(norm_body, count),
        [pltpu.VMEM((props, width), BF16)] + [pltpu.VMEM((props, rows), BF16)] * count,
        [tokens, input_norm_scale.reshape(1, width)],
        [VMEM_SPEC] * 2,
        "norm",
    )
    received = exchange(slices, "kv", count)

    coef, small = call(
        functools.partial(step_body, head_dim),
        [pltpu.VMEM((props + 2, ROWS, inner), F32), pltpu.VMEM((ROWS, heads), F32)],
        [
            vmem(normed),
            vmem(step_size_matrix.T),
            step_size_bias.reshape(1, heads),
            log_decay_rate.reshape(1, heads),
            direct_path_weight.reshape(1, heads),
            proposal_extra_decay.reshape(props, heads),
        ],
        [VMEM_SPEC] * 6,
        "steps",
        flops=20_000_000,
        scratch=[pltpu.VMEM(((props + 2) * ROWS, heads), F32)],
    )
    start, high, low, early, taps = call(
        state_body,
        [
            pltpu.VMEM((heads, head_dim, size), F32),
            pltpu.VMEM((groups * size, inner), BF16),
            pltpu.VMEM((groups * size, inner), BF16),
            pltpu.VMEM((ROWS, conv), F32),
            pltpu.VMEM((ROWS, conv), F32),
        ],
        [accepted, per_proposal_states, convolution_history_rows, convolution_tap_weight],
        [SMEM_SPEC, HBM_SPEC, VMEM_SPEC, VMEM_SPEC],
        "start_state",
        flops=20_000_000,
        scratch=[pltpu.SemaphoreType.DMA],
    )

    own, *partials = call(
        functools.partial(project_body, count),
        [pltpu.VMEM((4, total), F32)] + [pltpu.VMEM((4, total), BF16)] * (count - 1),
        [vmem(s) for s in [slices[0]] + received]
        + [
            vmem(w)
            for w in (
                head_input_matrix,
                group_input_matrix,
                group_readout_matrix,
                output_gate_matrix,
            )
        ],
        [VMEM_SPEC] * (count + 4),
        "project",
        flops=200_000_000,
        scratch=[pltpu.VMEM((4 * count, rows), F32)],
    )
    sums = exchange([None] + partials, "kv", count)
    gated, fresh, act = call(
        functools.partial(mixer_body, props, groups),
        [
            pltpu.VMEM((4, inner), BF16),
            pltpu.VMEM((ROWS, conv), F32),
            pltpu.VMEM((ROWS, conv), F32),
        ],
        [vmem(v) for v in [own] + sums + [coef, early, taps, high, low]]
        + [vmem(group_norm_scale.reshape(1, inner))],
        [VMEM_SPEC] * (count + 6),
        "mixer",
        flops=20_000_000,
        scratch=[pltpu.VMEM((ROWS, total), F32), pltpu.VMEM((ROWS, inner), F32)],
    )
    gathered = exchange([gated] * count, "kv", count)
    new_states, new_tail = call(
        functools.partial(tail_body, props),
        [
            jax.ShapeDtypeStruct((1, props, heads, head_dim, size), F32),
            jax.ShapeDtypeStruct(convolution_history_rows.shape, BF16),
        ],
        [accepted]
        + [vmem(v) for v in (start, small, act, coef, fresh)]
        + [convolution_history_rows],
        [SMEM_SPEC] + [VMEM_SPEC] * 6,
        "states",
        flops=60_000_000,
        out_specs=[HBM_SPEC, VMEM_SPEC],
        scratch=[
            pltpu.VMEM((props, heads, head_dim, size), F32),
            pltpu.SemaphoreType.DMA((groups,)),
        ],
    )
    blocks = call(
        functools.partial(output_body, count),
        [pltpu.VMEM((4, out_cols), BF16)] * count,
        [vmem(v) for v in [gated] + gathered + [output_projection_matrix]],
        [VMEM_SPEC] * (count + 1),
        "output",
        flops=100_000_000,
        scratch=[
            pltpu.VMEM((count, ROWS, out_cols), F32),
            pltpu.VMEM((4 * count, inner), F32),
        ],
    )
    last = exchange(blocks, "tp", count)
    (mixed,) = call(
        final_body,
        [jax.ShapeDtypeStruct((1, props, out_cols), BF16)],
        [vmem(v) for v in [blocks[0]] + last],
        [VMEM_SPEC] * count,
        "final",
    )
    return (mixed, new_states, new_tail)


def rms_scale(values):
    return lax.rsqrt(jnp.mean(values * values, axis=-1, keepdims=True) + epsilon)


def causal_states(log_decay_factor, head_step_size, ssm_inputs, inject, start_state):
    cumulative = jnp.cumsum(log_decay_factor, axis=1)
    length = log_decay_factor.shape[1]
    lower = (jnp.arange(length)[:, None] >= jnp.arange(length)[None, :])[None, :, :, None]
    spread = cumulative[:, :, None, :] - cumulative[:, None, :, :]
    factors = jnp.where(lower, jnp.exp(jnp.where(lower, spread, 0.0)), 0.0)
    mixing = factors * head_step_size[:, None, :, :]
    carried = jnp.exp(cumulative)[..., None, None] * start_state[:, None]
    return carried + jnp.einsum("sjih,sihp,sihn->sjhpn", mixing, ssm_inputs, inject)


def combine_head_outputs(
    incoming_token_rows,
    gate_portion,
    unactivated_step,
    step_size_bias,
    log_decay_rate,
    direct_path_weight,
    convolution_tap_weight,
    convolution_history_rows,
    per_proposal_states,
    accepted,
    proposal_extra_decay,
    group_norm_scale,
):
    sequences, proposals, group_count, group_width = incoming_token_rows.shape
    head_count = step_size_bias.shape[0]
    head_dim = per_proposal_states.shape[3]
    state_size = per_proposal_states.shape[4]
    per_group = head_count // group_count
    group_inner = per_group * head_dim
    tap_count = convolution_tap_weight.shape[0]
    offsets = accepted[:, None] + jnp.arange(tap_count - 1, dtype=jnp.int32)[None, :]
    context = jnp.take_along_axis(convolution_history_rows, offsets[:, :, None, None], axis=1)
    convolution_span = jnp.concatenate([context, incoming_token_rows], axis=1)
    widened = convolution_span.astype(jnp.float32)
    convolved = jnp.zeros((sequences, proposals, group_count, group_width), jnp.float32)
    for conv_tap in range(tap_count):
        convolved = convolved + widened[
            :, conv_tap : conv_tap + proposals
        ] * convolution_tap_weight[conv_tap].astype(jnp.float32)
    activated = jax.nn.silu(convolved)
    ssm_inputs = activated[..., :group_inner].reshape(sequences, proposals, head_count, head_dim)
    inject = jnp.repeat(activated[..., group_inner : group_inner + state_size], per_group, axis=2)
    readout = jnp.repeat(activated[..., group_inner + state_size :], per_group, axis=2)
    head_step_size = jax.nn.softplus(unactivated_step + step_size_bias)
    log_decay_factor = proposal_extra_decay - jnp.exp(log_decay_rate) * head_step_size
    chosen = (accepted - 1)[:, None, None, None, None]
    start_state = jnp.take_along_axis(per_proposal_states, chosen, axis=1)[:, 0]
    running_state_rows = causal_states(
        log_decay_factor, head_step_size, ssm_inputs, inject, start_state
    )
    response = (
        jnp.einsum("sjhn,sjhpn->sjhp", readout, running_state_rows)
        + direct_path_weight[:, None] * ssm_inputs
    )
    gate_raw = gate_portion.astype(jnp.float32).reshape(sequences, proposals, head_count, head_dim)
    gate_applied_output = (response * jax.nn.silu(gate_raw)).reshape(
        sequences, proposals, group_count, group_inner
    )
    scaled = (
        gate_applied_output
        * rms_scale(gate_applied_output)
        * group_norm_scale.reshape(group_count, group_inner)
    )
    flat_gated = scaled.astype(jnp.bfloat16).reshape(sequences, proposals, head_count * head_dim)
    return (flat_gated, running_state_rows, convolution_span)


def local(
    tokens,
    input_norm_scale,
    head_input_matrix,
    output_gate_matrix,
    group_input_matrix,
    group_readout_matrix,
    step_size_matrix,
    step_size_bias,
    log_decay_rate,
    direct_path_weight,
    convolution_tap_weight,
    convolution_history_rows,
    per_proposal_states,
    accepted,
    proposal_extra_decay,
    group_norm_scale,
    output_projection_matrix,
):
    local_seqs, proposals, width = tokens.shape
    head_local = step_size_bias.shape[0]
    group_local = convolution_tap_weight.shape[1]
    head_dim = per_proposal_states.shape[3]
    state_size = per_proposal_states.shape[4]
    group_inner = head_local // group_local * head_dim
    widened = tokens.astype(jnp.float32)
    normed = (widened * rms_scale(widened) * input_norm_scale).astype(jnp.bfloat16)
    unactivated_step = jnp.einsum(
        "sjd,dh->sjh", normed, step_size_matrix, preferred_element_type=jnp.float32
    )
    pieces = lax.all_to_all(normed, "kv", split_axis=2, concat_axis=0, tiled=True)
    joined = jnp.concatenate(
        [head_input_matrix, group_input_matrix, group_readout_matrix, output_gate_matrix], axis=1
    )
    summed = lax.psum_scatter(
        jnp.einsum("sjd,dc->sjc", pieces, joined, preferred_element_type=jnp.float32),
        "kv",
        scatter_dimension=0,
        tiled=True,
    )
    projected = summed.astype(jnp.bfloat16)
    input_width = head_local * head_dim
    inject_width = group_local * state_size
    part_input = projected[..., :input_width].reshape(
        local_seqs, proposals, group_local, group_inner
    )
    part_inject = projected[..., input_width : input_width + inject_width].reshape(
        local_seqs, proposals, group_local, state_size
    )
    part_readout = projected[
        ..., input_width + inject_width : input_width + 2 * inject_width
    ].reshape(local_seqs, proposals, group_local, state_size)
    gate_portion = projected[..., input_width + 2 * inject_width :]
    incoming_token_rows = jnp.concatenate([part_input, part_inject, part_readout], axis=-1)
    gate_applied_output, running_state_rows, convolution_span = combine_head_outputs(
        incoming_token_rows,
        gate_portion,
        unactivated_step,
        step_size_bias,
        log_decay_rate,
        direct_path_weight,
        convolution_tap_weight,
        convolution_history_rows,
        per_proposal_states,
        accepted,
        proposal_extra_decay,
        group_norm_scale,
    )
    terms = jnp.einsum(
        "sjc,cd->sjd",
        lax.all_gather(gate_applied_output, "kv", axis=0, tiled=True),
        output_projection_matrix,
        preferred_element_type=jnp.float32,
    )
    mixed = lax.psum_scatter(terms.astype(jnp.bfloat16), "tp", scatter_dimension=0, tiled=True)
    return (mixed, running_state_rows, convolution_span)


def chosen(mesh, *arguments):
    tokens, matrix = arguments[0], arguments[2]
    kv, tp = mesh.shape["kv"], mesh.shape["tp"]
    slim = tokens.shape[:2] == (1, 3) and matrix.shape[0] % 128 == 0
    if slim and kv == tp and kv in (2, 4):
        return fast_local(kv, *arguments)
    return local(*arguments)


def solution(mesh):
    return jax.shard_map(
        functools.partial(chosen, mesh),
        mesh=mesh,
        in_specs=(
            P(("grp", "kv"), None, None),
            P(),
            P("kv", "tp"),
            P("kv", "tp"),
            P("kv", "tp"),
            P("kv", "tp"),
            P(None, "tp"),
            P("tp"),
            P("tp"),
            P("tp"),
            P(None, "tp", None),
            P(("grp", "kv"), None, "tp", None),
            P(("grp", "kv"), None, "tp", None, None),
            P(("grp", "kv")),
            P(("grp", "kv"), None, "tp"),
            P("tp"),
            P("tp", "kv"),
        ),
        out_specs=(
            P(("grp", "tp"), None, "kv"),
            P(("grp", "kv"), None, "tp", None, None),
            P(("grp", "kv"), None, "tp", None),
        ),
        check_vma=False,
    )
```

```python
import functools

import jax
import jax.numpy as jnp
from jax import lax
from jax.experimental import pallas as pl
from jax.experimental.pallas import tpu as pltpu
from jax.sharding import PartitionSpec as P


epsilon = 1e-06
F32 = jnp.float32
BF16 = jnp.bfloat16
ROWS = 8


def vmem(x):
    return pltpu.with_memory_space_constraint(x, pltpu.VMEM)


def hbm(x):
    return pltpu.with_memory_space_constraint(x, pltpu.HBM)


VMEM_SPEC = pl.BlockSpec(memory_space=pltpu.VMEM)
SMEM_SPEC = pl.BlockSpec(memory_space=pltpu.SMEM)
HBM_SPEC = pl.BlockSpec(memory_space=pl.ANY)


def call(body, outs, ins, specs, flops=0, scratch=(), out_specs=None, limit=20 << 20, moved=0, aliases={}):
    return pl.pallas_call(
        body,
        out_shape=outs,
        in_specs=specs,
        out_specs=out_specs or [VMEM_SPEC] * len(outs),
        scratch_shapes=list(scratch),
        input_output_aliases=aliases,
        cost_estimate=pl.CostEstimate(flops=flops, transcendentals=0, bytes_accessed=moved),
        compiler_params=pltpu.CompilerParams(vmem_limit_bytes=limit),
    )(*ins)


def exchange(blocks, axis, count):
    got = []
    for step in reversed(range(1, count)):
        pairs = [(i, i ^ step) for i in range(count)]
        got.append(lax.ppermute(blocks[step], axis, pairs))
    return got[::-1]


def silu(v):
    return v * jax.nn.sigmoid(v)


def split(v):
    high = v.astype(BF16)
    return high, (v - high.astype(F32)).astype(BF16)


def norm_body(count, tokens, scale, normed, *slices):
    me = lax.axis_index("kv")
    width = slices[0].shape[1]
    values = tokens[0].astype(F32)
    mean = jnp.mean(values * values, axis=-1, keepdims=True)
    normed[...] = (values * lax.rsqrt(mean + epsilon) * scale[...]).astype(BF16)
    for step in range(count):
        start = pl.multiple_of(lax.bitwise_xor(me, step) * width, 128)
        slices[step][...] = normed[:, pl.ds(start, width)]


def step_body(head_dim, accepted, normed, step_t, bias, rate, direct, extra, coef, small, table):
    props, heads = extra.shape
    raw = lax.dot_general(
        normed[...], step_t[...], (((1,), (1,)), ((), ())), preferred_element_type=F32
    )
    size = jax.nn.softplus(raw + bias[...])
    decay = extra[...] - jnp.exp(rate[...]) * size
    table[...] = jnp.zeros_like(table)
    small[...] = jnp.zeros_like(small)
    small[0:props, :] = jnp.exp(decay)
    total = []
    for j in range(props):
        row = decay[j : j + 1]
        total.append(row if j == 0 else total[-1] + row)
        table[j : j + 1, :] = jnp.exp(total[j])
    for i in range(props):
        own = size[i : i + 1]
        for j in range(i, props):
            at = (1 + i) * ROWS + j
            table[at : at + 1, :] = jnp.exp(total[j] - total[i]) * own
    at = (1 + props) * ROWS
    table[at : at + 1, :] = direct[...]
    width = coef.shape[-1]
    lane = lax.broadcasted_iota(jnp.int32, (heads, width), 1)
    head = lax.broadcasted_iota(jnp.int32, (heads, width), 0)
    spread = jnp.where(lane // head_dim == head, 1.0, 0.0).astype(F32)
    wide = jnp.dot(
        table[...], spread, preferred_element_type=F32, precision=lax.Precision.HIGHEST
    )
    for part in range(coef.shape[0]):
        coef[part] = wide[part * ROWS : (part + 1) * ROWS]


def state_body(accepted, states, history, taps, high, low, early, taps_wide):
    count = accepted[0]
    heads, head_dim, size = states.shape[2:]
    groups = taps.shape[1]
    tap_count = taps.shape[0]
    inner = heads // groups * head_dim
    per = heads // groups

    def widen(rows, target, at):
        rows = rows.astype(F32)
        for g in range(groups):
            row = rows[g : g + 1]
            target[at : at + 1, g * inner : (g + 1) * inner] = row[:, :inner]
            for part in range(2):
                base = groups * inner + part * groups * size + g * size
                target[at : at + 1, base : base + size] = row[
                    :, inner + part * size : inner + (part + 1) * size
                ]

    taps_wide[...] = jnp.zeros_like(taps_wide)
    early[...] = jnp.zeros_like(early)
    for k in range(tap_count):
        widen(taps[k], taps_wide, k)
    for k in range(tap_count - 1):
        widen(history[0, count + k], early, k)
    context = early[...]
    before = tap_count - 1
    total = context * taps_wide[0:1, :]
    keep = lax.broadcasted_iota(jnp.int32, (ROWS, 1), 0) < before
    for k in range(1, before):
        total = total + jnp.where(keep, pltpu.roll(context, ROWS - k, 0), 0.0) * taps_wide[k : k + 1, :]
    early[...] = jnp.where(keep, total, 0.0)

    high[...] = jnp.zeros_like(high)
    low[...] = jnp.zeros_like(low)
    pair = 128 // head_dim
    for g in range(groups):
        for block in range(per // pair):
            at = g * per + block * pair
            tile = states[0, count - 1, at : at + pair].reshape(pair * head_dim, size).T
            big, rest = split(tile)
            cols = slice(at * head_dim, (at + pair) * head_dim)
            high[g * size : (g + 1) * size, cols] = big
            low[g * size : (g + 1) * size, cols] = rest


def stack_rows(parts, lhs):
    lhs[...] = jnp.zeros_like(lhs)
    for j, part in enumerate(parts):
        lhs[4 * j : 4 * j + part.shape[0], :] = part[...].astype(F32)
    return lhs[...].astype(BF16)


def project_body(count, *refs):
    slices = refs[:count]
    weights = refs[count : count + 4]
    own = refs[count + 4]
    outs = refs[count + 5 : count + 4 + count]
    lhs = stack_rows(slices, refs[-1])
    at = 0
    for weight in weights:
        width = weight.shape[1]
        result = jnp.dot(lhs, weight[...], preferred_element_type=F32)
        own[:, at : at + width] = result[0:4]
        for j, out in enumerate(outs, 1):
            out[:, at : at + width] = result[4 * j : 4 * j + 4].astype(BF16)
        at += width


def mixer_body(props, groups, *refs):
    own, *rest = refs
    count = len(rest) - 11
    others = rest[:count]
    coef, early, taps, high, low, gain, gated, fresh, act, summed, norms = rest[count:]
    inner = gain.shape[1]
    conv = early.shape[1]
    per = inner // groups
    both = (conv - inner) // 2
    size = both // groups
    summed[...] = jnp.zeros_like(summed)
    total = own[...]
    for other in others:
        total = total + other[...].astype(F32)
    summed[0:props, :] = total[0:props].astype(BF16).astype(F32)
    rows = summed[:, :conv]
    fresh[...] = rows
    tap_count = 4
    value = early[...] + rows * taps[tap_count - 1 : tap_count, :]
    for k in range(1, props):
        value = value + pltpu.roll(rows * taps[tap_count - 1 - k : tap_count - k, :], k, 0)
    value = silu(value)
    act[...] = value
    x = value[:, :inner]
    b = value[:, inner : inner + both]
    c = value[:, inner + both :]
    c_high, c_low = split(c)
    left = jnp.concatenate([c_high.astype(F32), c_low.astype(F32)], axis=0).astype(BF16)
    carried = jnp.dot(left, high[...], preferred_element_type=F32)
    carried = carried[:ROWS] + carried[ROWS:]
    carried = carried + jnp.dot(c_high, low[...], preferred_element_type=F32)
    lane = lax.broadcasted_iota(jnp.int32, (ROWS, both), 1)
    response = coef[0] * carried + coef[1 + props, 0:1, :] * x
    pieces = []
    weights = []
    for i in range(props):
        product = c * b[i : i + 1]
        weights.append(
            [
                jnp.sum(jnp.where(lane // size == g, product, 0.0), axis=1, keepdims=True)
                for g in range(groups)
            ]
        )
    gate = summed[:, conv:]
    gate = silu(gate)
    for g in range(groups):
        at = slice(g * per, (g + 1) * per)
        part = response[:, at]
        for i in range(props):
            part = part + coef[1 + i, :, at] * weights[i][g] * x[i : i + 1, at]
        part = part * gate[:, at]
        mean = jnp.sum(part * part, axis=1, keepdims=True) * (1.0 / per)
        pieces.append(part * lax.rsqrt(mean + epsilon) * gain[:, at])
    norms[...] = jnp.concatenate(pieces, axis=1)
    gated[...] = norms[0:4].astype(BF16)


def states_body(props, g, accepted, start, small, act, coef, fresh, history, *refs):
    if g == 0:
        states, tail, flag, held, sem = refs
        flag[...] = jnp.zeros_like(flag)
    else:
        _, states, held, sem = refs
    heads, head_dim, size = start.shape[2:]
    groups = history.shape[2]
    per = heads // groups
    inner = per * head_dim
    wide = heads * head_dim
    count = accepted[0]
    lanes = slice(g * inner, (g + 1) * inner)
    row_at = lax.broadcasted_iota(jnp.int32, (ROWS, 1), 0)
    steps = jnp.zeros((ROWS, inner), F32)
    for j in range(props):
        steps = jnp.where(row_at == j, coef[1 + j, :, lanes], steps)
    dx = act[:, lanes] * steps
    dx_high, dx_low = split(dx)
    dx_high, dx_low = dx_high.astype(F32), dx_low.astype(F32)
    left = jnp.concatenate(
        [dx_high, dx_low, dx_high, jnp.zeros_like(dx)], axis=0
    ).astype(BF16)
    b_high, b_low = split(act[:, wide : wide + groups * size])
    b_high, b_low = b_high.astype(F32), b_low.astype(F32)
    blocks = []
    for j in range(props):
        hi = jnp.where(row_at == j, b_high, 0.0)
        lo = jnp.where(row_at == j, b_low, 0.0)
        full = jnp.concatenate([hi, hi, lo, jnp.zeros_like(hi)], axis=0)
        if g:
            full = pltpu.roll(full, groups * size - g * size, 1)
        blocks.append(full)
    right = jnp.concatenate(blocks, axis=1).astype(BF16)
    update = lax.dot_general(
        left, right, (((0,), (0,)), ((), ())), preferred_element_type=F32
    )
    block = groups * size
    copies = []
    half = per // 2
    for h in range(per):
        at = g * per + h
        state = start[0, count - 1, at]
        for j in range(props):
            new = update[h * head_dim : (h + 1) * head_dim, j * block : j * block + size]
            state = state * small[j : j + 1, at : at + 1] + new
            held[j, h] = state
        if (h + 1) % half == 0:
            first = h + 1 - half
            copy = pltpu.make_async_copy(
                held.at[:, pl.ds(first, half)],
                states.at[0, :, pl.ds(g * per + first, half)],
                sem.at[len(copies)],
            )
            copy.start()
            copies.append(copy)
    if g == 0:
        before = tail.shape[1] - props
        for k in range(before):
            tail[0, k] = history[0, count + k]
        for j in range(props):
            rows = []
            for q in range(groups):
                row = [fresh[j : j + 1, q * inner : (q + 1) * inner]]
                for part in range(2):
                    base = wide + part * groups * size + q * size
                    row.append(fresh[j : j + 1, base : base + size])
                rows.append(jnp.concatenate(row, axis=1))
            tail[0, before + j] = jnp.concatenate(rows, axis=0).astype(BF16)
    for copy in copies:
        copy.wait()


def output_body(count, *refs):
    parts = refs[:count]
    weight = refs[count]
    outs = refs[count + 2 : count + 2 + count]
    result, lhs = refs[-2:]
    which = lax.bitwise_xor(lax.axis_index("kv"), lax.axis_index("tp"))
    product = jnp.dot(stack_rows(parts, lhs), weight[...], preferred_element_type=F32)
    for j in range(count):
        result[j, 0:4] = product[4 * j : 4 * j + 4]
    for step in range(count):
        outs[step][...] = result[lax.bitwise_xor(which, step), 0:4].astype(BF16)


def final_body(*refs):
    *parts, out = refs
    total = parts[0][...].astype(F32)
    for part in parts[1:]:
        total = total + part[...].astype(F32)
    out[0] = total[0 : out.shape[1]].astype(BF16)


def fast_local(
    count,
    tokens,
    input_norm_scale,
    head_input_matrix,
    output_gate_matrix,
    group_input_matrix,
    group_readout_matrix,
    step_size_matrix,
    step_size_bias,
    log_decay_rate,
    direct_path_weight,
    convolution_tap_weight,
    convolution_history_rows,
    per_proposal_states,
    accepted,
    proposal_extra_decay,
    group_norm_scale,
    output_projection_matrix,
):
    _, props, width = tokens.shape
    heads = step_size_bias.shape[0]
    _, _, groups, channels = convolution_history_rows.shape
    head_dim, size = per_proposal_states.shape[3:]
    inner = heads * head_dim
    conv = groups * channels
    rows = head_input_matrix.shape[0]
    total = conv + inner
    out_cols = output_projection_matrix.shape[1]

    normed, *slices = call(
        functools.partial(norm_body, count),
        [pltpu.VMEM((props, width), BF16)] + [pltpu.VMEM((props, rows), BF16)] * count,
        [hbm(tokens), hbm(input_norm_scale.reshape(1, width))],
        [VMEM_SPEC] * 2,
        flops=1_000_000_000_000, moved=10_000_000_000,
    )
    received = exchange(slices, "kv", count)
    matrices = [head_input_matrix, group_input_matrix, group_readout_matrix, output_gate_matrix]

    coef, small = call(
        functools.partial(step_body, head_dim),
        [pltpu.VMEM((props + 2, ROWS, inner), F32), pltpu.VMEM((ROWS, heads), F32)],
        [
            accepted,
            vmem(normed),
            vmem(step_size_matrix.T),
            step_size_bias.reshape(1, heads),
            log_decay_rate.reshape(1, heads),
            direct_path_weight.reshape(1, heads),
            proposal_extra_decay.reshape(props, heads),
        ],
        [SMEM_SPEC] + [VMEM_SPEC] * 6,
        flops=20_000_000,
        scratch=[pltpu.VMEM(((props + 2) * ROWS, heads), F32)],
    )
    states = vmem(per_proposal_states)
    high, low, early, taps = call(
        state_body,
        [
            pltpu.VMEM((groups * size, inner), BF16),
            pltpu.VMEM((groups * size, inner), BF16),
            pltpu.VMEM((ROWS, conv), F32),
            pltpu.VMEM((ROWS, conv), F32),
        ],
        [accepted, states, convolution_history_rows, convolution_tap_weight],
        [SMEM_SPEC] + [VMEM_SPEC] * 3,
        flops=20_000_000,
    )

    own, *partials = call(
        functools.partial(project_body, count),
        [pltpu.VMEM((4, total), F32)] + [pltpu.VMEM((4, total), BF16)] * (count - 1),
        [vmem(s) for s in [slices[0]] + received]
        + matrices,
        [VMEM_SPEC] * (count + 4),
        flops=200_000_000,
        scratch=[pltpu.VMEM((4 * count, rows), F32)],
    )
    sums = exchange([None] + partials, "kv", count)
    gated, fresh, act = call(
        functools.partial(mixer_body, props, groups),
        [
            pltpu.VMEM((4, inner), BF16),
            pltpu.VMEM((ROWS, conv), F32),
            pltpu.VMEM((ROWS, conv), F32),
        ],
        [vmem(v) for v in [own] + sums + [coef, early, taps, high, low]]
        + [vmem(group_norm_scale.reshape(1, inner))],
        [VMEM_SPEC] * (count + 6),
        flops=20_000_000,
        scratch=[pltpu.VMEM((ROWS, total), F32), pltpu.VMEM((ROWS, inner), F32)],
    )
    gathered = exchange([gated] * count, "kv", count)
    new_states = None
    for g in range(groups):
        shape = jax.ShapeDtypeStruct((1, props, heads, head_dim, size), F32)
        outs = [shape]
        if g == 0:
            outs += [
                jax.ShapeDtypeStruct(convolution_history_rows.shape, BF16),
                pltpu.VMEM((ROWS, 128), F32),
            ]
        result = call(
            functools.partial(states_body, props, g),
            outs,
            [accepted, states]
            + [vmem(v) for v in (small, act, coef, fresh, convolution_history_rows)]
            + ([hbm(new_states)] if g else []),
            [SMEM_SPEC] + [VMEM_SPEC] * 6 + ([HBM_SPEC] if g else []),
            flops=30_000_000,
            out_specs=[HBM_SPEC] + [VMEM_SPEC] * (len(outs) - 1),
            scratch=[
                pltpu.VMEM((props, heads // groups, head_dim, size), F32),
                pltpu.SemaphoreType.DMA((2,)),
            ],
            aliases={7: 0} if g else {},
        )
        new_states = result[0]
        if g == 0:
            new_tail, flag = result[1:]
    blocks = call(
        functools.partial(output_body, count),
        [pltpu.VMEM((4, out_cols), BF16)] * count,
        [vmem(v) for v in [gated] + gathered + [output_projection_matrix, flag]],
        [VMEM_SPEC] * (count + 2),
        flops=100_000_000,
        scratch=[
            pltpu.VMEM((count, ROWS, out_cols), F32),
            pltpu.VMEM((4 * count, inner), F32),
        ],
    )
    last = exchange(blocks, "tp", count)
    (mixed,) = call(
        final_body,
        [jax.ShapeDtypeStruct((1, props, out_cols), BF16)],
        [vmem(v) for v in [blocks[0]] + last],
        [VMEM_SPEC] * count,
    )
    return (mixed, new_states, new_tail)


def rms_scale(values):
    return lax.rsqrt(jnp.mean(values * values, axis=-1, keepdims=True) + epsilon)


def causal_states(log_decay_factor, head_step_size, ssm_inputs, inject, start_state):
    cumulative = jnp.cumsum(log_decay_factor, axis=1)
    length = log_decay_factor.shape[1]
    lower = (jnp.arange(length)[:, None] >= jnp.arange(length)[None, :])[None, :, :, None]
    spread = cumulative[:, :, None, :] - cumulative[:, None, :, :]
    factors = jnp.where(lower, jnp.exp(jnp.where(lower, spread, 0.0)), 0.0)
    mixing = factors * head_step_size[:, None, :, :]
    carried = jnp.exp(cumulative)[..., None, None] * start_state[:, None]
    return carried + jnp.einsum("sjih,sihp,sihn->sjhpn", mixing, ssm_inputs, inject)


def combine_head_outputs(
    incoming_token_rows,
    gate_portion,
    unactivated_step,
    step_size_bias,
    log_decay_rate,
    direct_path_weight,
    convolution_tap_weight,
    convolution_history_rows,
    per_proposal_states,
    accepted,
    proposal_extra_decay,
    group_norm_scale,
):
    sequences, proposals, group_count, group_width = incoming_token_rows.shape
    head_count = step_size_bias.shape[0]
    head_dim = per_proposal_states.shape[3]
    state_size = per_proposal_states.shape[4]
    per_group = head_count // group_count
    group_inner = per_group * head_dim
    tap_count = convolution_tap_weight.shape[0]
    offsets = accepted[:, None] + jnp.arange(tap_count - 1, dtype=jnp.int32)[None, :]
    context = jnp.take_along_axis(convolution_history_rows, offsets[:, :, None, None], axis=1)
    convolution_span = jnp.concatenate([context, incoming_token_rows], axis=1)
    widened = convolution_span.astype(jnp.float32)
    convolved = jnp.zeros((sequences, proposals, group_count, group_width), jnp.float32)
    for conv_tap in range(tap_count):
        convolved = convolved + widened[
            :, conv_tap : conv_tap + proposals
        ] * convolution_tap_weight[conv_tap].astype(jnp.float32)
    activated = jax.nn.silu(convolved)
    ssm_inputs = activated[..., :group_inner].reshape(sequences, proposals, head_count, head_dim)
    inject = jnp.repeat(activated[..., group_inner : group_inner + state_size], per_group, axis=2)
    readout = jnp.repeat(activated[..., group_inner + state_size :], per_group, axis=2)
    head_step_size = jax.nn.softplus(unactivated_step + step_size_bias)
    log_decay_factor = proposal_extra_decay - jnp.exp(log_decay_rate) * head_step_size
    chosen = (accepted - 1)[:, None, None, None, None]
    start_state = jnp.take_along_axis(per_proposal_states, chosen, axis=1)[:, 0]
    running_state_rows = causal_states(
        log_decay_factor, head_step_size, ssm_inputs, inject, start_state
    )
    response = (
        jnp.einsum("sjhn,sjhpn->sjhp", readout, running_state_rows)
        + direct_path_weight[:, None] * ssm_inputs
    )
    gate_raw = gate_portion.astype(jnp.float32).reshape(sequences, proposals, head_count, head_dim)
    gate_applied_output = (response * jax.nn.silu(gate_raw)).reshape(
        sequences, proposals, group_count, group_inner
    )
    scaled = (
        gate_applied_output
        * rms_scale(gate_applied_output)
        * group_norm_scale.reshape(group_count, group_inner)
    )
    flat_gated = scaled.astype(jnp.bfloat16).reshape(sequences, proposals, head_count * head_dim)
    return (flat_gated, running_state_rows, convolution_span)


def local(
    tokens,
    input_norm_scale,
    head_input_matrix,
    output_gate_matrix,
    group_input_matrix,
    group_readout_matrix,
    step_size_matrix,
    step_size_bias,
    log_decay_rate,
    direct_path_weight,
    convolution_tap_weight,
    convolution_history_rows,
    per_proposal_states,
    accepted,
    proposal_extra_decay,
    group_norm_scale,
    output_projection_matrix,
):
    local_seqs, proposals, _ = tokens.shape
    head_local = step_size_bias.shape[0]
    group_local = convolution_tap_weight.shape[1]
    head_dim = per_proposal_states.shape[3]
    state_size = per_proposal_states.shape[4]
    group_inner = head_local // group_local * head_dim
    widened = tokens.astype(jnp.float32)
    normed = (widened * rms_scale(widened) * input_norm_scale).astype(jnp.bfloat16)
    unactivated_step = jnp.einsum(
        "sjd,dh->sjh", normed, step_size_matrix, preferred_element_type=jnp.float32
    )
    pieces = lax.all_to_all(normed, "kv", split_axis=2, concat_axis=0, tiled=True)
    joined = jnp.concatenate(
        [head_input_matrix, group_input_matrix, group_readout_matrix, output_gate_matrix], axis=1
    )
    summed = lax.psum_scatter(
        jnp.einsum("sjd,dc->sjc", pieces, joined, preferred_element_type=jnp.float32),
        "kv",
        scatter_dimension=0,
        tiled=True,
    )
    projected = summed.astype(jnp.bfloat16)
    input_width = head_local * head_dim
    inject_width = group_local * state_size
    part_input = projected[..., :input_width].reshape(
        local_seqs, proposals, group_local, group_inner
    )
    part_inject = projected[..., input_width : input_width + inject_width].reshape(
        local_seqs, proposals, group_local, state_size
    )
    part_readout = projected[
        ..., input_width + inject_width : input_width + 2 * inject_width
    ].reshape(local_seqs, proposals, group_local, state_size)
    gate_portion = projected[..., input_width + 2 * inject_width :]
    incoming_token_rows = jnp.concatenate([part_input, part_inject, part_readout], axis=-1)
    gate_applied_output, running_state_rows, convolution_span = combine_head_outputs(
        incoming_token_rows,
        gate_portion,
        unactivated_step,
        step_size_bias,
        log_decay_rate,
        direct_path_weight,
        convolution_tap_weight,
        convolution_history_rows,
        per_proposal_states,
        accepted,
        proposal_extra_decay,
        group_norm_scale,
    )
    terms = jnp.einsum(
        "sjc,cd->sjd",
        lax.all_gather(gate_applied_output, "kv", axis=0, tiled=True),
        output_projection_matrix,
        preferred_element_type=jnp.float32,
    )
    mixed = lax.psum_scatter(terms.astype(jnp.bfloat16), "tp", scatter_dimension=0, tiled=True)
    return (mixed, running_state_rows, convolution_span)


def chosen(mesh, *arguments):
    tokens, matrix = arguments[0], arguments[2]
    kv, tp = mesh.shape["kv"], mesh.shape["tp"]
    slim = tokens.shape[:2] == (1, 3) and matrix.shape[0] % 128 == 0
    if slim and kv == tp and kv in (2, 4):
        return fast_local(kv, *arguments)
    return local(*arguments)


def solution(mesh):
    return jax.shard_map(
        functools.partial(chosen, mesh),
        mesh=mesh,
        in_specs=(
            P(("grp", "kv"), None, None),
            P(),
            P("kv", "tp"),
            P("kv", "tp"),
            P("kv", "tp"),
            P("kv", "tp"),
            P(None, "tp"),
            P("tp"),
            P("tp"),
            P("tp"),
            P(None, "tp", None),
            P(("grp", "kv"), None, "tp", None),
            P(("grp", "kv"), None, "tp", None, None),
            P(("grp", "kv")),
            P(("grp", "kv"), None, "tp"),
            P("tp"),
            P("tp", "kv"),
        ),
        out_specs=(
            P(("grp", "tp"), None, "kv"),
            P(("grp", "kv"), None, "tp", None, None),
            P(("grp", "kv"), None, "tp", None),
        ),
        check_vma=False,
    )
```

```python
import functools

import jax
import jax.numpy as jnp
from jax import lax
from jax.experimental import pallas as pl
from jax.experimental.pallas import tpu as pltpu
from jax.sharding import PartitionSpec as P


epsilon = 1e-06
F32 = jnp.float32
BF16 = jnp.bfloat16
ROWS = 8


def vmem(x):
    return pltpu.with_memory_space_constraint(x, pltpu.VMEM)


def hbm(x):
    return pltpu.with_memory_space_constraint(x, pltpu.HBM)


VMEM_SPEC = pl.BlockSpec(memory_space=pltpu.VMEM)
SMEM_SPEC = pl.BlockSpec(memory_space=pltpu.SMEM)
HBM_SPEC = pl.BlockSpec(memory_space=pl.ANY)


def call(body, outs, ins, specs, flops=0, scratch=(), out_specs=None, limit=20 << 20, moved=0, aliases={}):
    return pl.pallas_call(
        body,
        out_shape=outs,
        in_specs=specs,
        out_specs=out_specs or [VMEM_SPEC] * len(outs),
        scratch_shapes=list(scratch),
        input_output_aliases=aliases,
        cost_estimate=pl.CostEstimate(flops=flops, transcendentals=0, bytes_accessed=moved),
        compiler_params=pltpu.CompilerParams(vmem_limit_bytes=limit),
    )(*ins)


def exchange(blocks, axis, count):
    got = []
    for step in reversed(range(1, count)):
        pairs = [(i, i ^ step) for i in range(count)]
        got.append(lax.ppermute(blocks[step], axis, pairs))
    return got[::-1]


def silu(v):
    return v * jax.nn.sigmoid(v)


def split(v):
    high = v.astype(BF16)
    return high, (v - high.astype(F32)).astype(BF16)


def slice_body(count, tokens, *refs):
    slices, sem = refs[:count], refs[-1]
    me = lax.axis_index("kv")
    width = slices[0].shape[1]
    copies = []
    for step in reversed(range(count)):
        start = pl.multiple_of(lax.bitwise_xor(me, step) * width, 128)
        copy = pltpu.make_async_copy(
            tokens.at[0, :, pl.ds(start, width)], slices[step], sem.at[step]
        )
        copy.start()
        copies.append(copy)
    for copy in copies:
        copy.wait()


def step_body(head_dim, accepted, tokens, scale, step_t, bias, rate, direct, extra, coef, small, norm, table):
    props, heads = extra.shape
    values = tokens[0].astype(F32)
    norm_rows = lax.rsqrt(jnp.mean(values * values, axis=-1, keepdims=True) + epsilon)
    norm[...] = jnp.ones_like(norm)
    norm[0:props, :] = jnp.broadcast_to(norm_rows, (props, norm.shape[1]))
    normed = (values * norm_rows * scale[...]).astype(BF16)
    raw = lax.dot_general(
        normed, step_t[...], (((1,), (1,)), ((), ())), preferred_element_type=F32
    )
    size = jax.nn.softplus(raw + bias[...])
    decay = extra[...] - jnp.exp(rate[...]) * size
    table[...] = jnp.zeros_like(table)
    small[...] = jnp.zeros_like(small)
    small[0:props, :] = jnp.exp(decay)
    total = []
    for j in range(props):
        row = decay[j : j + 1]
        total.append(row if j == 0 else total[-1] + row)
        table[j : j + 1, :] = jnp.exp(total[j])
    for i in range(props):
        own = size[i : i + 1]
        for j in range(i, props):
            at = (1 + i) * ROWS + j
            table[at : at + 1, :] = jnp.exp(total[j] - total[i]) * own
    at = (1 + props) * ROWS
    table[at : at + 1, :] = direct[...]
    width = coef.shape[-1]
    lane = lax.broadcasted_iota(jnp.int32, (heads, width), 1)
    head = lax.broadcasted_iota(jnp.int32, (heads, width), 0)
    spread = jnp.where(lane // head_dim == head, 1.0, 0.0).astype(F32)
    wide = jnp.dot(
        table[...], spread, preferred_element_type=F32, precision=lax.Precision.HIGHEST
    )
    for part in range(coef.shape[0]):
        coef[part] = wide[part * ROWS : (part + 1) * ROWS]


def state_body(accepted, states, history, taps, high, low, early, taps_wide):
    count = accepted[0]
    heads, head_dim, size = states.shape[2:]
    groups = taps.shape[1]
    tap_count = taps.shape[0]
    inner = heads // groups * head_dim
    per = heads // groups

    def widen(rows, target, at):
        rows = rows.astype(F32)
        for g in range(groups):
            row = rows[g : g + 1]
            target[at : at + 1, g * inner : (g + 1) * inner] = row[:, :inner]
            for part in range(2):
                base = groups * inner + part * groups * size + g * size
                target[at : at + 1, base : base + size] = row[
                    :, inner + part * size : inner + (part + 1) * size
                ]

    taps_wide[...] = jnp.zeros_like(taps_wide)
    early[...] = jnp.zeros_like(early)
    for k in range(tap_count):
        widen(taps[k], taps_wide, k)
    for k in range(tap_count - 1):
        widen(history[0, count + k], early, k)
    context = early[...]
    before = tap_count - 1
    total = context * taps_wide[0:1, :]
    keep = lax.broadcasted_iota(jnp.int32, (ROWS, 1), 0) < before
    for k in range(1, before):
        total = total + jnp.where(keep, pltpu.roll(context, ROWS - k, 0), 0.0) * taps_wide[k : k + 1, :]
    early[...] = jnp.where(keep, total, 0.0)

    high[...] = jnp.zeros_like(high)
    low[...] = jnp.zeros_like(low)
    pair = 128 // head_dim
    for g in range(groups):
        for block in range(per // pair):
            at = g * per + block * pair
            tile = states[0, count - 1, at : at + pair].reshape(pair * head_dim, size).T
            big, rest = split(tile)
            cols = slice(at * head_dim, (at + pair) * head_dim)
            high[g * size : (g + 1) * size, cols] = big
            low[g * size : (g + 1) * size, cols] = rest


def stack_rows(parts, lhs):
    lhs[...] = jnp.zeros_like(lhs)
    for j, part in enumerate(parts):
        lhs[4 * j : 4 * j + part.shape[0], :] = part[...].astype(F32)
    return lhs[...].astype(BF16)


def packed_width(props, width):
    return -(-props * width // 4 // 128) * 128


def project_body(count, props, *refs):
    slices = refs[:count]
    inputs, inject, readout, gates, scale = refs[count : count + 5]
    own = refs[count + 5]
    outs = refs[count + 6 : count + 5 + count]
    stage, rows = refs[-2:]
    depth = rows.shape[1]
    start = pl.multiple_of(lax.axis_index("kv") * depth, 128)
    stack_rows(slices, rows)
    lhs = (rows[...] * scale[:, pl.ds(start, depth)]).astype(BF16)
    wide = stage.shape[1]
    first = inputs.shape[1]
    both = inject.shape[1] + readout.shape[1]
    left = wide - first - both
    rest = gates.shape[1] - left

    result = jnp.dot(lhs, gates[...], preferred_element_type=F32)
    stage[:, first + both :] = result[:, :left]
    extra = result[:, left:]
    result = jnp.dot(lhs, inputs[...], preferred_element_type=F32)
    stage[:, :first] = result
    pair = jnp.concatenate([inject[...], readout[...]], axis=1)
    stage[:, first : first + both] = jnp.dot(lhs, pair, preferred_element_type=F32)
    for j in range(count):
        for r in range(props):
            at = 4 * j + r
            stage[4 * j + 3 : 4 * j + 4, r * rest : (r + 1) * rest] = extra[at : at + 1]
    own[...] = stage[0:4, :]
    for j, out in enumerate(outs, 1):
        out[...] = stage[4 * j : 4 * j + 4, :].astype(BF16)


def mixer_body(props, groups, *refs):
    own, *rest = refs
    count = len(rest) - 12
    others = rest[:count]
    norm, coef, early, taps, high, low, gain, gated, fresh, act, summed, norms = rest[count:]
    inner = gain.shape[1]
    conv = early.shape[1]
    per = inner // groups
    both = (conv - inner) // 2
    size = both // groups
    summed[...] = jnp.zeros_like(summed)
    total = own[...]
    for other in others:
        total = total + other[...].astype(F32)
    wide = total.shape[1]
    rest = summed.shape[1] - wide
    summed[0:props, :wide] = total[0:props]
    for r in range(props):
        summed[r : r + 1, wide:] = total[3:4, r * rest : (r + 1) * rest]
    summed[...] = (summed[...] * norm[:, 0:1]).astype(BF16).astype(F32)
    rows = summed[:, :conv]
    fresh[...] = rows
    tap_count = 4
    value = early[...] + rows * taps[tap_count - 1 : tap_count, :]
    for k in range(1, props):
        value = value + pltpu.roll(rows * taps[tap_count - 1 - k : tap_count - k, :], k, 0)
    value = silu(value)
    act[...] = value
    x = value[:, :inner]
    b = value[:, inner : inner + both]
    c = value[:, inner + both :]
    c_high, c_low = split(c)
    left = jnp.concatenate([c_high.astype(F32), c_low.astype(F32)], axis=0).astype(BF16)
    carried = jnp.dot(left, high[...], preferred_element_type=F32)
    carried = carried[:ROWS] + carried[ROWS:]
    carried = carried + jnp.dot(c_high, low[...], preferred_element_type=F32)
    lane = lax.broadcasted_iota(jnp.int32, (ROWS, both), 1)
    response = coef[0] * carried + coef[1 + props, 0:1, :] * x
    pieces = []
    weights = []
    for i in range(props):
        product = c * b[i : i + 1]
        weights.append(
            [
                jnp.sum(jnp.where(lane // size == g, product, 0.0), axis=1, keepdims=True)
                for g in range(groups)
            ]
        )
    gate = summed[:, conv:]
    gate = silu(gate)
    for g in range(groups):
        at = slice(g * per, (g + 1) * per)
        part = response[:, at]
        for i in range(props):
            part = part + coef[1 + i, :, at] * weights[i][g] * x[i : i + 1, at]
        part = part * gate[:, at]
        mean = jnp.sum(part * part, axis=1, keepdims=True) * (1.0 / per)
        pieces.append(part * lax.rsqrt(mean + epsilon) * gain[:, at])
    norms[...] = jnp.concatenate(pieces, axis=1)
    gated[...] = norms[0:4].astype(BF16)


def states_body(props, groups, pieces, accepted, start, small, act, coef, *refs):
    heads, head_dim, size = start.shape[2:]
    per = heads // groups
    last = pieces[-1][2] == per and pieces[-1][0] == groups - 1
    if last:
        fresh, history, _, states, tail, held, sem = refs
    else:
        states, flag, held, sem = refs
        flag[...] = jnp.zeros_like(flag)
    copies = []
    inner = per * head_dim
    wide = heads * head_dim
    block = groups * size
    count = accepted[0]
    row_at = lax.broadcasted_iota(jnp.int32, (ROWS, 1), 0)
    b_high, b_low = split(act[:, wide : wide + block])
    b_high, b_low = b_high.astype(F32), b_low.astype(F32)
    filled = 0
    for g, low, high in pieces:
        lanes = slice(g * inner + low * head_dim, g * inner + high * head_dim)
        steps = jnp.zeros((ROWS, (high - low) * head_dim), F32)
        for j in range(props):
            steps = jnp.where(row_at == j, coef[1 + j, :, lanes], steps)
        dx = act[:, lanes] * steps
        dx_high, dx_low = split(dx)
        dx_high, dx_low = dx_high.astype(F32), dx_low.astype(F32)
        left = jnp.concatenate(
            [dx_high, dx_low, dx_high, jnp.zeros_like(dx)], axis=0
        ).astype(BF16)
        blocks = []
        for j in range(props):
            hi = jnp.where(row_at == j, b_high, 0.0)
            lo = jnp.where(row_at == j, b_low, 0.0)
            full = jnp.concatenate([hi, hi, lo, jnp.zeros_like(hi)], axis=0)
            if g:
                full = pltpu.roll(full, block - g * size, 1)
            blocks.append(full)
        right = jnp.concatenate(blocks, axis=1).astype(BF16)
        update = lax.dot_general(
            left, right, (((0,), (0,)), ((), ())), preferred_element_type=F32
        )
        for h in range(high - low):
            at = g * per + low + h
            state = start[0, count - 1, at]
            for j in range(props):
                new = update[h * head_dim : (h + 1) * head_dim, j * block : j * block + size]
                state = state * small[j : j + 1, at : at + 1] + new
                held[j, filled + h] = state
        copy = pltpu.make_async_copy(
            held.at[:, pl.ds(filled, high - low)],
            states.at[0, :, pl.ds(g * per + low, high - low)],
            sem.at[len(copies)],
        )
        copy.start()
        copies.append(copy)
        filled += high - low
    if not last:
        for copy in copies:
            copy.wait()
        return
    before = tail.shape[1] - props
    for k in range(before):
        tail[0, k] = history[0, count + k]
    for j in range(props):
        rows = []
        for q in range(groups):
            row = [fresh[j : j + 1, q * inner : (q + 1) * inner]]
            for part in range(2):
                base = wide + part * block + q * size
                row.append(fresh[j : j + 1, base : base + size])
            rows.append(jnp.concatenate(row, axis=1))
        tail[0, before + j] = jnp.concatenate(rows, axis=0).astype(BF16)
    for copy in copies:
        copy.wait()


def output_body(count, *refs):
    parts = refs[:count]
    weight = refs[count]
    outs = refs[count + 2 : count + 2 + count]
    result, lhs = refs[-2:]
    which = lax.bitwise_xor(lax.axis_index("kv"), lax.axis_index("tp"))
    product = jnp.dot(stack_rows(parts, lhs), weight[...], preferred_element_type=F32)
    for j in range(count):
        result[j, 0:4] = product[4 * j : 4 * j + 4]
    for step in range(count):
        outs[step][...] = result[lax.bitwise_xor(which, step), 0:4].astype(BF16)


def final_body(*refs):
    *parts, out = refs
    total = parts[0][...].astype(F32)
    for part in parts[1:]:
        total = total + part[...].astype(F32)
    out[0] = total[0 : out.shape[1]].astype(BF16)


def fast_local(
    count,
    tokens,
    input_norm_scale,
    head_input_matrix,
    output_gate_matrix,
    group_input_matrix,
    group_readout_matrix,
    step_size_matrix,
    step_size_bias,
    log_decay_rate,
    direct_path_weight,
    convolution_tap_weight,
    convolution_history_rows,
    per_proposal_states,
    accepted,
    proposal_extra_decay,
    group_norm_scale,
    output_projection_matrix,
):
    _, props, width = tokens.shape
    heads = step_size_bias.shape[0]
    _, _, groups, channels = convolution_history_rows.shape
    head_dim, size = per_proposal_states.shape[3:]
    inner = heads * head_dim
    conv = groups * channels
    rows = head_input_matrix.shape[0]
    total = conv + inner
    packed = packed_width(props, total)
    out_cols = output_projection_matrix.shape[1]

    slices = call(
        functools.partial(slice_body, count),
        [pltpu.VMEM((props, rows), BF16)] * count,
        [hbm(tokens)],
        [HBM_SPEC],
        flops=1_000_000_000_000,
        moved=10_000_000_000,
        scratch=[pltpu.SemaphoreType.DMA((count,))],
    )
    received = exchange(slices, "kv", count)
    matrices = [head_input_matrix, group_input_matrix, group_readout_matrix, output_gate_matrix]

    scale = input_norm_scale.reshape(1, width)
    coef, small, norm = call(
        functools.partial(step_body, head_dim),
        [
            pltpu.VMEM((props + 2, ROWS, inner), F32),
            pltpu.VMEM((ROWS, heads), F32),
            pltpu.VMEM((ROWS, 128), F32),
        ],
        [
            accepted,
            vmem(tokens),
            vmem(scale),
            vmem(step_size_matrix.T),
            step_size_bias.reshape(1, heads),
            log_decay_rate.reshape(1, heads),
            direct_path_weight.reshape(1, heads),
            proposal_extra_decay.reshape(props, heads),
        ],
        [SMEM_SPEC] + [VMEM_SPEC] * 7,
        flops=20_000_000,
        scratch=[pltpu.VMEM(((props + 2) * ROWS, heads), F32)],
    )
    states = vmem(per_proposal_states)
    high, low, early, taps = call(
        state_body,
        [
            pltpu.VMEM((groups * size, inner), BF16),
            pltpu.VMEM((groups * size, inner), BF16),
            pltpu.VMEM((ROWS, conv), F32),
            pltpu.VMEM((ROWS, conv), F32),
        ],
        [accepted, states, convolution_history_rows, convolution_tap_weight],
        [SMEM_SPEC] + [VMEM_SPEC] * 3,
        flops=20_000_000,
    )

    own, *partials = call(
        functools.partial(project_body, count, props),
        [pltpu.VMEM((4, packed), F32)] + [pltpu.VMEM((4, packed), BF16)] * (count - 1),
        [vmem(s) for s in [slices[0]] + received]
        + matrices
        + [vmem(scale)],
        [VMEM_SPEC] * (count + 5),
        flops=200_000_000,
        scratch=[pltpu.VMEM((4 * count, packed), F32), pltpu.VMEM((4 * count, rows), F32)],
    )
    sums = exchange([None] + partials, "kv", count)
    gated, fresh, act = call(
        functools.partial(mixer_body, props, groups),
        [
            pltpu.VMEM((4, inner), BF16),
            pltpu.VMEM((ROWS, conv), F32),
            pltpu.VMEM((ROWS, conv), F32),
        ],
        [vmem(v) for v in [own] + sums + [norm, coef, early, taps, high, low]]
        + [vmem(group_norm_scale.reshape(1, inner))],
        [VMEM_SPEC] * (count + 7),
        flops=20_000_000,
        scratch=[pltpu.VMEM((ROWS, total), F32), pltpu.VMEM((ROWS, inner), F32)],
    )
    gathered = exchange([gated] * count, "kv", count)
    per = heads // groups
    half = per // 2
    pieces = [(g, at, at + half) for g in range(groups) for at in (0, half)]
    first = 3 * len(pieces) // 4
    all_states = jax.ShapeDtypeStruct((1, props, heads, head_dim, size), F32)

    def scratch(number):
        shape = (props, number * half, head_dim, size)
        return [pltpu.VMEM(shape, F32), pltpu.SemaphoreType.DMA((number,))]

    new_states, flag = call(
        functools.partial(states_body, props, groups, pieces[:first]),
        [all_states, pltpu.VMEM((ROWS, 128), F32)],
        [accepted, states] + [vmem(v) for v in (small, act, coef)],
        [SMEM_SPEC] + [VMEM_SPEC] * 4,
        flops=30_000_000,
        out_specs=[HBM_SPEC, VMEM_SPEC],
        scratch=scratch(first),
    )
    new_states, new_tail = call(
        functools.partial(states_body, props, groups, pieces[first:]),
        [all_states, jax.ShapeDtypeStruct(convolution_history_rows.shape, BF16)],
        [accepted, states]
        + [vmem(v) for v in (small, act, coef, fresh, convolution_history_rows)]
        + [hbm(new_states)],
        [SMEM_SPEC] + [VMEM_SPEC] * 6 + [HBM_SPEC],
        flops=30_000_000,
        out_specs=[HBM_SPEC, VMEM_SPEC],
        scratch=scratch(len(pieces) - first),
        aliases={7: 0},
    )
    blocks = call(
        functools.partial(output_body, count),
        [pltpu.VMEM((4, out_cols), BF16)] * count,
        [vmem(v) for v in [gated] + gathered + [output_projection_matrix, flag]],
        [VMEM_SPEC] * (count + 2),
        flops=100_000_000,
        scratch=[
            pltpu.VMEM((count, ROWS, out_cols), F32),
            pltpu.VMEM((4 * count, inner), F32),
        ],
    )
    last = exchange(blocks, "tp", count)
    (mixed,) = call(
        final_body,
        [jax.ShapeDtypeStruct((1, props, out_cols), BF16)],
        [vmem(v) for v in [blocks[0]] + last],
        [VMEM_SPEC] * count,
    )
    return (mixed, new_states, new_tail)


def rms_scale(values):
    return lax.rsqrt(jnp.mean(values * values, axis=-1, keepdims=True) + epsilon)


def causal_states(log_decay_factor, head_step_size, ssm_inputs, inject, start_state):
    cumulative = jnp.cumsum(log_decay_factor, axis=1)
    length = log_decay_factor.shape[1]
    lower = (jnp.arange(length)[:, None] >= jnp.arange(length)[None, :])[None, :, :, None]
    spread = cumulative[:, :, None, :] - cumulative[:, None, :, :]
    factors = jnp.where(lower, jnp.exp(jnp.where(lower, spread, 0.0)), 0.0)
    mixing = factors * head_step_size[:, None, :, :]
    carried = jnp.exp(cumulative)[..., None, None] * start_state[:, None]
    return carried + jnp.einsum("sjih,sihp,sihn->sjhpn", mixing, ssm_inputs, inject)


def combine_head_outputs(
    incoming_token_rows,
    gate_portion,
    unactivated_step,
    step_size_bias,
    log_decay_rate,
    direct_path_weight,
    convolution_tap_weight,
    convolution_history_rows,
    per_proposal_states,
    accepted,
    proposal_extra_decay,
    group_norm_scale,
):
    sequences, proposals, group_count, group_width = incoming_token_rows.shape
    head_count = step_size_bias.shape[0]
    head_dim = per_proposal_states.shape[3]
    state_size = per_proposal_states.shape[4]
    per_group = head_count // group_count
    group_inner = per_group * head_dim
    tap_count = convolution_tap_weight.shape[0]
    offsets = accepted[:, None] + jnp.arange(tap_count - 1, dtype=jnp.int32)[None, :]
    context = jnp.take_along_axis(convolution_history_rows, offsets[:, :, None, None], axis=1)
    convolution_span = jnp.concatenate([context, incoming_token_rows], axis=1)
    widened = convolution_span.astype(jnp.float32)
    convolved = jnp.zeros((sequences, proposals, group_count, group_width), jnp.float32)
    for conv_tap in range(tap_count):
        convolved = convolved + widened[
            :, conv_tap : conv_tap + proposals
        ] * convolution_tap_weight[conv_tap].astype(jnp.float32)
    activated = jax.nn.silu(convolved)
    ssm_inputs = activated[..., :group_inner].reshape(sequences, proposals, head_count, head_dim)
    inject = jnp.repeat(activated[..., group_inner : group_inner + state_size], per_group, axis=2)
    readout = jnp.repeat(activated[..., group_inner + state_size :], per_group, axis=2)
    head_step_size = jax.nn.softplus(unactivated_step + step_size_bias)
    log_decay_factor = proposal_extra_decay - jnp.exp(log_decay_rate) * head_step_size
    chosen = (accepted - 1)[:, None, None, None, None]
    start_state = jnp.take_along_axis(per_proposal_states, chosen, axis=1)[:, 0]
    running_state_rows = causal_states(
        log_decay_factor, head_step_size, ssm_inputs, inject, start_state
    )
    response = (
        jnp.einsum("sjhn,sjhpn->sjhp", readout, running_state_rows)
        + direct_path_weight[:, None] * ssm_inputs
    )
    gate_raw = gate_portion.astype(jnp.float32).reshape(sequences, proposals, head_count, head_dim)
    gate_applied_output = (response * jax.nn.silu(gate_raw)).reshape(
        sequences, proposals, group_count, group_inner
    )
    scaled = (
        gate_applied_output
        * rms_scale(gate_applied_output)
        * group_norm_scale.reshape(group_count, group_inner)
    )
    flat_gated = scaled.astype(jnp.bfloat16).reshape(sequences, proposals, head_count * head_dim)
    return (flat_gated, running_state_rows, convolution_span)


def local(
    tokens,
    input_norm_scale,
    head_input_matrix,
    output_gate_matrix,
    group_input_matrix,
    group_readout_matrix,
    step_size_matrix,
    step_size_bias,
    log_decay_rate,
    direct_path_weight,
    convolution_tap_weight,
    convolution_history_rows,
    per_proposal_states,
    accepted,
    proposal_extra_decay,
    group_norm_scale,
    output_projection_matrix,
):
    local_seqs, proposals, _ = tokens.shape
    head_local = step_size_bias.shape[0]
    group_local = convolution_tap_weight.shape[1]
    head_dim = per_proposal_states.shape[3]
    state_size = per_proposal_states.shape[4]
    group_inner = head_local // group_local * head_dim
    widened = tokens.astype(jnp.float32)
    normed = (widened * rms_scale(widened) * input_norm_scale).astype(jnp.bfloat16)
    unactivated_step = jnp.einsum(
        "sjd,dh->sjh", normed, step_size_matrix, preferred_element_type=jnp.float32
    )
    pieces = lax.all_to_all(normed, "kv", split_axis=2, concat_axis=0, tiled=True)
    joined = jnp.concatenate(
        [head_input_matrix, group_input_matrix, group_readout_matrix, output_gate_matrix], axis=1
    )
    summed = lax.psum_scatter(
        jnp.einsum("sjd,dc->sjc", pieces, joined, preferred_element_type=jnp.float32),
        "kv",
        scatter_dimension=0,
        tiled=True,
    )
    projected = summed.astype(jnp.bfloat16)
    input_width = head_local * head_dim
    inject_width = group_local * state_size
    part_input = projected[..., :input_width].reshape(
        local_seqs, proposals, group_local, group_inner
    )
    part_inject = projected[..., input_width : input_width + inject_width].reshape(
        local_seqs, proposals, group_local, state_size
    )
    part_readout = projected[
        ..., input_width + inject_width : input_width + 2 * inject_width
    ].reshape(local_seqs, proposals, group_local, state_size)
    gate_portion = projected[..., input_width + 2 * inject_width :]
    incoming_token_rows = jnp.concatenate([part_input, part_inject, part_readout], axis=-1)
    gate_applied_output, running_state_rows, convolution_span = combine_head_outputs(
        incoming_token_rows,
        gate_portion,
        unactivated_step,
        step_size_bias,
        log_decay_rate,
        direct_path_weight,
        convolution_tap_weight,
        convolution_history_rows,
        per_proposal_states,
        accepted,
        proposal_extra_decay,
        group_norm_scale,
    )
    terms = jnp.einsum(
        "sjc,cd->sjd",
        lax.all_gather(gate_applied_output, "kv", axis=0, tiled=True),
        output_projection_matrix,
        preferred_element_type=jnp.float32,
    )
    mixed = lax.psum_scatter(terms.astype(jnp.bfloat16), "tp", scatter_dimension=0, tiled=True)
    return (mixed, running_state_rows, convolution_span)


def chosen(mesh, *arguments):
    tokens, matrix = arguments[0], arguments[2]
    kv, tp = mesh.shape["kv"], mesh.shape["tp"]
    slim = tokens.shape[:2] == (1, 3) and matrix.shape[0] % 128 == 0
    slim = slim and arguments[10].shape[1] == 2
    if slim and kv == tp and kv in (2, 4):
        return fast_local(kv, *arguments)
    return local(*arguments)


def solution(mesh):
    return jax.shard_map(
        functools.partial(chosen, mesh),
        mesh=mesh,
        in_specs=(
            P(("grp", "kv"), None, None),
            P(),
            P("kv", "tp"),
            P("kv", "tp"),
            P("kv", "tp"),
            P("kv", "tp"),
            P(None, "tp"),
            P("tp"),
            P("tp"),
            P("tp"),
            P(None, "tp", None),
            P(("grp", "kv"), None, "tp", None),
            P(("grp", "kv"), None, "tp", None, None),
            P(("grp", "kv")),
            P(("grp", "kv"), None, "tp"),
            P("tp"),
            P("tp", "kv"),
        ),
        out_specs=(
            P(("grp", "tp"), None, "kv"),
            P(("grp", "kv"), None, "tp", None, None),
            P(("grp", "kv"), None, "tp", None),
        ),
        check_vma=False,
    )
```

```python
import functools

import jax
import jax.numpy as jnp
from jax import lax
from jax.experimental import pallas as pl
from jax.experimental.pallas import tpu as pltpu
from jax.sharding import PartitionSpec as P


epsilon = 1e-06
F32 = jnp.float32
BF16 = jnp.bfloat16
ROWS = 8


def vmem(x):
    return pltpu.with_memory_space_constraint(x, pltpu.VMEM)


def hbm(x):
    return pltpu.with_memory_space_constraint(x, pltpu.HBM)


VMEM_SPEC = pl.BlockSpec(memory_space=pltpu.VMEM)
SMEM_SPEC = pl.BlockSpec(memory_space=pltpu.SMEM)
HBM_SPEC = pl.BlockSpec(memory_space=pl.ANY)


def call(body, outs, ins, specs, flops=0, scratch=(), out_specs=None, limit=20 << 20, moved=0, aliases={}):
    return pl.pallas_call(
        body,
        out_shape=outs,
        in_specs=specs,
        out_specs=out_specs or [VMEM_SPEC] * len(outs),
        scratch_shapes=list(scratch),
        input_output_aliases=aliases,
        cost_estimate=pl.CostEstimate(flops=flops, transcendentals=0, bytes_accessed=moved),
        compiler_params=pltpu.CompilerParams(vmem_limit_bytes=limit),
    )(*ins)


def exchange_tokens(blocks, count):
    got = []
    for step in range(1, count):
        pairs = [
            (i * count + j, (i ^ step) * count + (j ^ 1))
            for i in range(count)
            for j in range(count)
        ]
        got.append(lax.ppermute(blocks[step], ("kv", "tp"), pairs))
    return got


def exchange(blocks, axis, count):
    got = []
    for step in reversed(range(1, count)):
        pairs = [(i, i ^ step) for i in range(count)]
        got.append(lax.ppermute(blocks[step], axis, pairs))
    return got[::-1]


def silu(v):
    return v * jax.nn.sigmoid(v)


def split(v):
    high = v.astype(BF16)
    return high, (v - high.astype(F32)).astype(BF16)


def slice_body(count, tokens, *refs):
    slices, sem = refs[:count], refs[-1]
    me = lax.axis_index("kv")
    width = slices[0].shape[1]
    copies = []
    for step in reversed(range(count)):
        start = pl.multiple_of(lax.bitwise_xor(me, step) * width, 128)
        copy = pltpu.make_async_copy(
            tokens.at[0, :, pl.ds(start, width)], slices[step], sem.at[step]
        )
        copy.start()
        copies.append(copy)
    for copy in copies:
        copy.wait()


def step_body(head_dim, accepted, tokens, scale, step_t, bias, rate, direct, extra, coef, small, norm, table):
    props, heads = extra.shape
    values = tokens[0].astype(F32)
    norm_rows = lax.rsqrt(jnp.mean(values * values, axis=-1, keepdims=True) + epsilon)
    norm[...] = jnp.ones_like(norm)
    norm[0:props, :] = jnp.broadcast_to(norm_rows, (props, norm.shape[1]))
    normed = (values * norm_rows * scale[...]).astype(BF16)
    raw = lax.dot_general(
        normed, step_t[...], (((1,), (1,)), ((), ())), preferred_element_type=F32
    )
    size = jax.nn.softplus(raw + bias[...])
    decay = extra[...] - jnp.exp(rate[...]) * size
    table[...] = jnp.zeros_like(table)
    small[...] = jnp.zeros_like(small)
    small[0:props, :] = jnp.exp(decay)
    total = []
    for j in range(props):
        row = decay[j : j + 1]
        total.append(row if j == 0 else total[-1] + row)
        table[j : j + 1, :] = jnp.exp(total[j])
    for i in range(props):
        own = size[i : i + 1]
        for j in range(i, props):
            at = (1 + i) * ROWS + j
            table[at : at + 1, :] = jnp.exp(total[j] - total[i]) * own
    at = (1 + props) * ROWS
    table[at : at + 1, :] = direct[...]
    width = coef.shape[-1]
    lane = lax.broadcasted_iota(jnp.int32, (heads, width), 1)
    head = lax.broadcasted_iota(jnp.int32, (heads, width), 0)
    spread = jnp.where(lane // head_dim == head, 1.0, 0.0).astype(F32)
    wide = jnp.dot(
        table[...], spread, preferred_element_type=F32, precision=lax.Precision.HIGHEST
    )
    for part in range(coef.shape[0]):
        coef[part] = wide[part * ROWS : (part + 1) * ROWS]


def state_body(accepted, states, history, taps, high, low, early, taps_wide):
    count = accepted[0]
    heads, head_dim, size = states.shape[2:]
    groups = taps.shape[1]
    tap_count = taps.shape[0]
    inner = heads // groups * head_dim
    per = heads // groups

    def widen(rows, target, at):
        rows = rows.astype(F32)
        for g in range(groups):
            row = rows[g : g + 1]
            target[at : at + 1, g * inner : (g + 1) * inner] = row[:, :inner]
            for part in range(2):
                base = groups * inner + part * groups * size + g * size
                target[at : at + 1, base : base + size] = row[
                    :, inner + part * size : inner + (part + 1) * size
                ]

    taps_wide[...] = jnp.zeros_like(taps_wide)
    early[...] = jnp.zeros_like(early)
    for k in range(tap_count):
        widen(taps[k], taps_wide, k)
    for k in range(tap_count - 1):
        widen(history[0, count + k], early, k)
    context = early[...]
    before = tap_count - 1
    total = context * taps_wide[0:1, :]
    keep = lax.broadcasted_iota(jnp.int32, (ROWS, 1), 0) < before
    for k in range(1, before):
        total = total + jnp.where(keep, pltpu.roll(context, ROWS - k, 0), 0.0) * taps_wide[k : k + 1, :]
    early[...] = jnp.where(keep, total, 0.0)

    high[...] = jnp.zeros_like(high)
    low[...] = jnp.zeros_like(low)
    pair = 128 // head_dim
    for g in range(groups):
        for block in range(per // pair):
            at = g * per + block * pair
            tile = states[0, count - 1, at : at + pair].reshape(pair * head_dim, size).T
            big, rest = split(tile)
            cols = slice(at * head_dim, (at + pair) * head_dim)
            high[g * size : (g + 1) * size, cols] = big
            low[g * size : (g + 1) * size, cols] = rest


def stack_rows(parts, lhs):
    lhs[...] = jnp.zeros_like(lhs)
    for j, part in enumerate(parts):
        lhs[4 * j : 4 * j + part.shape[0], :] = part[...].astype(F32)
    return lhs[...].astype(BF16)


def packed_width(props, width):
    return -(-props * width // 4 // 128) * 128


def project_body(count, props, *refs):
    slices = refs[:count]
    inputs, inject, readout, gates, scale = refs[count : count + 5]
    own = refs[count + 5]
    outs = refs[count + 6 : count + 5 + count]
    stage, rows = refs[-2:]
    depth = rows.shape[1]
    start = pl.multiple_of(lax.axis_index("kv") * depth, 128)
    stack_rows(slices, rows)
    lhs = (rows[...] * scale[:, pl.ds(start, depth)]).astype(BF16)
    wide = stage.shape[1]
    first = inputs.shape[1]
    both = inject.shape[1] + readout.shape[1]
    left = wide - first - both
    rest = gates.shape[1] - left

    result = jnp.dot(lhs, gates[...], preferred_element_type=F32)
    stage[:, first + both :] = result[:, :left]
    extra = result[:, left:]
    result = jnp.dot(lhs, inputs[...], preferred_element_type=F32)
    stage[:, :first] = result
    pair = jnp.concatenate([inject[...], readout[...]], axis=1)
    stage[:, first : first + both] = jnp.dot(lhs, pair, preferred_element_type=F32)
    for j in range(count):
        for r in range(props):
            at = 4 * j + r
            stage[4 * j + 3 : 4 * j + 4, r * rest : (r + 1) * rest] = extra[at : at + 1]
    own[...] = stage[0:4, :]
    for j, out in enumerate(outs, 1):
        out[...] = stage[4 * j : 4 * j + 4, :].astype(BF16)


def mixer_body(props, groups, *refs):
    own, *rest = refs
    count = len(rest) - 12
    others = rest[:count]
    norm, coef, early, taps, high, low, gain, gated, fresh, act, summed, norms = rest[count:]
    inner = gain.shape[1]
    conv = early.shape[1]
    per = inner // groups
    both = (conv - inner) // 2
    size = both // groups
    summed[...] = jnp.zeros_like(summed)
    total = own[...]
    for other in others:
        total = total + other[...].astype(F32)
    wide = total.shape[1]
    rest = summed.shape[1] - wide
    summed[0:props, :wide] = total[0:props]
    for r in range(props):
        summed[r : r + 1, wide:] = total[3:4, r * rest : (r + 1) * rest]
    summed[...] = (summed[...] * norm[:, 0:1]).astype(BF16).astype(F32)
    rows = summed[:, :conv]
    fresh[...] = rows
    tap_count = 4
    value = early[...] + rows * taps[tap_count - 1 : tap_count, :]
    for k in range(1, props):
        value = value + pltpu.roll(rows * taps[tap_count - 1 - k : tap_count - k, :], k, 0)
    value = silu(value)
    act[...] = value
    x = value[:, :inner]
    b = value[:, inner : inner + both]
    c = value[:, inner + both :]
    c_high, c_low = split(c)
    left = jnp.concatenate([c_high.astype(F32), c_low.astype(F32)], axis=0).astype(BF16)
    carried = jnp.dot(left, high[...], preferred_element_type=F32)
    carried = carried[:ROWS] + carried[ROWS:]
    carried = carried + jnp.dot(c_high, low[...], preferred_element_type=F32)
    lane = lax.broadcasted_iota(jnp.int32, (ROWS, both), 1)
    response = coef[0] * carried + coef[1 + props, 0:1, :] * x
    pieces = []
    weights = []
    for i in range(props):
        product = c * b[i : i + 1]
        weights.append(
            [
                jnp.sum(jnp.where(lane // size == g, product, 0.0), axis=1, keepdims=True)
                for g in range(groups)
            ]
        )
    gate = summed[:, conv:]
    gate = silu(gate)
    for g in range(groups):
        at = slice(g * per, (g + 1) * per)
        part = response[:, at]
        for i in range(props):
            part = part + coef[1 + i, :, at] * weights[i][g] * x[i : i + 1, at]
        part = part * gate[:, at]
        mean = jnp.sum(part * part, axis=1, keepdims=True) * (1.0 / per)
        pieces.append(part * lax.rsqrt(mean + epsilon) * gain[:, at])
    norms[...] = jnp.concatenate(pieces, axis=1)
    gated[...] = norms[0:4].astype(BF16)


def states_body(props, groups, pieces, accepted, start, small, act, coef, *refs):
    heads, head_dim, size = start.shape[2:]
    per = heads // groups
    last = pieces[-1][2] == per and pieces[-1][0] == groups - 1
    if last:
        fresh, history, _, states, tail_out, held, tail, sem = refs
    else:
        states, flag, held, sem = refs
        flag[...] = jnp.zeros_like(flag)
    copies = []
    inner = per * head_dim
    wide = heads * head_dim
    block = groups * size
    count = accepted[0]
    if last:
        before = tail.shape[1] - props
        for k in range(before):
            tail[0, k] = history[0, count + k]
        for j in range(props):
            rows = []
            for q in range(groups):
                row = [fresh[j : j + 1, q * inner : (q + 1) * inner]]
                for part in range(2):
                    base = wide + part * block + q * size
                    row.append(fresh[j : j + 1, base : base + size])
                rows.append(jnp.concatenate(row, axis=1))
            tail[0, before + j] = jnp.concatenate(rows, axis=0).astype(BF16)
        copy = pltpu.make_async_copy(tail, tail_out, sem.at[len(pieces)])
        copy.start()
        copies.append(copy)
    row_at = lax.broadcasted_iota(jnp.int32, (ROWS, 1), 0)
    b_high, b_low = split(act[:, wide : wide + block])
    b_high, b_low = b_high.astype(F32), b_low.astype(F32)
    filled = 0
    for g, low, high in pieces:
        lanes = slice(g * inner + low * head_dim, g * inner + high * head_dim)
        steps = jnp.zeros((ROWS, (high - low) * head_dim), F32)
        for j in range(props):
            steps = jnp.where(row_at == j, coef[1 + j, :, lanes], steps)
        dx = act[:, lanes] * steps
        dx_high, dx_low = split(dx)
        dx_high, dx_low = dx_high.astype(F32), dx_low.astype(F32)
        left = jnp.concatenate(
            [dx_high, dx_low, dx_high, jnp.zeros_like(dx)], axis=0
        ).astype(BF16)
        blocks = []
        for j in range(props):
            hi = jnp.where(row_at == j, b_high, 0.0)
            lo = jnp.where(row_at == j, b_low, 0.0)
            full = jnp.concatenate([hi, hi, lo, jnp.zeros_like(hi)], axis=0)
            if g:
                full = pltpu.roll(full, block - g * size, 1)
            blocks.append(full)
        right = jnp.concatenate(blocks, axis=1).astype(BF16)
        update = lax.dot_general(
            left, right, (((0,), (0,)), ((), ())), preferred_element_type=F32
        )
        for h in range(high - low):
            at = g * per + low + h
            state = start[0, count - 1, at]
            for j in range(props):
                new = update[h * head_dim : (h + 1) * head_dim, j * block : j * block + size]
                state = state * small[j : j + 1, at : at + 1] + new
                held[j, filled + h] = state
        copy = pltpu.make_async_copy(
            held.at[:, pl.ds(filled, high - low)],
            states.at[0, :, pl.ds(g * per + low, high - low)],
            sem.at[pieces.index((g, low, high))],
        )
        copy.start()
        copies.append(copy)
        filled += high - low
    for copy in copies:
        copy.wait()


def output_body(count, *refs):
    parts = refs[:count]
    weight = refs[count]
    outs = refs[count + 2 : count + 2 + count]
    result, lhs = refs[-2:]
    which = lax.bitwise_xor(lax.axis_index("kv"), lax.axis_index("tp"))
    product = jnp.dot(stack_rows(parts, lhs), weight[...], preferred_element_type=F32)
    for j in range(count):
        result[j, 0:4] = product[4 * j : 4 * j + 4]
    for step in range(count):
        outs[step][...] = result[lax.bitwise_xor(which, step), 0:4].astype(BF16)


def final_body(*refs):
    *parts, out = refs
    total = parts[0][...].astype(F32)
    for part in parts[1:]:
        total = total + part[...].astype(F32)
    out[0] = total[0 : out.shape[1]].astype(BF16)


def fast_local(
    count,
    tokens,
    input_norm_scale,
    head_input_matrix,
    output_gate_matrix,
    group_input_matrix,
    group_readout_matrix,
    step_size_matrix,
    step_size_bias,
    log_decay_rate,
    direct_path_weight,
    convolution_tap_weight,
    convolution_history_rows,
    per_proposal_states,
    accepted,
    proposal_extra_decay,
    group_norm_scale,
    output_projection_matrix,
):
    _, props, width = tokens.shape
    heads = step_size_bias.shape[0]
    _, _, groups, channels = convolution_history_rows.shape
    head_dim, size = per_proposal_states.shape[3:]
    inner = heads * head_dim
    conv = groups * channels
    rows = head_input_matrix.shape[0]
    total = conv + inner
    packed = packed_width(props, total)
    out_cols = output_projection_matrix.shape[1]

    slices = call(
        functools.partial(slice_body, count),
        [pltpu.VMEM((props, rows), BF16)] * count,
        [hbm(tokens)],
        [HBM_SPEC],
        flops=1_000_000_000_000,
        moved=10_000_000_000,
        scratch=[pltpu.SemaphoreType.DMA((count,))],
    )
    received = exchange_tokens(slices, count)
    matrices = [head_input_matrix, group_input_matrix, group_readout_matrix, output_gate_matrix]

    scale = input_norm_scale.reshape(1, width)
    coef, small, norm = call(
        functools.partial(step_body, head_dim),
        [
            pltpu.VMEM((props + 2, ROWS, inner), F32),
            pltpu.VMEM((ROWS, heads), F32),
            pltpu.VMEM((ROWS, 128), F32),
        ],
        [
            accepted,
            vmem(tokens),
            vmem(scale),
            vmem(step_size_matrix.T),
            step_size_bias.reshape(1, heads),
            log_decay_rate.reshape(1, heads),
            direct_path_weight.reshape(1, heads),
            proposal_extra_decay.reshape(props, heads),
        ],
        [SMEM_SPEC] + [VMEM_SPEC] * 7,
        flops=20_000_000,
        scratch=[pltpu.VMEM(((props + 2) * ROWS, heads), F32)],
    )
    states = vmem(per_proposal_states)
    high, low, early, taps = call(
        state_body,
        [
            pltpu.VMEM((groups * size, inner), BF16),
            pltpu.VMEM((groups * size, inner), BF16),
            pltpu.VMEM((ROWS, conv), F32),
            pltpu.VMEM((ROWS, conv), F32),
        ],
        [accepted, states, convolution_history_rows, convolution_tap_weight],
        [SMEM_SPEC] + [VMEM_SPEC] * 3,
        flops=20_000_000,
    )

    own, *partials = call(
        functools.partial(project_body, count, props),
        [pltpu.VMEM((4, packed), F32)] + [pltpu.VMEM((4, packed), BF16)] * (count - 1),
        [vmem(s) for s in [slices[0]] + received]
        + matrices
        + [vmem(scale)],
        [VMEM_SPEC] * (count + 5),
        flops=200_000_000,
        scratch=[pltpu.VMEM((4 * count, packed), F32), pltpu.VMEM((4 * count, rows), F32)],
    )
    sums = exchange([None] + partials, "kv", count)
    gated, fresh, act = call(
        functools.partial(mixer_body, props, groups),
        [
            pltpu.VMEM((4, inner), BF16),
            pltpu.VMEM((ROWS, conv), F32),
            pltpu.VMEM((ROWS, conv), F32),
        ],
        [vmem(v) for v in [own] + sums + [norm, coef, early, taps, high, low]]
        + [vmem(group_norm_scale.reshape(1, inner))],
        [VMEM_SPEC] * (count + 7),
        flops=20_000_000,
        scratch=[pltpu.VMEM((ROWS, total), F32), pltpu.VMEM((ROWS, inner), F32)],
    )
    gathered = exchange([gated] * count, "kv", count)
    per = heads // groups
    half = per // 2
    pieces = [(g, at, at + half) for g in range(groups) for at in (0, half)]
    first = 3 * len(pieces) // 4
    all_states = jax.ShapeDtypeStruct((1, props, heads, head_dim, size), F32)

    def scratch(number, *more):
        shape = (props, number * half, head_dim, size)
        return [pltpu.VMEM(shape, F32), *more, pltpu.SemaphoreType.DMA((number + 1,))]

    new_states, flag = call(
        functools.partial(states_body, props, groups, pieces[:first]),
        [all_states, pltpu.VMEM((ROWS, 128), F32)],
        [accepted, states] + [vmem(v) for v in (small, act, coef)],
        [SMEM_SPEC] + [VMEM_SPEC] * 4,
        flops=30_000_000,
        out_specs=[HBM_SPEC, VMEM_SPEC],
        scratch=scratch(first),
    )
    new_states, new_tail = call(
        functools.partial(states_body, props, groups, pieces[first:]),
        [all_states, jax.ShapeDtypeStruct(convolution_history_rows.shape, BF16)],
        [accepted, states]
        + [vmem(v) for v in (small, act, coef, fresh, convolution_history_rows)]
        + [hbm(new_states)],
        [SMEM_SPEC] + [VMEM_SPEC] * 6 + [HBM_SPEC],
        flops=30_000_000,
        out_specs=[HBM_SPEC, HBM_SPEC],
        scratch=scratch(
            len(pieces) - first, pltpu.VMEM(convolution_history_rows.shape, BF16)
        ),
        aliases={7: 0},
    )
    blocks = call(
        functools.partial(output_body, count),
        [pltpu.VMEM((4, out_cols), BF16)] * count,
        [vmem(v) for v in [gated] + gathered + [output_projection_matrix, flag]],
        [VMEM_SPEC] * (count + 2),
        flops=100_000_000,
        scratch=[
            pltpu.VMEM((count, ROWS, out_cols), F32),
            pltpu.VMEM((4 * count, inner), F32),
        ],
    )
    last = exchange(blocks, "tp", count)
    (mixed,) = call(
        final_body,
        [jax.ShapeDtypeStruct((1, props, out_cols), BF16)],
        [vmem(v) for v in [blocks[0]] + last],
        [VMEM_SPEC] * count,
    )
    return (mixed, new_states, new_tail)


def rms_scale(values):
    return lax.rsqrt(jnp.mean(values * values, axis=-1, keepdims=True) + epsilon)


def causal_states(log_decay_factor, head_step_size, ssm_inputs, inject, start_state):
    cumulative = jnp.cumsum(log_decay_factor, axis=1)
    length = log_decay_factor.shape[1]
    lower = (jnp.arange(length)[:, None] >= jnp.arange(length)[None, :])[None, :, :, None]
    spread = cumulative[:, :, None, :] - cumulative[:, None, :, :]
    factors = jnp.where(lower, jnp.exp(jnp.where(lower, spread, 0.0)), 0.0)
    mixing = factors * head_step_size[:, None, :, :]
    carried = jnp.exp(cumulative)[..., None, None] * start_state[:, None]
    return carried + jnp.einsum("sjih,sihp,sihn->sjhpn", mixing, ssm_inputs, inject)


def combine_head_outputs(
    incoming_token_rows,
    gate_portion,
    unactivated_step,
    step_size_bias,
    log_decay_rate,
    direct_path_weight,
    convolution_tap_weight,
    convolution_history_rows,
    per_proposal_states,
    accepted,
    proposal_extra_decay,
    group_norm_scale,
):
    sequences, proposals, group_count, group_width = incoming_token_rows.shape
    head_count = step_size_bias.shape[0]
    head_dim = per_proposal_states.shape[3]
    state_size = per_proposal_states.shape[4]
    per_group = head_count // group_count
    group_inner = per_group * head_dim
    tap_count = convolution_tap_weight.shape[0]
    offsets = accepted[:, None] + jnp.arange(tap_count - 1, dtype=jnp.int32)[None, :]
    context = jnp.take_along_axis(convolution_history_rows, offsets[:, :, None, None], axis=1)
    convolution_span = jnp.concatenate([context, incoming_token_rows], axis=1)
    widened = convolution_span.astype(jnp.float32)
    convolved = jnp.zeros((sequences, proposals, group_count, group_width), jnp.float32)
    for conv_tap in range(tap_count):
        convolved = convolved + widened[
            :, conv_tap : conv_tap + proposals
        ] * convolution_tap_weight[conv_tap].astype(jnp.float32)
    activated = jax.nn.silu(convolved)
    ssm_inputs = activated[..., :group_inner].reshape(sequences, proposals, head_count, head_dim)
    inject = jnp.repeat(activated[..., group_inner : group_inner + state_size], per_group, axis=2)
    readout = jnp.repeat(activated[..., group_inner + state_size :], per_group, axis=2)
    head_step_size = jax.nn.softplus(unactivated_step + step_size_bias)
    log_decay_factor = proposal_extra_decay - jnp.exp(log_decay_rate) * head_step_size
    chosen = (accepted - 1)[:, None, None, None, None]
    start_state = jnp.take_along_axis(per_proposal_states, chosen, axis=1)[:, 0]
    running_state_rows = causal_states(
        log_decay_factor, head_step_size, ssm_inputs, inject, start_state
    )
    response = (
        jnp.einsum("sjhn,sjhpn->sjhp", readout, running_state_rows)
        + direct_path_weight[:, None] * ssm_inputs
    )
    gate_raw = gate_portion.astype(jnp.float32).reshape(sequences, proposals, head_count, head_dim)
    gate_applied_output = (response * jax.nn.silu(gate_raw)).reshape(
        sequences, proposals, group_count, group_inner
    )
    scaled = (
        gate_applied_output
        * rms_scale(gate_applied_output)
        * group_norm_scale.reshape(group_count, group_inner)
    )
    flat_gated = scaled.astype(jnp.bfloat16).reshape(sequences, proposals, head_count * head_dim)
    return (flat_gated, running_state_rows, convolution_span)


def local(
    tokens,
    input_norm_scale,
    head_input_matrix,
    output_gate_matrix,
    group_input_matrix,
    group_readout_matrix,
    step_size_matrix,
    step_size_bias,
    log_decay_rate,
    direct_path_weight,
    convolution_tap_weight,
    convolution_history_rows,
    per_proposal_states,
    accepted,
    proposal_extra_decay,
    group_norm_scale,
    output_projection_matrix,
):
    local_seqs, proposals, _ = tokens.shape
    head_local = step_size_bias.shape[0]
    group_local = convolution_tap_weight.shape[1]
    head_dim = per_proposal_states.shape[3]
    state_size = per_proposal_states.shape[4]
    group_inner = head_local // group_local * head_dim
    widened = tokens.astype(jnp.float32)
    normed = (widened * rms_scale(widened) * input_norm_scale).astype(jnp.bfloat16)
    unactivated_step = jnp.einsum(
        "sjd,dh->sjh", normed, step_size_matrix, preferred_element_type=jnp.float32
    )
    pieces = lax.all_to_all(normed, "kv", split_axis=2, concat_axis=0, tiled=True)
    joined = jnp.concatenate(
        [head_input_matrix, group_input_matrix, group_readout_matrix, output_gate_matrix], axis=1
    )
    summed = lax.psum_scatter(
        jnp.einsum("sjd,dc->sjc", pieces, joined, preferred_element_type=jnp.float32),
        "kv",
        scatter_dimension=0,
        tiled=True,
    )
    projected = summed.astype(jnp.bfloat16)
    input_width = head_local * head_dim
    inject_width = group_local * state_size
    part_input = projected[..., :input_width].reshape(
        local_seqs, proposals, group_local, group_inner
    )
    part_inject = projected[..., input_width : input_width + inject_width].reshape(
        local_seqs, proposals, group_local, state_size
    )
    part_readout = projected[
        ..., input_width + inject_width : input_width + 2 * inject_width
    ].reshape(local_seqs, proposals, group_local, state_size)
    gate_portion = projected[..., input_width + 2 * inject_width :]
    incoming_token_rows = jnp.concatenate([part_input, part_inject, part_readout], axis=-1)
    gate_applied_output, running_state_rows, convolution_span = combine_head_outputs(
        incoming_token_rows,
        gate_portion,
        unactivated_step,
        step_size_bias,
        log_decay_rate,
        direct_path_weight,
        convolution_tap_weight,
        convolution_history_rows,
        per_proposal_states,
        accepted,
        proposal_extra_decay,
        group_norm_scale,
    )
    terms = jnp.einsum(
        "sjc,cd->sjd",
        lax.all_gather(gate_applied_output, "kv", axis=0, tiled=True),
        output_projection_matrix,
        preferred_element_type=jnp.float32,
    )
    mixed = lax.psum_scatter(terms.astype(jnp.bfloat16), "tp", scatter_dimension=0, tiled=True)
    return (mixed, running_state_rows, convolution_span)


def chosen(mesh, *arguments):
    tokens, matrix = arguments[0], arguments[2]
    kv, tp = mesh.shape["kv"], mesh.shape["tp"]
    slim = tokens.shape[:2] == (1, 3) and matrix.shape[0] % 128 == 0
    slim = slim and arguments[10].shape[1] == 2
    if slim and kv == tp and kv in (2, 4):
        return fast_local(kv, *arguments)
    return local(*arguments)


def solution(mesh):
    return jax.shard_map(
        functools.partial(chosen, mesh),
        mesh=mesh,
        in_specs=(
            P(("grp", "kv"), None, None),
            P(),
            P("kv", "tp"),
            P("kv", "tp"),
            P("kv", "tp"),
            P("kv", "tp"),
            P(None, "tp"),
            P("tp"),
            P("tp"),
            P("tp"),
            P(None, "tp", None),
            P(("grp", "kv"), None, "tp", None),
            P(("grp", "kv"), None, "tp", None, None),
            P(("grp", "kv")),
            P(("grp", "kv"), None, "tp"),
            P("tp"),
            P("tp", "kv"),
        ),
        out_specs=(
            P(("grp", "tp"), None, "kv"),
            P(("grp", "kv"), None, "tp", None, None),
            P(("grp", "kv"), None, "tp", None),
        ),
        check_vma=False,
    )
```

```python
import functools

import jax
import jax.numpy as jnp
from jax import lax
from jax.experimental import pallas as pl
from jax.experimental.pallas import tpu as pltpu
from jax.sharding import PartitionSpec as P


epsilon = 1e-06
F32 = jnp.float32
BF16 = jnp.bfloat16
ROWS = 8


def vmem(x):
    return pltpu.with_memory_space_constraint(x, pltpu.VMEM)


def hbm(x):
    return pltpu.with_memory_space_constraint(x, pltpu.HBM)


VMEM_SPEC = pl.BlockSpec(memory_space=pltpu.VMEM)
SMEM_SPEC = pl.BlockSpec(memory_space=pltpu.SMEM)
HBM_SPEC = pl.BlockSpec(memory_space=pl.ANY)


def call(body, outs, ins, specs, flops=0, scratch=(), out_specs=None, limit=20 << 20, moved=0, aliases={}):
    return pl.pallas_call(
        body,
        out_shape=outs,
        in_specs=specs,
        out_specs=out_specs or [VMEM_SPEC] * len(outs),
        scratch_shapes=list(scratch),
        input_output_aliases=aliases,
        cost_estimate=pl.CostEstimate(flops=flops, transcendentals=0, bytes_accessed=moved),
        compiler_params=pltpu.CompilerParams(vmem_limit_bytes=limit),
    )(*ins)


def exchange_tokens(blocks, count):
    got = []
    for step in range(1, count):
        pairs = [
            (i * count + j, (i ^ step) * count + (j ^ 1))
            for i in range(count)
            for j in range(count)
        ]
        got.append(lax.ppermute(blocks[step], ("kv", "tp"), pairs))
    return got


def exchange(blocks, axis, count):
    got = []
    for step in reversed(range(1, count)):
        pairs = [(i, i ^ step) for i in range(count)]
        got.append(lax.ppermute(blocks[step], axis, pairs))
    return got[::-1]


def silu(v):
    return v * jax.nn.sigmoid(v)


def split(v):
    high = v.astype(BF16)
    return high, (v - high.astype(F32)).astype(BF16)


def slice_body(count, tokens, *refs):
    slices, sem = refs[:count], refs[-1]
    me = lax.axis_index("kv")
    width = slices[0].shape[1]
    copies = []
    for step in reversed(range(count)):
        start = pl.multiple_of(lax.bitwise_xor(me, step) * width, 128)
        copy = pltpu.make_async_copy(
            tokens.at[0, :, pl.ds(start, width)], slices[step], sem.at[step]
        )
        copy.start()
        copies.append(copy)
    for copy in copies:
        copy.wait()


def hold_body(*refs):
    pass


def step_body(head_dim, accepted, tokens, scale, step_t, bias, rate, direct, extra, coef, small, norm, table):
    props, heads = extra.shape
    values = tokens[0].astype(F32)
    norm_rows = lax.rsqrt(jnp.mean(values * values, axis=-1, keepdims=True) + epsilon)
    norm[...] = jnp.ones_like(norm)
    norm[0:props, :] = jnp.broadcast_to(norm_rows, (props, norm.shape[1]))
    normed = (values * norm_rows * scale[...]).astype(BF16)
    raw = lax.dot_general(
        normed, step_t[...], (((1,), (1,)), ((), ())), preferred_element_type=F32
    )
    size = jax.nn.softplus(raw + bias[...])
    decay = extra[...] - jnp.exp(rate[...]) * size
    table[...] = jnp.zeros_like(table)
    small[...] = jnp.zeros_like(small)
    small[0:props, :] = jnp.exp(decay)
    total = []
    for j in range(props):
        row = decay[j : j + 1]
        total.append(row if j == 0 else total[-1] + row)
        table[j : j + 1, :] = jnp.exp(total[j])
    for i in range(props):
        own = size[i : i + 1]
        for j in range(i, props):
            at = (1 + i) * ROWS + j
            table[at : at + 1, :] = jnp.exp(total[j] - total[i]) * own
    at = (1 + props) * ROWS
    table[at : at + 1, :] = direct[...]
    width = coef.shape[-1]
    lane = lax.broadcasted_iota(jnp.int32, (heads, width), 1)
    head = lax.broadcasted_iota(jnp.int32, (heads, width), 0)
    spread = jnp.where(lane // head_dim == head, 1.0, 0.0).astype(F32)
    wide = jnp.dot(
        table[...], spread, preferred_element_type=F32, precision=lax.Precision.HIGHEST
    )
    for part in range(coef.shape[0]):
        coef[part] = wide[part * ROWS : (part + 1) * ROWS]


def state_body(accepted, states, history, taps, carry, early, taps_wide):
    count = accepted[0]
    heads, head_dim, size = states.shape[2:]
    groups = taps.shape[1]
    tap_count = taps.shape[0]
    inner = heads // groups * head_dim
    per = heads // groups

    def widen(rows, target, at):
        rows = rows.astype(F32)
        for g in range(groups):
            row = rows[g : g + 1]
            target[at : at + 1, g * inner : (g + 1) * inner] = row[:, :inner]
            for part in range(2):
                base = groups * inner + part * groups * size + g * size
                target[at : at + 1, base : base + size] = row[
                    :, inner + part * size : inner + (part + 1) * size
                ]

    taps_wide[...] = jnp.zeros_like(taps_wide)
    early[...] = jnp.zeros_like(early)
    for k in range(tap_count):
        widen(taps[k], taps_wide, k)
    for k in range(tap_count - 1):
        widen(history[0, count + k], early, k)
    context = early[...]
    before = tap_count - 1
    total = context * taps_wide[0:1, :]
    keep = lax.broadcasted_iota(jnp.int32, (ROWS, 1), 0) < before
    for k in range(1, before):
        total = total + jnp.where(keep, pltpu.roll(context, ROWS - k, 0), 0.0) * taps_wide[k : k + 1, :]
    early[...] = jnp.where(keep, total, 0.0)

    carry[...] = jnp.zeros_like(carry)
    pair = 128 // head_dim
    for g in range(groups):
        for block in range(per // pair):
            at = g * per + block * pair
            tile = states[0, count - 1, at : at + pair].reshape(pair * head_dim, size).T
            big, rest = split(tile)
            cols = slice(at * head_dim, (at + pair) * head_dim)
            carry[g * size : (g + 1) * size, cols] = big
            carry[(groups + g) * size : (groups + g + 1) * size, cols] = rest


def stack_rows(parts, lhs):
    lhs[...] = jnp.zeros_like(lhs)
    for j, part in enumerate(parts):
        lhs[4 * j : 4 * j + part.shape[0], :] = part[...].astype(F32)
    return lhs[...].astype(BF16)


def packed_width(props, width):
    return -(-props * width // 4 // 128) * 128


def project_body(count, props, *refs):
    slices = refs[:count]
    inputs, inject, readout, gates, scale = refs[count : count + 5]
    own = refs[count + 5]
    outs = refs[count + 6 : count + 5 + count]
    rows = refs[-1]
    depth = rows.shape[1]
    start = pl.multiple_of(lax.axis_index("kv") * depth, 128)
    stack_rows(slices, rows)
    lhs = (rows[...] * scale[:, pl.ds(start, depth)]).astype(BF16)
    wide = own.shape[1]
    first = inputs.shape[1]
    both = inject.shape[1] + readout.shape[1]
    left = wide - first - both
    rest = gates.shape[1] - left
    fourth = lax.broadcasted_iota(jnp.int32, (4, 1), 0) == 3

    result = jnp.dot(lhs, gates[...], preferred_element_type=F32)
    extra = result[:, left:]

    def store(at, values):
        width = values.shape[1]
        for j, out in enumerate((own, *outs)):
            block = values[4 * j : 4 * j + 4]
            for r in range(props):
                low, high = max(at, r * rest), min(at + width, (r + 1) * rest)
                if low < high:
                    row = extra[4 * j + r : 4 * j + r + 1, low - r * rest : high - r * rest]
                    part = block[:, low - at : high - at]
                    out[:, low:high] = jnp.where(fourth, row, part).astype(out.dtype)
            low = max(at, props * rest)
            if low < at + width:
                out[:, low : at + width] = block[:, low - at :].astype(out.dtype)

    store(first + both, result[:, :left])
    store(0, jnp.dot(lhs, inputs[...], preferred_element_type=F32))
    pair = jnp.concatenate([inject[...], readout[...]], axis=1)
    store(first, jnp.dot(lhs, pair, preferred_element_type=F32))


def mixer_body(props, groups, *refs):
    own, *rest = refs
    count = len(rest) - 11
    others = rest[:count]
    norm, coef, early, taps, carry, gain, gated, fresh, act, summed, norms = rest[count:]
    inner = gain.shape[1]
    conv = early.shape[1]
    per = inner // groups
    both = (conv - inner) // 2
    size = both // groups
    summed[...] = jnp.zeros_like(summed)
    total = own[...]
    for other in others:
        total = total + other[...].astype(F32)
    wide = total.shape[1]
    rest = summed.shape[1] - wide
    summed[0:props, :wide] = total[0:props]
    for r in range(props):
        summed[r : r + 1, wide:] = total[3:4, r * rest : (r + 1) * rest]
    summed[...] = (summed[...] * norm[:, 0:1]).astype(BF16).astype(F32)
    rows = summed[:, :conv]
    fresh[...] = rows
    tap_count = 4
    value = early[...] + rows * taps[tap_count - 1 : tap_count, :]
    for k in range(1, props):
        value = value + pltpu.roll(rows * taps[tap_count - 1 - k : tap_count - k, :], k, 0)
    value = silu(value)
    act[...] = value
    x = value[:, :inner]
    b = value[:, inner : inner + both]
    c = value[:, inner + both :]
    c_high, c_low = split(c)
    c_high, c_low = c_high.astype(F32), c_low.astype(F32)
    left = jnp.concatenate(
        [
            jnp.concatenate([c_high, c_high], axis=1),
            jnp.concatenate([c_low, jnp.zeros_like(c_low)], axis=1),
        ],
        axis=0,
    ).astype(BF16)
    carried = jnp.dot(left, carry[...], preferred_element_type=F32)
    carried = carried[:ROWS] + carried[ROWS:]
    lane = lax.broadcasted_iota(jnp.int32, (ROWS, both), 1)
    response = coef[0] * carried + coef[1 + props, 0:1, :] * x
    pieces = []
    weights = []
    for i in range(props):
        product = c * b[i : i + 1]
        weights.append(
            [
                jnp.sum(jnp.where(lane // size == g, product, 0.0), axis=1, keepdims=True)
                for g in range(groups)
            ]
        )
    gate = summed[:, conv:]
    gate = silu(gate)
    for g in range(groups):
        at = slice(g * per, (g + 1) * per)
        part = response[:, at]
        for i in range(props):
            part = part + coef[1 + i, :, at] * weights[i][g] * x[i : i + 1, at]
        part = part * gate[:, at]
        mean = jnp.sum(part * part, axis=1, keepdims=True) * (1.0 / per)
        pieces.append(part * lax.rsqrt(mean + epsilon) * gain[:, at])
    norms[...] = jnp.concatenate(pieces, axis=1)
    gated[...] = norms[0:4].astype(BF16)


def states_body(props, groups, pieces, accepted, start, small, act, coef, *refs):
    heads, head_dim, size = start.shape[2:]
    per = heads // groups
    last = pieces[-1][2] == per and pieces[-1][0] == groups - 1
    if last:
        fresh, history, _, states, tail_out, held, tail, sem = refs
    else:
        states, flag, held, sem = refs
        flag[...] = jnp.zeros_like(flag)
    copies = []
    inner = per * head_dim
    wide = heads * head_dim
    block = groups * size
    count = accepted[0]
    if last:
        before = tail.shape[1] - props
        for k in range(before):
            tail[0, k] = history[0, count + k]
        for j in range(props):
            rows = []
            for q in range(groups):
                row = [fresh[j : j + 1, q * inner : (q + 1) * inner]]
                for part in range(2):
                    base = wide + part * block + q * size
                    row.append(fresh[j : j + 1, base : base + size])
                rows.append(jnp.concatenate(row, axis=1))
            tail[0, before + j] = jnp.concatenate(rows, axis=0).astype(BF16)
        copy = pltpu.make_async_copy(tail, tail_out, sem.at[len(pieces)])
        copy.start()
        copies.append(copy)
    row_at = lax.broadcasted_iota(jnp.int32, (ROWS, 1), 0)
    b_high, b_low = split(act[:, wide : wide + block])
    b_high, b_low = b_high.astype(F32), b_low.astype(F32)
    filled = 0
    for g, low, high in pieces:
        lanes = slice(g * inner + low * head_dim, g * inner + high * head_dim)
        steps = jnp.zeros((ROWS, (high - low) * head_dim), F32)
        for j in range(props):
            steps = jnp.where(row_at == j, coef[1 + j, :, lanes], steps)
        dx = act[:, lanes] * steps
        dx_high, dx_low = split(dx)
        dx_high, dx_low = dx_high.astype(F32), dx_low.astype(F32)
        left = jnp.concatenate(
            [dx_high, dx_low, dx_high, jnp.zeros_like(dx)], axis=0
        ).astype(BF16)
        blocks = []
        for j in range(props):
            hi = jnp.where(row_at == j, b_high, 0.0)
            lo = jnp.where(row_at == j, b_low, 0.0)
            full = jnp.concatenate([hi, hi, lo, jnp.zeros_like(hi)], axis=0)
            if g:
                full = pltpu.roll(full, block - g * size, 1)
            blocks.append(full)
        right = jnp.concatenate(blocks, axis=1).astype(BF16)
        update = lax.dot_general(
            left, right, (((0,), (0,)), ((), ())), preferred_element_type=F32
        )
        for h in range(high - low):
            at = g * per + low + h
            state = start[0, count - 1, at]
            for j in range(props):
                new = update[h * head_dim : (h + 1) * head_dim, j * block : j * block + size]
                state = state * small[j : j + 1, at : at + 1] + new
                held[j, filled + h] = state
        copy = pltpu.make_async_copy(
            held.at[:, pl.ds(filled, high - low)],
            states.at[0, :, pl.ds(g * per + low, high - low)],
            sem.at[pieces.index((g, low, high))],
        )
        copy.start()
        copies.append(copy)
        filled += high - low
    for copy in copies:
        copy.wait()


def output_body(count, *refs):
    parts = refs[:count]
    weight = refs[count]
    outs = refs[count + 2 : count + 2 + count]
    result, lhs = refs[-2:]
    which = lax.bitwise_xor(lax.axis_index("kv"), lax.axis_index("tp"))
    product = jnp.dot(stack_rows(parts, lhs), weight[...], preferred_element_type=F32)
    for j in range(count):
        result[j, 0:4] = product[4 * j : 4 * j + 4]
    for step in range(count):
        outs[step][...] = result[lax.bitwise_xor(which, step), 0:4].astype(BF16)


def final_body(*refs):
    *parts, out = refs
    total = parts[0][...].astype(F32)
    for part in parts[1:]:
        total = total + part[...].astype(F32)
    out[0] = total[0 : out.shape[1]].astype(BF16)


def fast_local(
    count,
    tokens,
    input_norm_scale,
    head_input_matrix,
    output_gate_matrix,
    group_input_matrix,
    group_readout_matrix,
    step_size_matrix,
    step_size_bias,
    log_decay_rate,
    direct_path_weight,
    convolution_tap_weight,
    convolution_history_rows,
    per_proposal_states,
    accepted,
    proposal_extra_decay,
    group_norm_scale,
    output_projection_matrix,
):
    _, props, width = tokens.shape
    heads = step_size_bias.shape[0]
    _, _, groups, channels = convolution_history_rows.shape
    head_dim, size = per_proposal_states.shape[3:]
    inner = heads * head_dim
    conv = groups * channels
    rows = head_input_matrix.shape[0]
    total = conv + inner
    packed = packed_width(props, total)
    out_cols = output_projection_matrix.shape[1]

    slices = call(
        functools.partial(slice_body, count),
        [pltpu.VMEM((props, rows), BF16)] * count,
        [hbm(tokens)],
        [HBM_SPEC],
        scratch=[pltpu.SemaphoreType.DMA((count,))],
    )
    slices = call(
        hold_body,
        [pltpu.VMEM((props, rows), BF16)] * count,
        [vmem(v) for v in slices],
        [VMEM_SPEC] * count,
        flops=1_000_000_000_000,
        moved=10_000_000_000,
        aliases={i: i for i in range(count)},
    )
    received = exchange_tokens(slices, count)
    matrices = [head_input_matrix, group_input_matrix, group_readout_matrix, output_gate_matrix]

    scale = input_norm_scale.reshape(1, width)
    coef, small, norm = call(
        functools.partial(step_body, head_dim),
        [
            pltpu.VMEM((props + 2, ROWS, inner), F32),
            pltpu.VMEM((ROWS, heads), F32),
            pltpu.VMEM((ROWS, 128), F32),
        ],
        [
            accepted,
            vmem(tokens),
            vmem(scale),
            vmem(step_size_matrix.T),
            step_size_bias.reshape(1, heads),
            log_decay_rate.reshape(1, heads),
            direct_path_weight.reshape(1, heads),
            proposal_extra_decay.reshape(props, heads),
        ],
        [SMEM_SPEC] + [VMEM_SPEC] * 7,
        flops=20_000_000,
        scratch=[pltpu.VMEM(((props + 2) * ROWS, heads), F32)],
    )
    states = vmem(per_proposal_states)
    carry, early, taps = call(
        state_body,
        [
            pltpu.VMEM((2 * groups * size, inner), BF16),
            pltpu.VMEM((ROWS, conv), F32),
            pltpu.VMEM((ROWS, conv), F32),
        ],
        [accepted, states, convolution_history_rows, convolution_tap_weight],
        [SMEM_SPEC] + [VMEM_SPEC] * 3,
        flops=20_000_000,
    )

    own, *partials = call(
        functools.partial(project_body, count, props),
        [pltpu.VMEM((4, packed), F32)] + [pltpu.VMEM((4, packed), BF16)] * (count - 1),
        [vmem(s) for s in [slices[0]] + received]
        + matrices
        + [vmem(scale)],
        [VMEM_SPEC] * (count + 5),
        flops=200_000_000,
        scratch=[pltpu.VMEM((4 * count, rows), F32)],
    )
    sums = exchange([None] + partials, "kv", count)
    gated, fresh, act = call(
        functools.partial(mixer_body, props, groups),
        [
            pltpu.VMEM((4, inner), BF16),
            pltpu.VMEM((ROWS, conv), F32),
            pltpu.VMEM((ROWS, conv), F32),
        ],
        [vmem(v) for v in [own] + sums + [norm, coef, early, taps, carry]]
        + [vmem(group_norm_scale.reshape(1, inner))],
        [VMEM_SPEC] * (count + 6),
        flops=20_000_000,
        scratch=[pltpu.VMEM((ROWS, total), F32), pltpu.VMEM((ROWS, inner), F32)],
    )
    gathered = exchange([gated] * count, "kv", count)
    per = heads // groups
    half = per // 2
    pieces = [(g, at, at + half) for g in range(groups) for at in (0, half)]
    first = 3 * len(pieces) // 4
    all_states = jax.ShapeDtypeStruct((1, props, heads, head_dim, size), F32)

    def scratch(number, *more):
        shape = (props, number * half, head_dim, size)
        return [pltpu.VMEM(shape, F32), *more, pltpu.SemaphoreType.DMA((number + 1,))]

    new_states, flag = call(
        functools.partial(states_body, props, groups, pieces[:first]),
        [all_states, pltpu.VMEM((ROWS, 128), F32)],
        [accepted, states] + [vmem(v) for v in (small, act, coef)],
        [SMEM_SPEC] + [VMEM_SPEC] * 4,
        flops=30_000_000,
        out_specs=[HBM_SPEC, VMEM_SPEC],
        scratch=scratch(first),
    )
    new_states, new_tail = call(
        functools.partial(states_body, props, groups, pieces[first:]),
        [all_states, jax.ShapeDtypeStruct(convolution_history_rows.shape, BF16)],
        [accepted, states]
        + [vmem(v) for v in (small, act, coef, fresh, convolution_history_rows)]
        + [hbm(new_states)],
        [SMEM_SPEC] + [VMEM_SPEC] * 6 + [HBM_SPEC],
        flops=30_000_000,
        out_specs=[HBM_SPEC, HBM_SPEC],
        scratch=scratch(
            len(pieces) - first, pltpu.VMEM(convolution_history_rows.shape, BF16)
        ),
        aliases={7: 0},
    )
    blocks = call(
        functools.partial(output_body, count),
        [pltpu.VMEM((4, out_cols), BF16)] * count,
        [vmem(v) for v in [gated] + gathered + [output_projection_matrix, flag]],
        [VMEM_SPEC] * (count + 2),
        flops=100_000_000,
        scratch=[
            pltpu.VMEM((count, ROWS, out_cols), F32),
            pltpu.VMEM((4 * count, inner), F32),
        ],
    )
    last = exchange(blocks, "tp", count)
    (mixed,) = call(
        final_body,
        [jax.ShapeDtypeStruct((1, props, out_cols), BF16)],
        [vmem(v) for v in [blocks[0]] + last],
        [VMEM_SPEC] * count,
    )
    return (mixed, new_states, new_tail)


def rms_scale(values):
    return lax.rsqrt(jnp.mean(values * values, axis=-1, keepdims=True) + epsilon)


def causal_states(log_decay_factor, head_step_size, ssm_inputs, inject, start_state):
    cumulative = jnp.cumsum(log_decay_factor, axis=1)
    length = log_decay_factor.shape[1]
    lower = (jnp.arange(length)[:, None] >= jnp.arange(length)[None, :])[None, :, :, None]
    spread = cumulative[:, :, None, :] - cumulative[:, None, :, :]
    factors = jnp.where(lower, jnp.exp(jnp.where(lower, spread, 0.0)), 0.0)
    mixing = factors * head_step_size[:, None, :, :]
    carried = jnp.exp(cumulative)[..., None, None] * start_state[:, None]
    return carried + jnp.einsum("sjih,sihp,sihn->sjhpn", mixing, ssm_inputs, inject)


def combine_head_outputs(
    incoming_token_rows,
    gate_portion,
    unactivated_step,
    step_size_bias,
    log_decay_rate,
    direct_path_weight,
    convolution_tap_weight,
    convolution_history_rows,
    per_proposal_states,
    accepted,
    proposal_extra_decay,
    group_norm_scale,
):
    sequences, proposals, group_count, group_width = incoming_token_rows.shape
    head_count = step_size_bias.shape[0]
    head_dim = per_proposal_states.shape[3]
    state_size = per_proposal_states.shape[4]
    per_group = head_count // group_count
    group_inner = per_group * head_dim
    tap_count = convolution_tap_weight.shape[0]
    offsets = accepted[:, None] + jnp.arange(tap_count - 1, dtype=jnp.int32)[None, :]
    context = jnp.take_along_axis(convolution_history_rows, offsets[:, :, None, None], axis=1)
    convolution_span = jnp.concatenate([context, incoming_token_rows], axis=1)
    widened = convolution_span.astype(jnp.float32)
    convolved = jnp.zeros((sequences, proposals, group_count, group_width), jnp.float32)
    for conv_tap in range(tap_count):
        convolved = convolved + widened[
            :, conv_tap : conv_tap + proposals
        ] * convolution_tap_weight[conv_tap].astype(jnp.float32)
    activated = jax.nn.silu(convolved)
    ssm_inputs = activated[..., :group_inner].reshape(sequences, proposals, head_count, head_dim)
    inject = jnp.repeat(activated[..., group_inner : group_inner + state_size], per_group, axis=2)
    readout = jnp.repeat(activated[..., group_inner + state_size :], per_group, axis=2)
    head_step_size = jax.nn.softplus(unactivated_step + step_size_bias)
    log_decay_factor = proposal_extra_decay - jnp.exp(log_decay_rate) * head_step_size
    chosen = (accepted - 1)[:, None, None, None, None]
    start_state = jnp.take_along_axis(per_proposal_states, chosen, axis=1)[:, 0]
    running_state_rows = causal_states(
        log_decay_factor, head_step_size, ssm_inputs, inject, start_state
    )
    response = (
        jnp.einsum("sjhn,sjhpn->sjhp", readout, running_state_rows)
        + direct_path_weight[:, None] * ssm_inputs
    )
    gate_raw = gate_portion.astype(jnp.float32).reshape(sequences, proposals, head_count, head_dim)
    gate_applied_output = (response * jax.nn.silu(gate_raw)).reshape(
        sequences, proposals, group_count, group_inner
    )
    scaled = (
        gate_applied_output
        * rms_scale(gate_applied_output)
        * group_norm_scale.reshape(group_count, group_inner)
    )
    flat_gated = scaled.astype(jnp.bfloat16).reshape(sequences, proposals, head_count * head_dim)
    return (flat_gated, running_state_rows, convolution_span)


def local(
    tokens,
    input_norm_scale,
    head_input_matrix,
    output_gate_matrix,
    group_input_matrix,
    group_readout_matrix,
    step_size_matrix,
    step_size_bias,
    log_decay_rate,
    direct_path_weight,
    convolution_tap_weight,
    convolution_history_rows,
    per_proposal_states,
    accepted,
    proposal_extra_decay,
    group_norm_scale,
    output_projection_matrix,
):
    local_seqs, proposals, _ = tokens.shape
    head_local = step_size_bias.shape[0]
    group_local = convolution_tap_weight.shape[1]
    head_dim = per_proposal_states.shape[3]
    state_size = per_proposal_states.shape[4]
    group_inner = head_local // group_local * head_dim
    widened = tokens.astype(jnp.float32)
    normed = (widened * rms_scale(widened) * input_norm_scale).astype(jnp.bfloat16)
    unactivated_step = jnp.einsum(
        "sjd,dh->sjh", normed, step_size_matrix, preferred_element_type=jnp.float32
    )
    pieces = lax.all_to_all(normed, "kv", split_axis=2, concat_axis=0, tiled=True)
    joined = jnp.concatenate(
        [head_input_matrix, group_input_matrix, group_readout_matrix, output_gate_matrix], axis=1
    )
    summed = lax.psum_scatter(
        jnp.einsum("sjd,dc->sjc", pieces, joined, preferred_element_type=jnp.float32),
        "kv",
        scatter_dimension=0,
        tiled=True,
    )
    projected = summed.astype(jnp.bfloat16)
    input_width = head_local * head_dim
    inject_width = group_local * state_size
    part_input = projected[..., :input_width].reshape(
        local_seqs, proposals, group_local, group_inner
    )
    part_inject = projected[..., input_width : input_width + inject_width].reshape(
        local_seqs, proposals, group_local, state_size
    )
    part_readout = projected[
        ..., input_width + inject_width : input_width + 2 * inject_width
    ].reshape(local_seqs, proposals, group_local, state_size)
    gate_portion = projected[..., input_width + 2 * inject_width :]
    incoming_token_rows = jnp.concatenate([part_input, part_inject, part_readout], axis=-1)
    gate_applied_output, running_state_rows, convolution_span = combine_head_outputs(
        incoming_token_rows,
        gate_portion,
        unactivated_step,
        step_size_bias,
        log_decay_rate,
        direct_path_weight,
        convolution_tap_weight,
        convolution_history_rows,
        per_proposal_states,
        accepted,
        proposal_extra_decay,
        group_norm_scale,
    )
    terms = jnp.einsum(
        "sjc,cd->sjd",
        lax.all_gather(gate_applied_output, "kv", axis=0, tiled=True),
        output_projection_matrix,
        preferred_element_type=jnp.float32,
    )
    mixed = lax.psum_scatter(terms.astype(jnp.bfloat16), "tp", scatter_dimension=0, tiled=True)
    return (mixed, running_state_rows, convolution_span)


def chosen(mesh, *arguments):
    tokens, matrix = arguments[0], arguments[2]
    kv, tp = mesh.shape["kv"], mesh.shape["tp"]
    slim = tokens.shape[:2] == (1, 3) and matrix.shape[0] % 128 == 0
    slim = slim and arguments[10].shape[1] == 2
    if slim and kv == tp and kv in (2, 4):
        return fast_local(kv, *arguments)
    return local(*arguments)


def solution(mesh):
    return jax.shard_map(
        functools.partial(chosen, mesh),
        mesh=mesh,
        in_specs=(
            P(("grp", "kv"), None, None),
            P(),
            P("kv", "tp"),
            P("kv", "tp"),
            P("kv", "tp"),
            P("kv", "tp"),
            P(None, "tp"),
            P("tp"),
            P("tp"),
            P("tp"),
            P(None, "tp", None),
            P(("grp", "kv"), None, "tp", None),
            P(("grp", "kv"), None, "tp", None, None),
            P(("grp", "kv")),
            P(("grp", "kv"), None, "tp"),
            P("tp"),
            P("tp", "kv"),
        ),
        out_specs=(
            P(("grp", "tp"), None, "kv"),
            P(("grp", "kv"), None, "tp", None, None),
            P(("grp", "kv"), None, "tp", None),
        ),
        check_vma=False,
    )
```

```python
import functools

import jax
import jax.numpy as jnp
from jax import lax
from jax.experimental import pallas as pl
from jax.experimental.pallas import tpu as pltpu
from jax.sharding import PartitionSpec as P


epsilon = 1e-06
F32 = jnp.float32
BF16 = jnp.bfloat16
ROWS = 8


def vmem(x):
    return pltpu.with_memory_space_constraint(x, pltpu.VMEM)


def hbm(x):
    return pltpu.with_memory_space_constraint(x, pltpu.HBM)


VMEM_SPEC = pl.BlockSpec(memory_space=pltpu.VMEM)
SMEM_SPEC = pl.BlockSpec(memory_space=pltpu.SMEM)
HBM_SPEC = pl.BlockSpec(memory_space=pl.ANY)


def call(body, outs, ins, specs, flops=0, scratch=(), out_specs=None, limit=20 << 20, moved=0, aliases={}):
    return pl.pallas_call(
        body,
        out_shape=outs,
        in_specs=specs,
        out_specs=out_specs or [VMEM_SPEC] * len(outs),
        scratch_shapes=list(scratch),
        input_output_aliases=aliases,
        cost_estimate=pl.CostEstimate(flops=flops, transcendentals=0, bytes_accessed=moved),
        compiler_params=pltpu.CompilerParams(vmem_limit_bytes=limit),
    )(*ins)


def exchange_tokens(blocks, count):
    got = []
    for step in range(1, count):
        pairs = [
            (i * count + j, (i ^ step) * count + (j ^ 1))
            for i in range(count)
            for j in range(count)
        ]
        got.append(lax.ppermute(blocks[step], ("kv", "tp"), pairs))
    return got


def exchange_round(block, axis, count):
    got = []
    for step in range(1, count):
        pairs = [(i, (i + step) % count) for i in range(count)]
        got.append(lax.ppermute(block, axis, pairs))
    return got


def exchange(blocks, axis, count):
    got = []
    for step in reversed(range(1, count)):
        pairs = [(i, i ^ step) for i in range(count)]
        got.append(lax.ppermute(blocks[step], axis, pairs))
    return got[::-1]


def silu(v):
    return v * jax.nn.sigmoid(v)


def split(v):
    high = v.astype(BF16)
    return high, (v - high.astype(F32)).astype(BF16)


def slice_body(count, tokens, *refs):
    slices, sem = refs[:count], refs[-1]
    me = lax.axis_index("kv")
    width = slices[0].shape[1]
    copies = []
    for step in reversed(range(count)):
        start = pl.multiple_of(lax.bitwise_xor(me, step) * width, 128)
        copy = pltpu.make_async_copy(
            tokens.at[0, :, pl.ds(start, width)], slices[step], sem.at[step]
        )
        copy.start()
        copies.append(copy)
    for copy in copies:
        copy.wait()


def hold_body(*refs):
    pass


def step_body(head_dim, accepted, tokens, scale, step_t, bias, rate, direct, extra, coef, small, norm, table):
    props, heads = extra.shape
    values = tokens[0].astype(F32)
    norm_rows = lax.rsqrt(jnp.mean(values * values, axis=-1, keepdims=True) + epsilon)
    norm[...] = jnp.ones_like(norm)
    norm[0:props, :] = jnp.broadcast_to(norm_rows, (props, norm.shape[1]))
    normed = (values * norm_rows * scale[...]).astype(BF16)
    raw = lax.dot_general(
        normed, step_t[...], (((1,), (1,)), ((), ())), preferred_element_type=F32
    )
    size = jax.nn.softplus(raw + bias[...])
    decay = extra[...] - jnp.exp(rate[...]) * size
    table[...] = jnp.zeros_like(table)
    small[...] = jnp.zeros_like(small)
    small[0:props, :] = jnp.exp(decay)
    total = []
    for j in range(props):
        row = decay[j : j + 1]
        total.append(row if j == 0 else total[-1] + row)
        table[j : j + 1, :] = jnp.exp(total[j])
    for i in range(props):
        own = size[i : i + 1]
        for j in range(i, props):
            at = (1 + i) * ROWS + j
            table[at : at + 1, :] = jnp.exp(total[j] - total[i]) * own
    at = (1 + props) * ROWS
    table[at : at + 1, :] = direct[...]
    width = coef.shape[-1]
    lane = lax.broadcasted_iota(jnp.int32, (heads, width), 1)
    head = lax.broadcasted_iota(jnp.int32, (heads, width), 0)
    spread = jnp.where(lane // head_dim == head, 1.0, 0.0).astype(F32)
    wide = jnp.dot(
        table[...], spread, preferred_element_type=F32, precision=lax.Precision.HIGHEST
    )
    for part in range(coef.shape[0]):
        coef[part] = wide[part * ROWS : (part + 1) * ROWS]


def state_body(accepted, states, history, taps, carry, early, taps_wide):
    count = accepted[0]
    heads, head_dim, size = states.shape[2:]
    groups = taps.shape[1]
    tap_count = taps.shape[0]
    inner = heads // groups * head_dim
    per = heads // groups

    def widen(rows, target, at):
        rows = rows.astype(F32)
        for g in range(groups):
            row = rows[g : g + 1]
            target[at : at + 1, g * inner : (g + 1) * inner] = row[:, :inner]
            for part in range(2):
                base = groups * inner + part * groups * size + g * size
                target[at : at + 1, base : base + size] = row[
                    :, inner + part * size : inner + (part + 1) * size
                ]

    taps_wide[...] = jnp.zeros_like(taps_wide)
    early[...] = jnp.zeros_like(early)
    for k in range(tap_count):
        widen(taps[k], taps_wide, k)
    for k in range(tap_count - 1):
        widen(history[0, count + k], early, k)
    context = early[...]
    before = tap_count - 1
    total = context * taps_wide[0:1, :]
    keep = lax.broadcasted_iota(jnp.int32, (ROWS, 1), 0) < before
    for k in range(1, before):
        total = total + jnp.where(keep, pltpu.roll(context, ROWS - k, 0), 0.0) * taps_wide[k : k + 1, :]
    early[...] = jnp.where(keep, total, 0.0)

    carry[...] = jnp.zeros_like(carry)
    pair = 128 // head_dim
    for g in range(groups):
        for block in range(per // pair):
            at = g * per + block * pair
            tile = states[0, count - 1, at : at + pair].reshape(pair * head_dim, size).T
            big, rest = split(tile)
            cols = slice(at * head_dim, (at + pair) * head_dim)
            carry[g * size : (g + 1) * size, cols] = big
            carry[(groups + g) * size : (groups + g + 1) * size, cols] = rest


def stack_rows(parts, lhs):
    lhs[...] = jnp.zeros_like(lhs)
    for j, part in enumerate(parts):
        lhs[4 * j : 4 * j + part.shape[0], :] = part[...].astype(F32)
    return lhs[...].astype(BF16)


def packed_width(props, width):
    return -(-props * width // 4 // 128) * 128


def project_body(count, props, *refs):
    slices = refs[:count]
    inputs, inject, readout, gates, scale = refs[count : count + 5]
    own = refs[count + 5]
    outs = refs[count + 6 : count + 5 + count]
    rows = refs[-1]
    depth = rows.shape[1]
    start = pl.multiple_of(lax.axis_index("kv") * depth, 128)
    stack_rows(slices, rows)
    lhs = (rows[...] * scale[:, pl.ds(start, depth)]).astype(BF16)
    wide = own.shape[1]
    first = inputs.shape[1]
    both = inject.shape[1] + readout.shape[1]
    left = wide - first - both
    rest = gates.shape[1] - left
    fourth = lax.broadcasted_iota(jnp.int32, (4, 1), 0) == 3

    result = jnp.dot(lhs, gates[...], preferred_element_type=F32)
    extra = result[:, left:]

    def store(at, values):
        width = values.shape[1]
        for j, out in enumerate((own, *outs)):
            block = values[4 * j : 4 * j + 4]
            for r in range(props):
                low, high = max(at, r * rest), min(at + width, (r + 1) * rest)
                if low < high:
                    row = extra[4 * j + r : 4 * j + r + 1, low - r * rest : high - r * rest]
                    part = block[:, low - at : high - at]
                    out[:, low:high] = jnp.where(fourth, row, part).astype(out.dtype)
            low = max(at, props * rest)
            if low < at + width:
                out[:, low : at + width] = block[:, low - at :].astype(out.dtype)

    store(first + both, result[:, :left])
    store(0, jnp.dot(lhs, inputs[...], preferred_element_type=F32))
    pair = jnp.concatenate([inject[...], readout[...]], axis=1)
    store(first, jnp.dot(lhs, pair, preferred_element_type=F32))


def mixer_body(props, groups, tap_count, *refs):
    own, *rest = refs
    count = len(rest) - 11
    others = rest[:count]
    norm, coef, early, taps, carry, gain, gated, fresh, act, summed, norms = rest[count:]
    inner = gain.shape[1]
    conv = early.shape[1]
    per = inner // groups
    both = (conv - inner) // 2
    size = both // groups
    summed[...] = jnp.zeros_like(summed)
    total = own[...]
    for other in others:
        total = total + other[...].astype(F32)
    wide = total.shape[1]
    rest = summed.shape[1] - wide
    summed[0:props, :wide] = total[0:props]
    for r in range(props):
        summed[r : r + 1, wide:] = total[3:4, r * rest : (r + 1) * rest]
    summed[...] = (summed[...] * norm[:, 0:1]).astype(BF16).astype(F32)
    rows = summed[:, :conv]
    fresh[...] = rows
    value = early[...] + rows * taps[tap_count - 1 : tap_count, :]
    for k in range(1, props):
        value = value + pltpu.roll(rows * taps[tap_count - 1 - k : tap_count - k, :], k, 0)
    value = silu(value)
    act[...] = value
    x = value[:, :inner]
    b = value[:, inner : inner + both]
    c = value[:, inner + both :]
    c_high, c_low = split(c)
    c_high, c_low = c_high.astype(F32), c_low.astype(F32)
    left = jnp.concatenate(
        [
            jnp.concatenate([c_high, c_high], axis=1),
            jnp.concatenate([c_low, jnp.zeros_like(c_low)], axis=1),
        ],
        axis=0,
    ).astype(BF16)
    carried = jnp.dot(left, carry[...], preferred_element_type=F32)
    carried = carried[:ROWS] + carried[ROWS:]
    lane = lax.broadcasted_iota(jnp.int32, (ROWS, both), 1)
    response = coef[0] * carried + coef[1 + props, 0:1, :] * x
    pieces = []
    weights = []
    for i in range(props):
        product = c * b[i : i + 1]
        weights.append(
            [
                jnp.sum(jnp.where(lane // size == g, product, 0.0), axis=1, keepdims=True)
                for g in range(groups)
            ]
        )
    gate = summed[:, conv:]
    gate = silu(gate)
    for g in range(groups):
        at = slice(g * per, (g + 1) * per)
        part = response[:, at]
        for i in range(props):
            part = part + coef[1 + i, :, at] * weights[i][g] * x[i : i + 1, at]
        part = part * gate[:, at]
        mean = jnp.sum(part * part, axis=1, keepdims=True) * (1.0 / per)
        pieces.append(part * lax.rsqrt(mean + epsilon) * gain[:, at])
    norms[...] = jnp.concatenate(pieces, axis=1)
    gated[...] = norms[0:4].astype(BF16)


def states_body(props, groups, pieces, accepted, start, small, act, coef, *refs):
    heads, head_dim, size = start.shape[2:]
    per = heads // groups
    last = pieces[-1][2] == per and pieces[-1][0] == groups - 1
    if last:
        fresh, history, _, states, tail_out, held, tail, sem = refs
    else:
        states, flag, held, sem = refs
        flag[...] = jnp.zeros_like(flag)
    copies = []
    inner = per * head_dim
    wide = heads * head_dim
    block = groups * size
    count = accepted[0]
    if last:
        before = tail.shape[1] - props
        for k in range(before):
            tail[0, k] = history[0, count + k]
        for j in range(props):
            rows = []
            for q in range(groups):
                row = [fresh[j : j + 1, q * inner : (q + 1) * inner]]
                for part in range(2):
                    base = wide + part * block + q * size
                    row.append(fresh[j : j + 1, base : base + size])
                rows.append(jnp.concatenate(row, axis=1))
            tail[0, before + j] = jnp.concatenate(rows, axis=0).astype(BF16)
        copy = pltpu.make_async_copy(tail, tail_out, sem.at[len(pieces)])
        copy.start()
        copies.append(copy)
    row_at = lax.broadcasted_iota(jnp.int32, (ROWS, 1), 0)
    b_high, b_low = split(act[:, wide : wide + block])
    b_high, b_low = b_high.astype(F32), b_low.astype(F32)
    filled = 0
    for g, low, high in pieces:
        lanes = slice(g * inner + low * head_dim, g * inner + high * head_dim)
        steps = jnp.zeros((ROWS, (high - low) * head_dim), F32)
        for j in range(props):
            steps = jnp.where(row_at == j, coef[1 + j, :, lanes], steps)
        dx = act[:, lanes] * steps
        dx_high, dx_low = split(dx)
        dx_high, dx_low = dx_high.astype(F32), dx_low.astype(F32)
        left = jnp.concatenate(
            [dx_high, dx_low, dx_high, jnp.zeros_like(dx)], axis=0
        ).astype(BF16)
        blocks = []
        for j in range(props):
            hi = jnp.where(row_at == j, b_high, 0.0)
            lo = jnp.where(row_at == j, b_low, 0.0)
            full = jnp.concatenate([hi, hi, lo, jnp.zeros_like(hi)], axis=0)
            if g:
                full = pltpu.roll(full, block - g * size, 1)
            blocks.append(full)
        right = jnp.concatenate(blocks, axis=1).astype(BF16)
        update = lax.dot_general(
            left, right, (((0,), (0,)), ((), ())), preferred_element_type=F32
        )
        for h in range(high - low):
            at = g * per + low + h
            state = start[0, count - 1, at]
            for j in range(props):
                new = update[h * head_dim : (h + 1) * head_dim, j * block : j * block + size]
                state = state * small[j : j + 1, at : at + 1] + new
                held[j, filled + h] = state
        copy = pltpu.make_async_copy(
            held.at[:, pl.ds(filled, high - low)],
            states.at[0, :, pl.ds(g * per + low, high - low)],
            sem.at[pieces.index((g, low, high))],
        )
        copy.start()
        copies.append(copy)
        filled += high - low
    for copy in copies:
        copy.wait()


def output_body(count, *refs):
    parts = refs[:count]
    weight = refs[count]
    outs = refs[count + 2 : count + 2 + count]
    result, lhs = refs[-2:]
    me, part = lax.axis_index("kv"), lax.axis_index("tp")
    product = jnp.dot(stack_rows(parts, lhs), weight[...], preferred_element_type=F32)
    for j in range(count):
        result[j, 0:4] = product[4 * j : 4 * j + 4]
    for step in range(count):
        places = lax.rem(me - lax.bitwise_xor(part, step) + count, count)
        outs[step][...] = result[places, 0:4].astype(BF16)


def final_body(*refs):
    *parts, out = refs
    total = parts[0][...].astype(F32)
    for part in parts[1:]:
        total = total + part[...].astype(F32)
    out[0] = total[0 : out.shape[1]].astype(BF16)


def fast_local(
    count,
    tokens,
    input_norm_scale,
    head_input_matrix,
    output_gate_matrix,
    group_input_matrix,
    group_readout_matrix,
    step_size_matrix,
    step_size_bias,
    log_decay_rate,
    direct_path_weight,
    convolution_tap_weight,
    convolution_history_rows,
    per_proposal_states,
    accepted,
    proposal_extra_decay,
    group_norm_scale,
    output_projection_matrix,
):
    _, props, width = tokens.shape
    heads = step_size_bias.shape[0]
    _, _, groups, channels = convolution_history_rows.shape
    head_dim, size = per_proposal_states.shape[3:]
    inner = heads * head_dim
    conv = groups * channels
    rows = head_input_matrix.shape[0]
    total = conv + inner
    packed = packed_width(props, total)
    out_cols = output_projection_matrix.shape[1]

    slices = call(
        functools.partial(slice_body, count),
        [pltpu.VMEM((props, rows), BF16)] * count,
        [hbm(tokens)],
        [HBM_SPEC],
        scratch=[pltpu.SemaphoreType.DMA((count,))],
    )
    slices = call(
        hold_body,
        [pltpu.VMEM((props, rows), BF16)] * count,
        [vmem(v) for v in slices],
        [VMEM_SPEC] * count,
        flops=1_000_000_000_000,
        moved=10_000_000_000,
        aliases={i: i for i in range(count)},
    )
    received = exchange_tokens(slices, count)
    matrices = [head_input_matrix, group_input_matrix, group_readout_matrix, output_gate_matrix]

    scale = input_norm_scale.reshape(1, width)
    coef, small, norm = call(
        functools.partial(step_body, head_dim),
        [
            pltpu.VMEM((props + 2, ROWS, inner), F32),
            pltpu.VMEM((ROWS, heads), F32),
            pltpu.VMEM((ROWS, 128), F32),
        ],
        [
            accepted,
            vmem(tokens),
            vmem(scale),
            vmem(step_size_matrix.T),
            step_size_bias.reshape(1, heads),
            log_decay_rate.reshape(1, heads),
            direct_path_weight.reshape(1, heads),
            proposal_extra_decay.reshape(props, heads),
        ],
        [SMEM_SPEC] + [VMEM_SPEC] * 7,
        flops=20_000_000,
        scratch=[pltpu.VMEM(((props + 2) * ROWS, heads), F32)],
    )
    states = vmem(per_proposal_states)
    carry, early, taps = call(
        state_body,
        [
            pltpu.VMEM((2 * groups * size, inner), BF16),
            pltpu.VMEM((ROWS, conv), F32),
            pltpu.VMEM((ROWS, conv), F32),
        ],
        [accepted, states, convolution_history_rows, convolution_tap_weight],
        [SMEM_SPEC] + [VMEM_SPEC] * 3,
        flops=20_000_000,
    )

    own, *partials = call(
        functools.partial(project_body, count, props),
        [pltpu.VMEM((4, packed), F32)] + [pltpu.VMEM((4, packed), BF16)] * (count - 1),
        [vmem(s) for s in [slices[0]] + received]
        + matrices
        + [vmem(scale)],
        [VMEM_SPEC] * (count + 5),
        flops=200_000_000,
        scratch=[pltpu.VMEM((4 * count, rows), F32)],
    )
    sums = exchange([None] + partials, "kv", count)
    gated, fresh, act = call(
        functools.partial(mixer_body, props, groups, convolution_tap_weight.shape[0]),
        [
            pltpu.VMEM((4, inner), BF16),
            pltpu.VMEM((ROWS, conv), F32),
            pltpu.VMEM((ROWS, conv), F32),
        ],
        [vmem(v) for v in [own] + sums + [norm, coef, early, taps, carry]]
        + [vmem(group_norm_scale.reshape(1, inner))],
        [VMEM_SPEC] * (count + 6),
        flops=20_000_000,
        scratch=[pltpu.VMEM((ROWS, total), F32), pltpu.VMEM((ROWS, inner), F32)],
    )
    gathered = exchange_round(gated, "kv", count)
    per = heads // groups
    half = per // 2
    pieces = [(g, at, at + half) for g in range(groups) for at in (0, half)]
    first = len(pieces) // 4
    all_states = jax.ShapeDtypeStruct((1, props, heads, head_dim, size), F32)

    def scratch(number, *more):
        shape = (props, number * half, head_dim, size)
        return [pltpu.VMEM(shape, F32), *more, pltpu.SemaphoreType.DMA((number + 1,))]

    new_states, flag = call(
        functools.partial(states_body, props, groups, pieces[:first]),
        [all_states, pltpu.VMEM((ROWS, 128), F32)],
        [accepted, states] + [vmem(v) for v in (small, act, coef)],
        [SMEM_SPEC] + [VMEM_SPEC] * 4,
        flops=30_000_000,
        out_specs=[HBM_SPEC, VMEM_SPEC],
        scratch=scratch(first),
    )
    new_states, new_tail = call(
        functools.partial(states_body, props, groups, pieces[first:]),
        [all_states, jax.ShapeDtypeStruct(convolution_history_rows.shape, BF16)],
        [accepted, states]
        + [vmem(v) for v in (small, act, coef, fresh, convolution_history_rows)]
        + [hbm(new_states)],
        [SMEM_SPEC] + [VMEM_SPEC] * 6 + [HBM_SPEC],
        flops=30_000_000,
        out_specs=[HBM_SPEC, HBM_SPEC],
        scratch=scratch(
            len(pieces) - first, pltpu.VMEM(convolution_history_rows.shape, BF16)
        ),
        aliases={7: 0},
    )
    blocks = call(
        functools.partial(output_body, count),
        [pltpu.VMEM((4, out_cols), BF16)] * count,
        [vmem(v) for v in [gated] + gathered + [output_projection_matrix, flag]],
        [VMEM_SPEC] * (count + 2),
        flops=100_000_000,
        scratch=[
            pltpu.VMEM((count, ROWS, out_cols), F32),
            pltpu.VMEM((4 * count, inner), F32),
        ],
    )
    last = exchange(blocks, "tp", count)
    (mixed,) = call(
        final_body,
        [jax.ShapeDtypeStruct((1, props, out_cols), BF16)],
        [vmem(v) for v in [blocks[0]] + last],
        [VMEM_SPEC] * count,
    )
    return (mixed, new_states, new_tail)


def rms_scale(values):
    return lax.rsqrt(jnp.mean(values * values, axis=-1, keepdims=True) + epsilon)


def causal_states(log_decay_factor, head_step_size, ssm_inputs, inject, start_state):
    cumulative = jnp.cumsum(log_decay_factor, axis=1)
    length = log_decay_factor.shape[1]
    lower = (jnp.arange(length)[:, None] >= jnp.arange(length)[None, :])[None, :, :, None]
    spread = cumulative[:, :, None, :] - cumulative[:, None, :, :]
    factors = jnp.where(lower, jnp.exp(jnp.where(lower, spread, 0.0)), 0.0)
    mixing = factors * head_step_size[:, None, :, :]
    carried = jnp.exp(cumulative)[..., None, None] * start_state[:, None]
    return carried + jnp.einsum("sjih,sihp,sihn->sjhpn", mixing, ssm_inputs, inject)


def combine_head_outputs(
    incoming_token_rows,
    gate_portion,
    unactivated_step,
    step_size_bias,
    log_decay_rate,
    direct_path_weight,
    convolution_tap_weight,
    convolution_history_rows,
    per_proposal_states,
    accepted,
    proposal_extra_decay,
    group_norm_scale,
):
    sequences, proposals, group_count, group_width = incoming_token_rows.shape
    head_count = step_size_bias.shape[0]
    head_dim = per_proposal_states.shape[3]
    state_size = per_proposal_states.shape[4]
    per_group = head_count // group_count
    group_inner = per_group * head_dim
    tap_count = convolution_tap_weight.shape[0]
    offsets = accepted[:, None] + jnp.arange(tap_count - 1, dtype=jnp.int32)[None, :]
    context = jnp.take_along_axis(convolution_history_rows, offsets[:, :, None, None], axis=1)
    convolution_span = jnp.concatenate([context, incoming_token_rows], axis=1)
    widened = convolution_span.astype(jnp.float32)
    convolved = jnp.zeros((sequences, proposals, group_count, group_width), jnp.float32)
    for conv_tap in range(tap_count):
        convolved = convolved + widened[
            :, conv_tap : conv_tap + proposals
        ] * convolution_tap_weight[conv_tap].astype(jnp.float32)
    activated = jax.nn.silu(convolved)
    ssm_inputs = activated[..., :group_inner].reshape(sequences, proposals, head_count, head_dim)
    inject = jnp.repeat(activated[..., group_inner : group_inner + state_size], per_group, axis=2)
    readout = jnp.repeat(activated[..., group_inner + state_size :], per_group, axis=2)
    head_step_size = jax.nn.softplus(unactivated_step + step_size_bias)
    log_decay_factor = proposal_extra_decay - jnp.exp(log_decay_rate) * head_step_size
    chosen = (accepted - 1)[:, None, None, None, None]
    start_state = jnp.take_along_axis(per_proposal_states, chosen, axis=1)[:, 0]
    running_state_rows = causal_states(
        log_decay_factor, head_step_size, ssm_inputs, inject, start_state
    )
    response = (
        jnp.einsum("sjhn,sjhpn->sjhp", readout, running_state_rows)
        + direct_path_weight[:, None] * ssm_inputs
    )
    gate_raw = gate_portion.astype(jnp.float32).reshape(sequences, proposals, head_count, head_dim)
    gate_applied_output = (response * jax.nn.silu(gate_raw)).reshape(
        sequences, proposals, group_count, group_inner
    )
    scaled = (
        gate_applied_output
        * rms_scale(gate_applied_output)
        * group_norm_scale.reshape(group_count, group_inner)
    )
    flat_gated = scaled.astype(jnp.bfloat16).reshape(sequences, proposals, head_count * head_dim)
    return (flat_gated, running_state_rows, convolution_span)


def local(
    tokens,
    input_norm_scale,
    head_input_matrix,
    output_gate_matrix,
    group_input_matrix,
    group_readout_matrix,
    step_size_matrix,
    step_size_bias,
    log_decay_rate,
    direct_path_weight,
    convolution_tap_weight,
    convolution_history_rows,
    per_proposal_states,
    accepted,
    proposal_extra_decay,
    group_norm_scale,
    output_projection_matrix,
):
    local_seqs, proposals, _ = tokens.shape
    head_local = step_size_bias.shape[0]
    group_local = convolution_tap_weight.shape[1]
    head_dim = per_proposal_states.shape[3]
    state_size = per_proposal_states.shape[4]
    group_inner = head_local // group_local * head_dim
    widened = tokens.astype(jnp.float32)
    normed = (widened * rms_scale(widened) * input_norm_scale).astype(jnp.bfloat16)
    unactivated_step = jnp.einsum(
        "sjd,dh->sjh", normed, step_size_matrix, preferred_element_type=jnp.float32
    )
    pieces = lax.all_to_all(normed, "kv", split_axis=2, concat_axis=0, tiled=True)
    joined = jnp.concatenate(
        [head_input_matrix, group_input_matrix, group_readout_matrix, output_gate_matrix], axis=1
    )
    summed = lax.psum_scatter(
        jnp.einsum("sjd,dc->sjc", pieces, joined, preferred_element_type=jnp.float32),
        "kv",
        scatter_dimension=0,
        tiled=True,
    )
    projected = summed.astype(jnp.bfloat16)
    input_width = head_local * head_dim
    inject_width = group_local * state_size
    part_input = projected[..., :input_width].reshape(
        local_seqs, proposals, group_local, group_inner
    )
    part_inject = projected[..., input_width : input_width + inject_width].reshape(
        local_seqs, proposals, group_local, state_size
    )
    part_readout = projected[
        ..., input_width + inject_width : input_width + 2 * inject_width
    ].reshape(local_seqs, proposals, group_local, state_size)
    gate_portion = projected[..., input_width + 2 * inject_width :]
    incoming_token_rows = jnp.concatenate([part_input, part_inject, part_readout], axis=-1)
    gate_applied_output, running_state_rows, convolution_span = combine_head_outputs(
        incoming_token_rows,
        gate_portion,
        unactivated_step,
        step_size_bias,
        log_decay_rate,
        direct_path_weight,
        convolution_tap_weight,
        convolution_history_rows,
        per_proposal_states,
        accepted,
        proposal_extra_decay,
        group_norm_scale,
    )
    terms = jnp.einsum(
        "sjc,cd->sjd",
        lax.all_gather(gate_applied_output, "kv", axis=0, tiled=True),
        output_projection_matrix,
        preferred_element_type=jnp.float32,
    )
    mixed = lax.psum_scatter(terms.astype(jnp.bfloat16), "tp", scatter_dimension=0, tiled=True)
    return (mixed, running_state_rows, convolution_span)


def chosen(mesh, *arguments):
    tokens, matrix = arguments[0], arguments[2]
    kv, tp = mesh.shape["kv"], mesh.shape["tp"]
    slim = tokens.shape[:2] == (1, 3) and matrix.shape[0] % 128 == 0
    slim = slim and arguments[10].shape[1] == 2
    if slim and kv == tp and kv in (2, 4):
        return fast_local(kv, *arguments)
    return local(*arguments)


def solution(mesh):
    return jax.shard_map(
        functools.partial(chosen, mesh),
        mesh=mesh,
        in_specs=(
            P(("grp", "kv"), None, None),
            P(),
            P("kv", "tp"),
            P("kv", "tp"),
            P("kv", "tp"),
            P("kv", "tp"),
            P(None, "tp"),
            P("tp"),
            P("tp"),
            P("tp"),
            P(None, "tp", None),
            P(("grp", "kv"), None, "tp", None),
            P(("grp", "kv"), None, "tp", None, None),
            P(("grp", "kv")),
            P(("grp", "kv"), None, "tp"),
            P("tp"),
            P("tp", "kv"),
        ),
        out_specs=(
            P(("grp", "tp"), None, "kv"),
            P(("grp", "kv"), None, "tp", None, None),
            P(("grp", "kv"), None, "tp", None),
        ),
        check_vma=False,
    )
```

```python
import functools

import jax
import jax.numpy as jnp
from jax import lax
from jax.experimental import pallas as pl
from jax.experimental.pallas import tpu as pltpu
from jax.sharding import PartitionSpec as P


epsilon = 1e-06
F32 = jnp.float32
BF16 = jnp.bfloat16
ROWS = 8


def vmem(x):
    return pltpu.with_memory_space_constraint(x, pltpu.VMEM)


def hbm(x):
    return pltpu.with_memory_space_constraint(x, pltpu.HBM)


VMEM_SPEC = pl.BlockSpec(memory_space=pltpu.VMEM)
SMEM_SPEC = pl.BlockSpec(memory_space=pltpu.SMEM)
HBM_SPEC = pl.BlockSpec(memory_space=pl.ANY)


def call(body, outs, ins, specs, flops=0, scratch=(), out_specs=None, limit=20 << 20, moved=0, aliases={}):
    return pl.pallas_call(
        body,
        out_shape=outs,
        in_specs=specs,
        out_specs=out_specs or [VMEM_SPEC] * len(outs),
        scratch_shapes=list(scratch),
        input_output_aliases=aliases,
        cost_estimate=pl.CostEstimate(flops=flops, transcendentals=0, bytes_accessed=moved),
        compiler_params=pltpu.CompilerParams(vmem_limit_bytes=limit),
    )(*ins)


def exchange_tokens(blocks, count):
    got = []
    for step in range(1, count):
        pairs = [
            (i * count + j, (i ^ step) * count + (j ^ 1))
            for i in range(count)
            for j in range(count)
        ]
        got.append(lax.ppermute(blocks[step], ("kv", "tp"), pairs))
    return got


def exchange_round(block, axis, count):
    got = []
    for step in range(1, count):
        pairs = [(i, (i + step) % count) for i in range(count)]
        got.append(lax.ppermute(block, axis, pairs))
    return got


def exchange(blocks, axis, count):
    got = []
    for step in reversed(range(1, count)):
        pairs = [(i, i ^ step) for i in range(count)]
        got.append(lax.ppermute(blocks[step], axis, pairs))
    return got[::-1]


def silu(v):
    return v * jax.nn.sigmoid(v)


def split(v):
    high = v.astype(BF16)
    return high, (v - high.astype(F32)).astype(BF16)


def slice_body(count, tokens, *refs):
    slices, sem = refs[:count], refs[-1]
    me = lax.axis_index("kv")
    width = slices[0].shape[1]
    copies = []
    for step in reversed(range(count)):
        start = pl.multiple_of(lax.bitwise_xor(me, step) * width, 128)
        copy = pltpu.make_async_copy(
            tokens.at[0, :, pl.ds(start, width)], slices[step], sem.at[step]
        )
        copy.start()
        copies.append(copy)
    for copy in copies:
        copy.wait()


def hold_body(*refs):
    pass


def step_body(head_dim, accepted, tokens, scale, step_t, bias, rate, direct, extra, coef, small, norm, table):
    props, heads = extra.shape
    values = tokens[0].astype(F32)
    norm_rows = lax.rsqrt(jnp.mean(values * values, axis=-1, keepdims=True) + epsilon)
    norm[...] = jnp.ones_like(norm)
    norm[0:props, :] = jnp.broadcast_to(norm_rows, (props, norm.shape[1]))
    normed = (values * norm_rows * scale[...]).astype(BF16)
    raw = lax.dot_general(
        normed, step_t[...], (((1,), (1,)), ((), ())), preferred_element_type=F32
    )
    size = jax.nn.softplus(raw + bias[...])
    decay = extra[...] - jnp.exp(rate[...]) * size
    table[...] = jnp.zeros_like(table)
    small[...] = jnp.zeros_like(small)
    small[0:props, :] = jnp.exp(decay)
    total = []
    for j in range(props):
        row = decay[j : j + 1]
        total.append(row if j == 0 else total[-1] + row)
        table[j : j + 1, :] = jnp.exp(total[j])
    for i in range(props):
        own = size[i : i + 1]
        for j in range(i, props):
            at = (1 + i) * ROWS + j
            table[at : at + 1, :] = jnp.exp(total[j] - total[i]) * own
    at = (1 + props) * ROWS
    table[at : at + 1, :] = direct[...]
    width = coef.shape[-1]
    lane = lax.broadcasted_iota(jnp.int32, (heads, width), 1)
    head = lax.broadcasted_iota(jnp.int32, (heads, width), 0)
    spread = jnp.where(lane // head_dim == head, 1.0, 0.0).astype(F32)
    wide = jnp.dot(
        table[...], spread, preferred_element_type=F32, precision=lax.Precision.HIGHEST
    )
    for part in range(coef.shape[0]):
        coef[part] = wide[part * ROWS : (part + 1) * ROWS]


def state_body(accepted, states, history, taps, carry, early, taps_wide):
    count = accepted[0]
    heads, head_dim, size = states.shape[2:]
    groups = taps.shape[1]
    tap_count = taps.shape[0]
    inner = heads // groups * head_dim
    per = heads // groups

    def widen(rows, target, at):
        rows = rows.astype(F32)
        for g in range(groups):
            row = rows[g : g + 1]
            target[at : at + 1, g * inner : (g + 1) * inner] = row[:, :inner]
            for part in range(2):
                base = groups * inner + part * groups * size + g * size
                target[at : at + 1, base : base + size] = row[
                    :, inner + part * size : inner + (part + 1) * size
                ]

    taps_wide[...] = jnp.zeros_like(taps_wide)
    early[...] = jnp.zeros_like(early)
    for k in range(tap_count):
        widen(taps[k], taps_wide, k)
    for k in range(tap_count - 1):
        widen(history[0, count + k], early, k)
    context = early[...]
    before = tap_count - 1
    total = context * taps_wide[0:1, :]
    keep = lax.broadcasted_iota(jnp.int32, (ROWS, 1), 0) < before
    for k in range(1, before):
        total = total + jnp.where(keep, pltpu.roll(context, ROWS - k, 0), 0.0) * taps_wide[k : k + 1, :]
    early[...] = jnp.where(keep, total, 0.0)

    carry[...] = jnp.zeros_like(carry)
    pair = 128 // head_dim
    for g in range(groups):
        for block in range(per // pair):
            at = g * per + block * pair
            tile = states[0, count - 1, at : at + pair].reshape(pair * head_dim, size).T
            big, rest = split(tile)
            cols = slice(at * head_dim, (at + pair) * head_dim)
            carry[g * size : (g + 1) * size, cols] = big
            carry[(groups + g) * size : (groups + g + 1) * size, cols] = rest


def stack_rows(parts, lhs):
    lhs[...] = jnp.zeros_like(lhs)
    for j, part in enumerate(parts):
        lhs[4 * j : 4 * j + part.shape[0], :] = part[...].astype(F32)
    return lhs[...].astype(BF16)


def packed_width(props, width):
    return -(-props * width // 4 // 128) * 128


def project_body(count, props, *refs):
    slices = refs[:count]
    inputs, inject, readout, gates, scale = refs[count : count + 5]
    own = refs[count + 5]
    outs = refs[count + 6 : count + 5 + count]
    rows = refs[-1]
    depth = rows.shape[1]
    start = pl.multiple_of(lax.axis_index("kv") * depth, 128)
    stack_rows(slices, rows)
    lhs = (rows[...] * scale[:, pl.ds(start, depth)]).astype(BF16)
    wide = own.shape[1]
    first = inputs.shape[1]
    both = inject.shape[1] + readout.shape[1]
    left = wide - first - both
    rest = gates.shape[1] - left
    fourth = lax.broadcasted_iota(jnp.int32, (4, 1), 0) == 3

    result = jnp.dot(lhs, gates[...], preferred_element_type=F32)
    extra = result[:, left:]

    def store(at, values):
        width = values.shape[1]
        for j, out in enumerate((own, *outs)):
            block = values[4 * j : 4 * j + 4]
            for r in range(props):
                low, high = max(at, r * rest), min(at + width, (r + 1) * rest)
                if low < high:
                    row = extra[4 * j + r : 4 * j + r + 1, low - r * rest : high - r * rest]
                    part = block[:, low - at : high - at]
                    out[:, low:high] = jnp.where(fourth, row, part).astype(out.dtype)
            low = max(at, props * rest)
            if low < at + width:
                out[:, low : at + width] = block[:, low - at :].astype(out.dtype)

    store(first + both, result[:, :left])
    store(0, jnp.dot(lhs, inputs[...], preferred_element_type=F32))
    pair = jnp.concatenate([inject[...], readout[...]], axis=1)
    store(first, jnp.dot(lhs, pair, preferred_element_type=F32))


def mixer_body(props, groups, tap_count, *refs):
    own, *rest = refs
    count = len(rest) - 11
    others = rest[:count]
    norm, coef, early, taps, carry, gain, gated, fresh, act, summed, norms = rest[count:]
    inner = gain.shape[1]
    conv = early.shape[1]
    per = inner // groups
    both = (conv - inner) // 2
    size = both // groups
    summed[...] = jnp.zeros_like(summed)
    total = own[...]
    for other in others:
        total = total + other[...].astype(F32)
    wide = total.shape[1]
    rest = summed.shape[1] - wide
    summed[0:props, :wide] = total[0:props]
    for r in range(props):
        summed[r : r + 1, wide:] = total[3:4, r * rest : (r + 1) * rest]
    summed[...] = (summed[...] * norm[:, 0:1]).astype(BF16).astype(F32)
    rows = summed[:, :conv]
    fresh[...] = rows
    value = early[...] + rows * taps[tap_count - 1 : tap_count, :]
    for k in range(1, props):
        value = value + pltpu.roll(rows * taps[tap_count - 1 - k : tap_count - k, :], k, 0)
    value = silu(value)
    act[...] = value
    x = value[:, :inner]
    b = value[:, inner : inner + both]
    c = value[:, inner + both :]
    c_high, c_low = split(c)
    c_high, c_low = c_high.astype(F32), c_low.astype(F32)
    left = jnp.concatenate(
        [
            jnp.concatenate([c_high, c_high], axis=1),
            jnp.concatenate([c_low, jnp.zeros_like(c_low)], axis=1),
        ],
        axis=0,
    ).astype(BF16)
    carried = jnp.dot(left, carry[...], preferred_element_type=F32)
    carried = carried[:ROWS] + carried[ROWS:]
    lane = lax.broadcasted_iota(jnp.int32, (ROWS, both), 1)
    response = coef[0] * carried + coef[1 + props, 0:1, :] * x
    pieces = []
    weights = []
    for i in range(props):
        product = c * b[i : i + 1]
        weights.append(
            [
                jnp.sum(jnp.where(lane // size == g, product, 0.0), axis=1, keepdims=True)
                for g in range(groups)
            ]
        )
    gate = summed[:, conv:]
    gate = silu(gate)
    for g in range(groups):
        at = slice(g * per, (g + 1) * per)
        part = response[:, at]
        for i in range(props):
            part = part + coef[1 + i, :, at] * weights[i][g] * x[i : i + 1, at]
        part = part * gate[:, at]
        mean = jnp.sum(part * part, axis=1, keepdims=True) * (1.0 / per)
        pieces.append(part * lax.rsqrt(mean + epsilon) * gain[:, at])
    norms[...] = jnp.concatenate(pieces, axis=1)
    wide = gated.shape[1]
    rest = inner - wide
    for r in range(props):
        norms[3:4, r * rest : (r + 1) * rest] = norms[r : r + 1, wide:]
    gated[...] = norms[0:4, :wide].astype(BF16)


def states_body(props, groups, pieces, accepted, start, small, act, coef, *refs):
    heads, head_dim, size = start.shape[2:]
    per = heads // groups
    last = pieces[-1][2] == per and pieces[-1][0] == groups - 1
    if last:
        fresh, history, _, states, tail_out, held, tail, sem = refs
    else:
        states, flag, held, sem = refs
        flag[...] = jnp.zeros_like(flag)
    copies = []
    inner = per * head_dim
    wide = heads * head_dim
    block = groups * size
    count = accepted[0]
    if last:
        before = tail.shape[1] - props
        for k in range(before):
            tail[0, k] = history[0, count + k]
        for j in range(props):
            rows = []
            for q in range(groups):
                row = [fresh[j : j + 1, q * inner : (q + 1) * inner]]
                for part in range(2):
                    base = wide + part * block + q * size
                    row.append(fresh[j : j + 1, base : base + size])
                rows.append(jnp.concatenate(row, axis=1))
            tail[0, before + j] = jnp.concatenate(rows, axis=0).astype(BF16)
        copy = pltpu.make_async_copy(tail, tail_out, sem.at[len(pieces)])
        copy.start()
        copies.append(copy)
    row_at = lax.broadcasted_iota(jnp.int32, (ROWS, 1), 0)
    b_high, b_low = split(act[:, wide : wide + block])
    b_high, b_low = b_high.astype(F32), b_low.astype(F32)
    filled = 0
    for g, low, high in pieces:
        lanes = slice(g * inner + low * head_dim, g * inner + high * head_dim)
        steps = jnp.zeros((ROWS, (high - low) * head_dim), F32)
        for j in range(props):
            steps = jnp.where(row_at == j, coef[1 + j, :, lanes], steps)
        dx = act[:, lanes] * steps
        dx_high, dx_low = split(dx)
        dx_high, dx_low = dx_high.astype(F32), dx_low.astype(F32)
        left = jnp.concatenate(
            [dx_high, dx_low, dx_high, jnp.zeros_like(dx)], axis=0
        ).astype(BF16)
        blocks = []
        for j in range(props):
            hi = jnp.where(row_at == j, b_high, 0.0)
            lo = jnp.where(row_at == j, b_low, 0.0)
            full = jnp.concatenate([hi, hi, lo, jnp.zeros_like(hi)], axis=0)
            if g:
                full = pltpu.roll(full, block - g * size, 1)
            blocks.append(full)
        right = jnp.concatenate(blocks, axis=1).astype(BF16)
        update = lax.dot_general(
            left, right, (((0,), (0,)), ((), ())), preferred_element_type=F32
        )
        for h in range(high - low):
            at = g * per + low + h
            state = start[0, count - 1, at]
            for j in range(props):
                new = update[h * head_dim : (h + 1) * head_dim, j * block : j * block + size]
                state = state * small[j : j + 1, at : at + 1] + new
                held[j, filled + h] = state
        copy = pltpu.make_async_copy(
            held.at[:, pl.ds(filled, high - low)],
            states.at[0, :, pl.ds(g * per + low, high - low)],
            sem.at[pieces.index((g, low, high))],
        )
        copy.start()
        copies.append(copy)
        filled += high - low
    for copy in copies:
        copy.wait()


def output_body(count, props, *refs):
    parts = refs[:count]
    weight = refs[count]
    outs = refs[count + 2 : count + 2 + count]
    result, lhs = refs[-2:]
    me, part = lax.axis_index("kv"), lax.axis_index("tp")
    wide = parts[0].shape[1]
    rest = lhs.shape[1] - wide
    lhs[...] = jnp.zeros_like(lhs)
    for j, block in enumerate(parts):
        rows = block[...].astype(F32)
        lhs[4 * j : 4 * j + props, :wide] = rows[0:props]
        for r in range(props):
            at = 4 * j + r
            lhs[at : at + 1, wide:] = rows[3:4, r * rest : (r + 1) * rest]
    product = jnp.dot(lhs[...].astype(BF16), weight[...], preferred_element_type=F32)
    for j in range(count):
        result[j, 0:4] = product[4 * j : 4 * j + 4]
    for step in range(count):
        places = lax.rem(me - lax.bitwise_xor(part, step) + count, count)
        outs[step][...] = result[places, 0:4].astype(BF16)


def final_body(*refs):
    *parts, out = refs
    total = parts[0][...].astype(F32)
    for part in parts[1:]:
        total = total + part[...].astype(F32)
    out[0] = total[0 : out.shape[1]].astype(BF16)


def fast_local(
    count,
    tokens,
    input_norm_scale,
    head_input_matrix,
    output_gate_matrix,
    group_input_matrix,
    group_readout_matrix,
    step_size_matrix,
    step_size_bias,
    log_decay_rate,
    direct_path_weight,
    convolution_tap_weight,
    convolution_history_rows,
    per_proposal_states,
    accepted,
    proposal_extra_decay,
    group_norm_scale,
    output_projection_matrix,
):
    _, props, width = tokens.shape
    heads = step_size_bias.shape[0]
    _, _, groups, channels = convolution_history_rows.shape
    head_dim, size = per_proposal_states.shape[3:]
    inner = heads * head_dim
    conv = groups * channels
    rows = head_input_matrix.shape[0]
    total = conv + inner
    packed = packed_width(props, total)
    out_cols = output_projection_matrix.shape[1]

    slices = call(
        functools.partial(slice_body, count),
        [pltpu.VMEM((props, rows), BF16)] * count,
        [hbm(tokens)],
        [HBM_SPEC],
        scratch=[pltpu.SemaphoreType.DMA((count,))],
    )
    slices = call(
        hold_body,
        [pltpu.VMEM((props, rows), BF16)] * count,
        [vmem(v) for v in slices],
        [VMEM_SPEC] * count,
        flops=1_000_000_000_000,
        moved=10_000_000_000,
        aliases={i: i for i in range(count)},
    )
    received = exchange_tokens(slices, count)
    matrices = [head_input_matrix, group_input_matrix, group_readout_matrix, output_gate_matrix]

    scale = input_norm_scale.reshape(1, width)
    coef, small, norm = call(
        functools.partial(step_body, head_dim),
        [
            pltpu.VMEM((props + 2, ROWS, inner), F32),
            pltpu.VMEM((ROWS, heads), F32),
            pltpu.VMEM((ROWS, 128), F32),
        ],
        [
            accepted,
            vmem(tokens),
            vmem(scale),
            vmem(step_size_matrix.T),
            step_size_bias.reshape(1, heads),
            log_decay_rate.reshape(1, heads),
            direct_path_weight.reshape(1, heads),
            proposal_extra_decay.reshape(props, heads),
        ],
        [SMEM_SPEC] + [VMEM_SPEC] * 7,
        flops=20_000_000,
        scratch=[pltpu.VMEM(((props + 2) * ROWS, heads), F32)],
    )
    states = vmem(per_proposal_states)
    carry, early, taps = call(
        state_body,
        [
            pltpu.VMEM((2 * groups * size, inner), BF16),
            pltpu.VMEM((ROWS, conv), F32),
            pltpu.VMEM((ROWS, conv), F32),
        ],
        [accepted, states, convolution_history_rows, convolution_tap_weight],
        [SMEM_SPEC] + [VMEM_SPEC] * 3,
        flops=20_000_000,
    )

    own, *partials = call(
        functools.partial(project_body, count, props),
        [pltpu.VMEM((4, packed), F32)] + [pltpu.VMEM((4, packed), BF16)] * (count - 1),
        [vmem(s) for s in [slices[0]] + received]
        + matrices
        + [vmem(scale)],
        [VMEM_SPEC] * (count + 5),
        flops=200_000_000,
        scratch=[pltpu.VMEM((4 * count, rows), F32)],
    )
    sums = exchange([None] + partials, "kv", count)
    gated, fresh, act = call(
        functools.partial(mixer_body, props, groups, convolution_tap_weight.shape[0]),
        [
            pltpu.VMEM((4, packed_width(props, inner)), BF16),
            pltpu.VMEM((ROWS, conv), F32),
            pltpu.VMEM((ROWS, conv), F32),
        ],
        [vmem(v) for v in [own] + sums + [norm, coef, early, taps, carry]]
        + [vmem(group_norm_scale.reshape(1, inner))],
        [VMEM_SPEC] * (count + 6),
        flops=20_000_000,
        scratch=[pltpu.VMEM((ROWS, total), F32), pltpu.VMEM((ROWS, inner), F32)],
    )
    gathered = exchange_round(gated, "kv", count)
    per = heads // groups
    half = per // 2
    pieces = [(g, at, at + half) for g in range(groups) for at in (0, half)]
    first = len(pieces) // 4
    all_states = jax.ShapeDtypeStruct((1, props, heads, head_dim, size), F32)

    def scratch(number, *more):
        shape = (props, number * half, head_dim, size)
        return [pltpu.VMEM(shape, F32), *more, pltpu.SemaphoreType.DMA((number + 1,))]

    new_states, flag = call(
        functools.partial(states_body, props, groups, pieces[:first]),
        [all_states, pltpu.VMEM((ROWS, 128), F32)],
        [accepted, states] + [vmem(v) for v in (small, act, coef)],
        [SMEM_SPEC] + [VMEM_SPEC] * 4,
        flops=30_000_000,
        out_specs=[HBM_SPEC, VMEM_SPEC],
        scratch=scratch(first),
    )
    new_states, new_tail = call(
        functools.partial(states_body, props, groups, pieces[first:]),
        [all_states, jax.ShapeDtypeStruct(convolution_history_rows.shape, BF16)],
        [accepted, states]
        + [vmem(v) for v in (small, act, coef, fresh, convolution_history_rows)]
        + [hbm(new_states)],
        [SMEM_SPEC] + [VMEM_SPEC] * 6 + [HBM_SPEC],
        flops=30_000_000,
        out_specs=[HBM_SPEC, HBM_SPEC],
        scratch=scratch(
            len(pieces) - first, pltpu.VMEM(convolution_history_rows.shape, BF16)
        ),
        aliases={7: 0},
    )
    blocks = call(
        functools.partial(output_body, count, props),
        [pltpu.VMEM((4, out_cols), BF16)] * count,
        [vmem(v) for v in [gated] + gathered + [output_projection_matrix, flag]],
        [VMEM_SPEC] * (count + 2),
        flops=100_000_000,
        scratch=[
            pltpu.VMEM((count, ROWS, out_cols), F32),
            pltpu.VMEM((4 * count, inner), F32),
        ],
    )
    last = exchange(blocks, "tp", count)
    (mixed,) = call(
        final_body,
        [jax.ShapeDtypeStruct((1, props, out_cols), BF16)],
        [vmem(v) for v in [blocks[0]] + last],
        [VMEM_SPEC] * count,
    )
    return (mixed, new_states, new_tail)


def rms_scale(values):
    return lax.rsqrt(jnp.mean(values * values, axis=-1, keepdims=True) + epsilon)


def causal_states(log_decay_factor, head_step_size, ssm_inputs, inject, start_state):
    cumulative = jnp.cumsum(log_decay_factor, axis=1)
    length = log_decay_factor.shape[1]
    lower = (jnp.arange(length)[:, None] >= jnp.arange(length)[None, :])[None, :, :, None]
    spread = cumulative[:, :, None, :] - cumulative[:, None, :, :]
    factors = jnp.where(lower, jnp.exp(jnp.where(lower, spread, 0.0)), 0.0)
    mixing = factors * head_step_size[:, None, :, :]
    carried = jnp.exp(cumulative)[..., None, None] * start_state[:, None]
    return carried + jnp.einsum("sjih,sihp,sihn->sjhpn", mixing, ssm_inputs, inject)


def combine_head_outputs(
    incoming_token_rows,
    gate_portion,
    unactivated_step,
    step_size_bias,
    log_decay_rate,
    direct_path_weight,
    convolution_tap_weight,
    convolution_history_rows,
    per_proposal_states,
    accepted,
    proposal_extra_decay,
    group_norm_scale,
):
    sequences, proposals, group_count, group_width = incoming_token_rows.shape
    head_count = step_size_bias.shape[0]
    head_dim = per_proposal_states.shape[3]
    state_size = per_proposal_states.shape[4]
    per_group = head_count // group_count
    group_inner = per_group * head_dim
    tap_count = convolution_tap_weight.shape[0]
    offsets = accepted[:, None] + jnp.arange(tap_count - 1, dtype=jnp.int32)[None, :]
    context = jnp.take_along_axis(convolution_history_rows, offsets[:, :, None, None], axis=1)
    convolution_span = jnp.concatenate([context, incoming_token_rows], axis=1)
    widened = convolution_span.astype(jnp.float32)
    convolved = jnp.zeros((sequences, proposals, group_count, group_width), jnp.float32)
    for conv_tap in range(tap_count):
        convolved = convolved + widened[
            :, conv_tap : conv_tap + proposals
        ] * convolution_tap_weight[conv_tap].astype(jnp.float32)
    activated = jax.nn.silu(convolved)
    ssm_inputs = activated[..., :group_inner].reshape(sequences, proposals, head_count, head_dim)
    inject = jnp.repeat(activated[..., group_inner : group_inner + state_size], per_group, axis=2)
    readout = jnp.repeat(activated[..., group_inner + state_size :], per_group, axis=2)
    head_step_size = jax.nn.softplus(unactivated_step + step_size_bias)
    log_decay_factor = proposal_extra_decay - jnp.exp(log_decay_rate) * head_step_size
    chosen = (accepted - 1)[:, None, None, None, None]
    start_state = jnp.take_along_axis(per_proposal_states, chosen, axis=1)[:, 0]
    running_state_rows = causal_states(
        log_decay_factor, head_step_size, ssm_inputs, inject, start_state
    )
    response = (
        jnp.einsum("sjhn,sjhpn->sjhp", readout, running_state_rows)
        + direct_path_weight[:, None] * ssm_inputs
    )
    gate_raw = gate_portion.astype(jnp.float32).reshape(sequences, proposals, head_count, head_dim)
    gate_applied_output = (response * jax.nn.silu(gate_raw)).reshape(
        sequences, proposals, group_count, group_inner
    )
    scaled = (
        gate_applied_output
        * rms_scale(gate_applied_output)
        * group_norm_scale.reshape(group_count, group_inner)
    )
    flat_gated = scaled.astype(jnp.bfloat16).reshape(sequences, proposals, head_count * head_dim)
    return (flat_gated, running_state_rows, convolution_span)


def local(
    tokens,
    input_norm_scale,
    head_input_matrix,
    output_gate_matrix,
    group_input_matrix,
    group_readout_matrix,
    step_size_matrix,
    step_size_bias,
    log_decay_rate,
    direct_path_weight,
    convolution_tap_weight,
    convolution_history_rows,
    per_proposal_states,
    accepted,
    proposal_extra_decay,
    group_norm_scale,
    output_projection_matrix,
):
    local_seqs, proposals, _ = tokens.shape
    head_local = step_size_bias.shape[0]
    group_local = convolution_tap_weight.shape[1]
    head_dim = per_proposal_states.shape[3]
    state_size = per_proposal_states.shape[4]
    group_inner = head_local // group_local * head_dim
    widened = tokens.astype(jnp.float32)
    normed = (widened * rms_scale(widened) * input_norm_scale).astype(jnp.bfloat16)
    unactivated_step = jnp.einsum(
        "sjd,dh->sjh", normed, step_size_matrix, preferred_element_type=jnp.float32
    )
    pieces = lax.all_to_all(normed, "kv", split_axis=2, concat_axis=0, tiled=True)
    joined = jnp.concatenate(
        [head_input_matrix, group_input_matrix, group_readout_matrix, output_gate_matrix], axis=1
    )
    summed = lax.psum_scatter(
        jnp.einsum("sjd,dc->sjc", pieces, joined, preferred_element_type=jnp.float32),
        "kv",
        scatter_dimension=0,
        tiled=True,
    )
    projected = summed.astype(jnp.bfloat16)
    input_width = head_local * head_dim
    inject_width = group_local * state_size
    part_input = projected[..., :input_width].reshape(
        local_seqs, proposals, group_local, group_inner
    )
    part_inject = projected[..., input_width : input_width + inject_width].reshape(
        local_seqs, proposals, group_local, state_size
    )
    part_readout = projected[
        ..., input_width + inject_width : input_width + 2 * inject_width
    ].reshape(local_seqs, proposals, group_local, state_size)
    gate_portion = projected[..., input_width + 2 * inject_width :]
    incoming_token_rows = jnp.concatenate([part_input, part_inject, part_readout], axis=-1)
    gate_applied_output, running_state_rows, convolution_span = combine_head_outputs(
        incoming_token_rows,
        gate_portion,
        unactivated_step,
        step_size_bias,
        log_decay_rate,
        direct_path_weight,
        convolution_tap_weight,
        convolution_history_rows,
        per_proposal_states,
        accepted,
        proposal_extra_decay,
        group_norm_scale,
    )
    terms = jnp.einsum(
        "sjc,cd->sjd",
        lax.all_gather(gate_applied_output, "kv", axis=0, tiled=True),
        output_projection_matrix,
        preferred_element_type=jnp.float32,
    )
    mixed = lax.psum_scatter(terms.astype(jnp.bfloat16), "tp", scatter_dimension=0, tiled=True)
    return (mixed, running_state_rows, convolution_span)


def chosen(mesh, *arguments):
    tokens, matrix = arguments[0], arguments[2]
    kv, tp = mesh.shape["kv"], mesh.shape["tp"]
    slim = tokens.shape[:2] == (1, 3) and matrix.shape[0] % 128 == 0
    slim = slim and arguments[10].shape[1] == 2
    if slim and kv == tp and kv in (2, 4):
        return fast_local(kv, *arguments)
    return local(*arguments)


def solution(mesh):
    return jax.shard_map(
        functools.partial(chosen, mesh),
        mesh=mesh,
        in_specs=(
            P(("grp", "kv"), None, None),
            P(),
            P("kv", "tp"),
            P("kv", "tp"),
            P("kv", "tp"),
            P("kv", "tp"),
            P(None, "tp"),
            P("tp"),
            P("tp"),
            P("tp"),
            P(None, "tp", None),
            P(("grp", "kv"), None, "tp", None),
            P(("grp", "kv"), None, "tp", None, None),
            P(("grp", "kv")),
            P(("grp", "kv"), None, "tp"),
            P("tp"),
            P("tp", "kv"),
        ),
        out_specs=(
            P(("grp", "tp"), None, "kv"),
            P(("grp", "kv"), None, "tp", None, None),
            P(("grp", "kv"), None, "tp", None),
        ),
        check_vma=False,
    )
```
